128 devices in a mesh: sp: 64 (over z, y, x), tp: 2 (over core).
Axes of the slice: x: 4, y: 4, z: 4, core: 2. Of those that a mesh axis runs over, the one named last changes fastest.
Arguments:
- out_grad: bfloat16 [14336, 2048], P('sp'), may hold values from -16 to 16
- moe_input: bfloat16 [14336, 2048], P('sp'), may hold values from -6 to 6
- routes: int32 [14336, 2], P('sp'), may hold values from 0 to 63, all different within a row; in each aligned block of 224 rows (0 to 223, 224 to 447, ...) at most 14 rows name the same one
- route_weights: float32 [14336, 2], P('sp'), may hold values from 0.2 to 1
- conv_result: bfloat16 [14336, 1024], P('sp', 'tp'), may hold values from -60 to 60
- glu_value: bfloat16 [14336, 1024], P('sp', 'tp'), may hold values from -6 to 6
- glu_gate: bfloat16 [14336, 1024], P('sp', 'tp'), may hold values from -6 to 6
- conv_taps: bfloat16 [31, 1024], P(None, 'tp'), may hold values from -1 to 1
- norm_gain: float32 [1024], P('tp'), may hold values from 0.1 to 1.9
- proj_weight: bfloat16 [2048, 1024], P(None, 'tp'), may hold values from -0.1875 to 0.1875
- expert_gate: bfloat16 [64, 2048, 1024], P('sp', None, 'tp'), may hold values from -0.125 to 0.125
- expert_up: bfloat16 [64, 2048, 1024], P('sp', None, 'tp'), may hold values from -0.125 to 0.125
- expert_down: bfloat16 [64, 1024, 2048], P('sp', 'tp'), may hold values from -0.1875 to 0.1875
Outputs:
- input_grad: bfloat16 [14336, 2048], P('sp')
- proj_grad: float32 [2048, 1024], P('sp', 'tp')
- gate_grad: float32 [64, 2048, 1024], P('sp', None, 'tp')
- up_grad: float32 [64, 2048, 1024], P('sp', None, 'tp')
- down_grad: float32 [64, 1024, 2048], P('sp', 'tp')
- value_grad: bfloat16 [14336, 1024], P('sp', 'tp')
- gate_side_grad: bfloat16 [14336, 1024], P('sp', 'tp')
The draws below stay inside these ranges and needn't reach their ends.
Inputs may be any that keep to these rules, and one draw needn't show every extreme that they name: `routes`: in each aligned block of 224 tokens no expert is named more than 14 times, a bound that some block reaches; a token's experts differ.
All inputs are finite; a program needn't handle non-finite values.
Results may differ from the reference program's by a relative error of at most 0.0061.
Values may be sent and summed in bfloat16 or wider, within the bound.
No kernel may reach another device: no remote copies, remote signals or barrier semaphores. Data moves between devices by JAX's collectives and lax.ppermute only.
A program may use at most 128 MiB of HBM per device.

```python
import math
import jax
import jax.numpy as jnp
import numpy as np
from jax import lax

D = 2048
CH = 1024
FFE = 1024
CONV_K = 31
TOP = 2
TOK_DEV = 224
TOKENS = 14336
EXPERTS = 64
CAP = 14
N_SP = 64
N_TP = 2


def draw_conv_result(key, part):
    first_key = jax.random.fold_in(jax.random.fold_in(key, 17), 0)
    channel = jnp.arange(CH, dtype=jnp.float32) / CH
    scale = (10.0 ** channel)[None, :]
    values = jnp.clip(jax.random.normal(first_key, (TOKENS, CH), jnp.float32), -6.0, 6.0) * scale
    return values.astype(jnp.bfloat16)


def with_spikes(entries, stream_key, source, target, blocks, factor):
    owner, partner = [(jnp.arange(entries.shape[dim]) // (entries.shape[dim] // blocks)).reshape([-1 if axis == dim else 1 for axis in range(entries.ndim)]) for dim in (source, target)]
    chosen = jax.random.permutation(stream_key, blocks)[partner]
    strong = (owner == chosen) | (owner == (partner + blocks // 2) % blocks)
    return jnp.where(strong, factor * entries, entries)


def steps_of(stream_key, extent, cuts, smallest, high):
    level = 1.0
    for axis_at, shards_of in cuts:
        heights = jax.random.uniform(jax.random.fold_in(jax.random.fold_in(stream_key, 6), axis_at), (shards_of,), jnp.float32, smallest / len(cuts), high / len(cuts))
        level = level * jnp.repeat(jnp.exp(heights), extent[axis_at] // shards_of).reshape((-1,) + (1,) * (len(extent) - 1 - axis_at))
    return level


def deal_out(key, own, number, rows, number_of, top, bound, skew):
    order = jax.random.permutation(key, number_of)
    heavy_load, common = load_shares(number_of, rows * top, bound, skew, True), load_shares(number_of, rows * top, bound, skew, False)
    places = jnp.arange(number_of)

    def named(tallies, offset_by):
        used = int((tallies > 0).sum())
        fixed = max(1, used // 4)
        moved = fixed + (places - fixed + offset_by * (used - fixed)) % max(1, number_of - fixed)
        return jnp.zeros((number_of,), jnp.int32).at[order[jnp.where(places < fixed, places, moved)]].set(jnp.asarray(tallies, jnp.int32))

    tallies = jnp.where(number % 4 == 0, named(heavy_load, number // 4), named(common, number - number // 4 - 1))
    mixed = jax.random.permutation(jax.random.fold_in(own, 3), number_of)
    donor, taker = mixed[0:number_of // 2 * 2:2], mixed[1:number_of // 2 * 2:2]
    margin = jnp.minimum(tallies[donor] - 1, bound - tallies[taker]) // 2
    margin = jnp.where((donor == order[0]) | (taker == order[0]) | (tallies[taker] == 0), 0, jnp.maximum(margin, 0))
    moved = jax.random.randint(jax.random.fold_in(own, 4), (number_of // 2,), 0, 1 << 20) % (margin + 1)
    tallies = tallies.at[donor].add(-moved).at[taker].add(moved)
    members = jnp.searchsorted(jnp.cumsum(tallies), jnp.arange(rows * top), side="right").astype(jnp.int32)
    grid = members.reshape(top, rows).T
    grid = grid[jax.random.permutation(jax.random.fold_in(own, 1), rows)]
    offset_by = jax.random.randint(jax.random.fold_in(own, 2), (rows, 1), 0, top)
    return jnp.take_along_axis(grid, (jnp.arange(top)[None, :] + offset_by) % top, axis=1)


def load_shares(number_of, total, most, slope, full):
    loads = [(1 << 20) // math.isqrt(rank ** slope) + 1 for rank in range(1, number_of + 1)]
    largest = most if full else min(most, max(-(-total // number_of), total * loads[0] // sum(loads)))
    least = 1 if total - largest >= number_of - 1 else 0
    holding, rest = [largest] + [least] * (number_of - 1), total - largest - least * (number_of - 1)
    while rest > 0:
        movable = [i for i in range(1, number_of) if holding[i] < largest] or [i for i in range(1, number_of) if holding[i] < most]
        whole, left = sum([loads[i] for i in movable]), rest
        for i in movable:
            extra = min(most - holding[i], max(1, left * loads[i] // whole), rest)
            holding[i] = holding[i] + extra
            rest = rest - extra
    return np.array(holding)


def centred(key, dims, deviation, limit, pieces=(), kind=jnp.bfloat16):
    drawn = jax.random.normal(key, dims, jnp.float32) * deviation
    if len(pieces) > 0:
        drawn = steps_of(key, dims, pieces, -0.22, 0.18) * drawn
    return jnp.clip(drawn, min=-limit, max=limit).astype(kind)


def gaussian_with(stream_key, extent, width, bound, pieces, heavy, kind=jnp.bfloat16):
    entries = width * jax.random.normal(stream_key, extent, jnp.float32)
    if pieces:
        entries = entries * steps_of(stream_key, extent, pieces, -0.22, 0.18)
    return jnp.clip(with_spikes(entries, jax.random.fold_in(stream_key, 3), *heavy), -bound, bound).astype(kind)


def setup_inputs(seed: int = 0) -> dict:
    seeds = jax.random.split(jax.random.key(seed), 14)
    out_grad = gaussian_with(seeds[0], (TOKENS, D), 1.0, 16.0, ((0, 64),), (0, 1, 64, 4.0))
    moe_input = centred(seeds[1], (TOKENS, D), 1.0, 6.0, ((0, 64),))
    routes_keys = jax.random.split(jax.random.fold_in(seeds[2], 1), TOKENS // TOK_DEV)
    routes_turns = jax.random.permutation(jax.random.fold_in(seeds[2], 3), TOKENS // TOK_DEV)
    routes = jax.vmap(lambda own, number: deal_out(jax.random.fold_in(seeds[2], 2), own, number, TOK_DEV, EXPERTS, TOP, CAP, 1))(routes_keys, routes_turns).reshape((TOKENS, TOP))
    route_weights = jnp.clip(0.2 + 0.8 * jax.random.uniform(seeds[3], (TOKENS, TOP), jnp.float32) ** steps_of(seeds[3], (TOKENS, TOP), ((0, 64),), -0.2, 0.2), 0.2, 1.0)
    conv_result = draw_conv_result(jax.random.fold_in(seeds[13], 71), 0)
    glu_value = centred(seeds[5], (TOKENS, CH), 1.0, 6.0, ((0, 64), (1, 2)))
    glu_gate = centred(seeds[6], (TOKENS, CH), 1.0, 6.0, ((0, 64), (1, 2)))
    conv_taps = centred(seeds[7], (CONV_K, CH), CONV_K ** -0.5, 1.0, ((1, 2),))
    norm_gain = jnp.clip(1.0 + 0.18 * jax.random.normal(seeds[8], (CH,), jnp.float32), 0.1, 1.9)
    proj_weight = centred(seeds[9], (D, CH), CH ** -0.5, 0.1875, ((1, 2),))
    expert_gate = centred(seeds[10], (EXPERTS, D, FFE), D ** -0.5, 0.125, ((0, 64), (2, 2)))
    expert_up = centred(seeds[11], (EXPERTS, D, FFE), D ** -0.5, 0.125, ((0, 64), (2, 2)))
    expert_down = centred(seeds[12], (EXPERTS, FFE, D), FFE ** -0.5, 0.1875, ((0, 64), (1, 2)))
    return dict(out_grad=out_grad, moe_input=moe_input, routes=routes, route_weights=route_weights, conv_result=conv_result, glu_value=glu_value, glu_gate=glu_gate, conv_taps=conv_taps, norm_gain=norm_gain, proj_weight=proj_weight, expert_gate=expert_gate, expert_up=expert_up, expert_down=expert_down)


norm_eps = 1e-05

def contract_rows(left, right):
    return lax.dot_general(left, right, (((0,), (0,)), ((), ())), preferred_element_type=jnp.float32)

def reference(out_grad, moe_input, routes, route_weights, conv_result, glu_value, glu_gate, conv_taps, norm_gain, proj_weight, expert_gate, expert_up, expert_down):
    slots = N_SP * CAP
    assigned = TOKENS * TOP
    flat = routes.reshape(N_SP, TOK_DEV * TOP).astype(jnp.int32)
    onehot = (flat[:, :, None] == jnp.arange(EXPERTS, dtype=jnp.int32)[None, None, :]).astype(jnp.int32)
    earlier = jnp.cumsum(onehot, axis=1) - onehot
    slot_index = lax.optimization_barrier(jnp.sum(earlier * onehot, axis=2))
    position = (jnp.arange(N_SP, dtype=jnp.int32)[:, None] * CAP + slot_index).reshape(-1).astype(jnp.int32)
    expert_flat = flat.reshape(-1)
    table = jnp.full((EXPERTS, slots), assigned, jnp.int32).at[expert_flat, position].set(jnp.arange(assigned, dtype=jnp.int32))
    grad_padded = jnp.concatenate([out_grad, jnp.zeros((1, D), jnp.bfloat16)], axis=0)
    input_padded = jnp.concatenate([moe_input, jnp.zeros((1, D), jnp.bfloat16)], axis=0)
    weight_padded = jnp.concatenate([route_weights.reshape(-1), jnp.zeros((1,), jnp.float32)])
    row_scale = float(slots) ** (-0.5)
    piece = FFE // N_TP

    def per_expert(args):
        index, weight_g, weight_u, weight_d = args
        token = jnp.where(index < assigned, index // TOP, TOKENS).astype(jnp.int32)
        inputs = input_padded[token]
        grads = (grad_padded[token].astype(jnp.float32) * weight_padded[index][:, None]).astype(jnp.bfloat16)
        gate_pre = jnp.dot(inputs, weight_g, preferred_element_type=jnp.float32)
        up_pre = jnp.dot(inputs, weight_u, preferred_element_type=jnp.float32)
        sigma = jax.nn.sigmoid(gate_pre)
        silu_gate = gate_pre * sigma
        hidden = (silu_gate * up_pre).astype(jnp.bfloat16)
        down_g = contract_rows(hidden, grads) * row_scale
        hidden_grad = lax.dot_general(grads, weight_d, (((1,), (1,)), ((), ())), preferred_element_type=jnp.float32)
        gate_back = (hidden_grad * up_pre * sigma * (1.0 + gate_pre * (1.0 - sigma))).astype(jnp.bfloat16)
        up_back = (hidden_grad * silu_gate).astype(jnp.bfloat16)
        gate_g = contract_rows(inputs, gate_back) * row_scale
        up_g = contract_rows(inputs, up_back) * row_scale
        back_gate = jnp.einsum('rpf,dpf->prd', gate_back.reshape(slots, N_TP, piece).astype(jnp.float32), weight_g.reshape(D, N_TP, piece).astype(jnp.float32))
        back_up = jnp.einsum('rpf,dpf->prd', up_back.reshape(slots, N_TP, piece).astype(jnp.float32), weight_u.reshape(D, N_TP, piece).astype(jnp.float32))
        partial_value = lax.optimization_barrier((back_gate + back_up).astype(jnp.bfloat16)).astype(jnp.float32)
        rows_back = lax.optimization_barrier(jnp.sum(partial_value, axis=0)).astype(jnp.bfloat16)
        return (gate_g, up_g, down_g, rows_back)
    gate_grad, up_grad, down_grad, returned = lax.map(per_expert, (table, expert_gate, expert_up, expert_down))
    contrib = returned.reshape(EXPERTS * slots, D)[(expert_flat * slots + position).astype(jnp.int32)]
    total = out_grad.astype(jnp.float32) + lax.optimization_barrier(jnp.sum(contrib.reshape(TOKENS, TOP, D).astype(jnp.float32), axis=1))
    input_grad = total.astype(jnp.bfloat16)
    values = conv_result.astype(jnp.float32)
    center = lax.optimization_barrier(jnp.mean(values, axis=1, keepdims=True))
    spread = lax.optimization_barrier(jnp.mean(values * values, axis=1, keepdims=True)) - center * center
    inv_std = lax.rsqrt(spread + norm_eps)
    normed = (values - center) * inv_std
    scaled = normed * norm_gain[None, :]
    sig_norm = jax.nn.sigmoid(scaled)
    activ = (scaled * sig_norm).astype(jnp.bfloat16)
    proj_grad = contract_rows(input_grad, activ) * float(TOKENS) ** (-0.5)
    act_grad = jnp.dot(input_grad, proj_weight, preferred_element_type=jnp.float32)
    norm_grad = act_grad * sig_norm * (1.0 + scaled * (1.0 - sig_norm)) * norm_gain[None, :]
    first = lax.optimization_barrier(jnp.mean(norm_grad, axis=1, keepdims=True))
    second = lax.optimization_barrier(jnp.mean(norm_grad * normed, axis=1, keepdims=True))
    conv_grad = inv_std * (norm_grad - first - normed * second)
    extended = jnp.concatenate([conv_grad, jnp.zeros((CONV_K - 1, CH), jnp.float32)], axis=0)
    taps_float = conv_taps.astype(jnp.float32)
    mixed_grad = jnp.zeros((TOKENS, CH), jnp.float32)
    for lag in range(CONV_K):
        mixed_grad = mixed_grad + taps_float[CONV_K - 1 - lag][None, :] * extended[lag:lag + TOKENS]
    sig_gate = jax.nn.sigmoid(glu_gate.astype(jnp.float32))
    value_grad = (mixed_grad * sig_gate).astype(jnp.bfloat16)
    gate_side_grad = (mixed_grad * glu_value.astype(jnp.float32) * sig_gate * (1.0 - sig_gate)).astype(jnp.bfloat16)
    return (input_grad, proj_grad, gate_grad, up_grad, down_grad, value_grad, gate_side_grad)
```

```python
import functools

import jax
import jax.numpy as jnp
from jax import lax
from jax.experimental import pallas as pl
from jax.experimental.pallas import tpu as pltpu
from jax.sharding import PartitionSpec as P

norm_eps = 1e-05
swap = [(0, 1), (1, 0)]


def in_blocks(shard, dim, count):
    before, after = (shard.shape[:dim], shard.shape[dim + 1 :])
    return jnp.moveaxis(shard.reshape(*before, count, -1, *after), dim, 0)


def summed_on_arrival(shard, axis, dim):
    parts = in_blocks(shard, dim, lax.axis_size(axis))
    arrived = lax.all_to_all(parts, axis, split_axis=0, concat_axis=0, tiled=True)
    return arrived.astype(jnp.float32).sum(axis=0)


def from_behind(shard, axis, by):
    count = lax.axis_size(axis)
    pairs = [(i, i + by) for i in range(count) if 0 <= i + by < count]
    return lax.ppermute(shard, axis, pairs)


def contract_rows(left, right):
    return lax.dot_general(
        left, right, (((0,), (0,)), ((), ())), preferred_element_type=jnp.float32
    )


def contract_cols(left, right):
    return lax.dot_general(
        left, right, (((1,), (1,)), ((), ())), preferred_element_type=jnp.float32
    )


def matmul(left, right):
    return jnp.dot(left, right, preferred_element_type=jnp.float32)


def iota(shape, dim):
    return lax.broadcasted_iota(jnp.int32, shape, dim)


def whole(shape):
    return pl.BlockSpec(shape, lambda *_: (0,) * len(shape))


smem = pl.BlockSpec(memory_space=pltpu.SMEM)


def slot_tables(routes_ref, experts):
    tokens = routes_ref.shape[0]
    column = iota((tokens, experts), 1)
    named = [routes_ref[:, k : k + 1] == column for k in range(2)]
    both = jnp.where(named[0] | named[1], 1.0, 0.0).astype(jnp.bfloat16)
    earlier = jnp.where(iota((tokens, tokens), 1) < iota((tokens, tokens), 0), 1.0, 0.0)
    slot = matmul(earlier.astype(jnp.bfloat16), both)
    return [jnp.where(n, slot, -1.0).astype(jnp.bfloat16) for n in named]


def pick_rows(tables, row_expert, row_slot):
    rows = row_slot.shape[0]
    experts = tables[0].shape[1]
    spread = jnp.where(row_expert == iota((rows, experts), 1), 1.0, 0.0).astype(jnp.bfloat16)
    return [contract_cols(spread, table) == row_slot.astype(jnp.float32) for table in tables]


def dispatch_body(tp_ref, routes_ref, weights_ref, input_ref, grad_ref, out_ref, pick_ref, half):
    step = pl.program_id(0)
    blocks = pl.num_programs(0) // 2
    rows, tokens = out_ref.shape[0], routes_ref.shape[0]
    experts = rows // 8

    @pl.when(step == 0)
    def _():
        tables = slot_tables(routes_ref, experts)
        place = iota((rows, tokens), 0)
        within = place & 7
        slot = jnp.where(within < half, tp_ref[0] * half + within, -2)
        picks = pick_rows(tables, iota((rows, experts), 0) >> 3, slot)
        for k in range(2):
            pick_ref[k] = jnp.where(picks[k], 1.0, 0.0).astype(jnp.bfloat16)

    @pl.when(step < blocks)
    def _():
        out_ref[...] = matmul(pick_ref[0] + pick_ref[1], input_ref[...]).astype(jnp.bfloat16)

    @pl.when(step >= blocks)
    def _():
        grad = grad_ref[...].astype(jnp.float32)
        scaled = [(grad * weights_ref[:, k : k + 1]).astype(jnp.bfloat16) for k in range(2)]
        out_ref[...] = (matmul(pick_ref[0], scaled[0]) + matmul(pick_ref[1], scaled[1])).astype(
            jnp.bfloat16
        )


def dispatch(tp, routes, weights, moe_input, out_grad, experts, half):
    tokens, width = out_grad.shape
    rows = experts * 8
    blocks = 4
    wide = width // blocks
    return pl.pallas_call(
        functools.partial(dispatch_body, half=half),
        grid=(2 * blocks,),
        in_specs=[
            smem,
            whole(routes.shape),
            whole(weights.shape),
            pl.BlockSpec((tokens, wide), lambda i: (0, jnp.minimum(i, blocks - 1))),
            pl.BlockSpec((tokens, wide), lambda i: (0, jnp.maximum(i - blocks, 0))),
        ],
        out_specs=pl.BlockSpec((rows, wide), lambda i: (0, i)),
        out_shape=jax.ShapeDtypeStruct((rows, 2 * width), jnp.bfloat16),
        scratch_shapes=[pltpu.VMEM((2, rows, tokens), jnp.bfloat16)],
        name="dispatch",
    )(tp, routes, weights, moe_input, out_grad)


def picks_body(tp_ref, routes_ref, out_ref, half):
    rows, tokens = out_ref.shape
    experts = rows // 16
    tables = slot_tables(routes_ref, experts)
    place = iota((rows, tokens), 0)
    within = place & 7
    side = (tp_ref[0] + ((place >> 3) & 1)) & 1
    slot = jnp.where(within < half, side * half + within, -2)
    picks = pick_rows(tables, iota((rows, experts), 0) >> 4, slot)
    out_ref[...] = jnp.where(picks[0] | picks[1], 1.0, 0.0).astype(jnp.bfloat16)


def return_picks(tp, routes, experts, half):
    shape = (experts * 16, routes.shape[0])
    return pl.pallas_call(
        functools.partial(picks_body, half=half),
        in_specs=[smem, whole(routes.shape)],
        out_specs=whole(shape),
        out_shape=jax.ShapeDtypeStruct(shape, jnp.bfloat16),
        name="picks",
    )(tp, routes)


def expert_body(tp_ref, rows_ref, gate_ref, up_ref, down_ref, hid_ref, gb_ref, ub_ref, pv_ref):
    width = gate_ref.shape[0]
    share = width // 2
    inputs = rows_ref[:, :width]
    gate_pre = matmul(inputs, gate_ref[...])
    up_pre = matmul(inputs, up_ref[...])
    sigma = jax.nn.sigmoid(gate_pre)
    silu_gate = gate_pre * sigma
    hid_ref[...] = (silu_gate * up_pre).astype(jnp.bfloat16)
    hidden_grad = contract_cols(rows_ref[:, width:], down_ref[...])
    gb_ref[...] = (hidden_grad * up_pre * sigma * (1.0 + gate_pre * (1.0 - sigma))).astype(
        jnp.bfloat16
    )
    ub_ref[...] = (hidden_grad * silu_gate).astype(jnp.bfloat16)
    away = pl.ds(pl.multiple_of((1 - tp_ref[0]) * share, share), share)
    pv_ref[...] = (
        contract_cols(gb_ref[...], gate_ref[away, :]) + contract_cols(ub_ref[...], up_ref[away, :])
    ).astype(jnp.bfloat16)


def expert(tp, rows, gate, up, down, name):
    count = rows.shape[0]
    width, units = gate.shape
    outs = [(count, units)] * 3 + [(count, width // 2)]
    return pl.pallas_call(
        expert_body,
        in_specs=[smem, whole(rows.shape), whole(gate.shape), whole(up.shape), whole(down.shape)],
        out_specs=[whole(s) for s in outs],
        out_shape=[jax.ShapeDtypeStruct(s, jnp.bfloat16) for s in outs],
        name=name,
    )(tp, rows, gate, up, down)


def kept_body(tp_ref, gb0_ref, ub0_ref, gb1_ref, ub1_ref, gate_ref, up_ref, out0_ref, out1_ref):
    share = gate_ref.shape[0] // 2
    here = pl.ds(pl.multiple_of(tp_ref[0] * share, share), share)
    for gb_ref, ub_ref, out_ref in ((gb0_ref, ub0_ref, out0_ref), (gb1_ref, ub1_ref, out1_ref)):
        out_ref[...] = (
            contract_cols(gb_ref[...], gate_ref[here, :])
            + contract_cols(ub_ref[...], up_ref[here, :])
        ).astype(jnp.bfloat16)


def kept_partials(tp, gb0, ub0, gb1, ub1, gate, up):
    out = (gb0.shape[0], gate.shape[0] // 2)
    arrays = (gb0, ub0, gb1, ub1, gate, up)
    return pl.pallas_call(
        kept_body,
        in_specs=[smem] + [whole(a.shape) for a in arrays],
        out_specs=[whole(out)] * 2,
        out_shape=[jax.ShapeDtypeStruct(out, jnp.bfloat16)] * 2,
        name="kept",
    )(tp, *arrays)


def total_body(kept0_ref, kept1_ref, came0_ref, came1_ref, out_ref):
    groups = out_ref.shape[0]
    for side, (kept_ref, came_ref) in enumerate(((kept0_ref, came0_ref), (kept1_ref, came1_ref))):
        total = kept_ref[...].astype(jnp.float32) + came_ref[...].astype(jnp.float32)
        out_ref[:, 8 * side : 8 * side + 8, :] = total.reshape(groups, 8, -1).astype(jnp.bfloat16)


def total_rows(kept0, kept1, came0, came1):
    rows, share = kept0.shape
    blocks = 4
    wide = share // blocks
    spec = pl.BlockSpec((rows, wide), lambda i: (0, i))
    return pl.pallas_call(
        total_body,
        grid=(blocks,),
        in_specs=[spec] * 4,
        out_specs=pl.BlockSpec((rows // 8, 16, wide), lambda i: (0, 0, i)),
        out_shape=jax.ShapeDtypeStruct((rows // 8, 16, share), jnp.bfloat16),
        name="total",
    )(kept0, kept1, came0, came1)


def weights_body(
    in0_ref, in1_ref, gr0_ref, gr1_ref, hid0_ref, hid1_ref, gb0_ref, gb1_ref, ub0_ref, ub1_ref,
    gate_ref, up_ref, down_ref, scale,
):
    gate_ref[...] = (
        contract_rows(in0_ref[...], gb0_ref[...]) + contract_rows(in1_ref[...], gb1_ref[...])
    ) * scale
    up_ref[...] = (
        contract_rows(in0_ref[...], ub0_ref[...]) + contract_rows(in1_ref[...], ub1_ref[...])
    ) * scale
    down_ref[...] = (
        contract_rows(hid0_ref[...], gr0_ref[...]) + contract_rows(hid1_ref[...], gr1_ref[...])
    ) * scale


def weight_grads(rows0, rows1, own, other, scale):
    count, units = own[0].shape
    width = rows0.shape[1] // 2
    blocks = 8
    wide = width // blocks
    first = pl.BlockSpec((count, wide), lambda i: (0, i))
    second = pl.BlockSpec((count, wide), lambda i: (0, blocks + i))
    flops = 3 * 2 * 2 * count * width * units
    return pl.pallas_call(
        functools.partial(weights_body, scale=scale),
        grid=(blocks,),
        in_specs=[first, first, second, second] + [whole((count, units))] * 6,
        out_specs=[
            pl.BlockSpec((wide, units), lambda i: (i, 0)),
            pl.BlockSpec((wide, units), lambda i: (i, 0)),
            pl.BlockSpec((units, wide), lambda i: (0, i)),
        ],
        out_shape=[
            jax.ShapeDtypeStruct((width, units), jnp.float32),
            jax.ShapeDtypeStruct((width, units), jnp.float32),
            jax.ShapeDtypeStruct((units, width), jnp.float32),
        ],
        cost_estimate=pl.CostEstimate(
            flops=flops, bytes_accessed=12 * width * units, transcendentals=0
        ),
        name="weight_grads",
    )(rows0, rows1, rows0, rows1, own[0], other[0], own[1], other[1], own[2], other[2])


def per_device(
    out_grad,
    moe_input,
    routes,
    route_weights,
    conv_result,
    glu_value,
    glu_gate,
    conv_taps,
    norm_gain,
    proj_weight,
    expert_gate,
    expert_up,
    expert_down,
):
    n_sp = lax.axis_size("sp")
    n_tp = lax.axis_size("tp")
    tok_rows, width = out_grad.shape
    top_count = routes.shape[1]
    capacity = 2 * top_count * tok_rows // n_sp
    half = capacity // n_tp
    slots = n_sp * capacity
    tp = lax.axis_index("tp")
    tp_array = tp.reshape(1).astype(jnp.int32)
    share = width // n_tp
    channels = conv_result.shape[1] * n_tp

    send = dispatch(tp_array, routes, route_weights, moe_input, out_grad, n_sp, half)
    rows0 = lax.all_to_all(
        send.reshape(n_sp, 8, 2 * width), "sp", split_axis=0, concat_axis=0, tiled=True
    ).reshape(n_sp * 8, 2 * width)
    rows1 = lax.ppermute(rows0, "tp", swap)

    gate, up, down = expert_gate[0], expert_up[0], expert_down[0]
    own = expert(tp_array, rows0, gate, up, down, "expert_own")
    other = expert(tp_array, rows1, gate, up, down, "expert_other")
    came1 = lax.ppermute(own[3], "tp", swap)
    came0 = lax.ppermute(other[3], "tp", swap)
    kept0, kept1 = kept_partials(tp_array, own[1], own[2], other[1], other[2], gate, up)
    summed = total_rows(kept0, kept1, came0, came1)
    returned = lax.all_to_all(summed, "sp", split_axis=0, concat_axis=0, tiled=True).reshape(
        n_sp * 16, share
    )
    gate_g, up_g, down_g = weight_grads(rows0, rows1, own, other, float(slots) ** (-0.5))

    values = conv_result.astype(jnp.float32)
    sums = lax.psum(
        (jnp.sum(values, axis=1), jnp.sum(values * values, axis=1)), "tp"
    )
    center = sums[0] / channels
    spread = sums[1] / channels - center * center
    inv_std = lax.rsqrt(spread + norm_eps)[:, None]
    normed = (values - center[:, None]) * inv_std
    scaled = normed * norm_gain[None, :]
    sig_norm = jax.nn.sigmoid(scaled)
    activ = (scaled * sig_norm).astype(jnp.bfloat16)

    picks = return_picks(tp_array, routes, n_sp, half)
    grad_here = lax.dynamic_slice_in_dim(out_grad, tp * share, share, 1).astype(jnp.float32)
    here = (grad_here + contract_rows(picks, returned)).astype(jnp.bfloat16)
    there = lax.ppermute(here, "tp", swap)
    input_grad = jnp.where(
        tp == 0,
        jnp.concatenate([here, there], axis=1),
        jnp.concatenate([there, here], axis=1),
    )
    token_scale = float(tok_rows * n_sp) ** (-0.5)
    proj_grad = summed_on_arrival(
        (contract_rows(input_grad, activ) * token_scale).astype(jnp.bfloat16), "sp", 0
    )
    act_grad = matmul(input_grad, proj_weight)
    norm_grad = act_grad * sig_norm * (1.0 + scaled * (1.0 - sig_norm)) * norm_gain[None, :]
    first, second = lax.psum(
        (jnp.sum(norm_grad, axis=1), jnp.sum(norm_grad * normed, axis=1)), "tp"
    )
    conv_grad = inv_std * (
        norm_grad - first[:, None] / channels - normed * (second[:, None] / channels)
    )
    reach = conv_taps.shape[0]
    rim = from_behind(conv_grad[: reach - 1].astype(jnp.bfloat16), "sp", -1).astype(jnp.float32)
    extended = jnp.concatenate([conv_grad, rim], axis=0)
    taps_float = conv_taps.astype(jnp.float32)
    mixed_grad = jnp.zeros_like(conv_grad)
    for lag in range(reach):
        mixed_grad = (
            mixed_grad + taps_float[reach - 1 - lag][None, :] * extended[lag : lag + tok_rows]
        )
    sig_gate = jax.nn.sigmoid(glu_gate.astype(jnp.float32))
    value_grad = (mixed_grad * sig_gate).astype(jnp.bfloat16)
    gate_side_grad = (
        mixed_grad * glu_value.astype(jnp.float32) * sig_gate * (1.0 - sig_gate)
    ).astype(jnp.bfloat16)
    return (
        input_grad,
        proj_grad,
        gate_g[None],
        up_g[None],
        down_g[None],
        value_grad,
        gate_side_grad,
    )


def solution(mesh):
    in_specs = (
        P("sp", None),
        P("sp", None),
        P("sp", None),
        P("sp", None),
        P("sp", "tp"),
        P("sp", "tp"),
        P("sp", "tp"),
        P(None, "tp"),
        P("tp"),
        P(None, "tp"),
        P("sp", None, "tp"),
        P("sp", None, "tp"),
        P("sp", "tp", None),
    )
    out_specs = (
        P("sp", None),
        P("sp", "tp"),
        P("sp", None, "tp"),
        P("sp", None, "tp"),
        P("sp", "tp", None),
        P("sp", "tp"),
        P("sp", "tp"),
    )
    return jax.shard_map(
        per_device, mesh=mesh, in_specs=in_specs, out_specs=out_specs, check_vma=False
    )
```

```python
import functools

import jax
import jax.numpy as jnp
from jax import lax
from jax.experimental import pallas as pl
from jax.experimental.pallas import tpu as pltpu
from jax.sharding import PartitionSpec as P

norm_eps = 1e-05
swap = [(0, 1), (1, 0)]


def in_blocks(shard, dim, count):
    before, after = (shard.shape[:dim], shard.shape[dim + 1 :])
    return jnp.moveaxis(shard.reshape(*before, count, -1, *after), dim, 0)


def summed_on_arrival(shard, axis, dim):
    parts = in_blocks(shard, dim, lax.axis_size(axis))
    arrived = lax.all_to_all(parts, axis, split_axis=0, concat_axis=0, tiled=True)
    return arrived.astype(jnp.float32).sum(axis=0)


def from_behind(shard, axis, by):
    count = lax.axis_size(axis)
    pairs = [(i, i + by) for i in range(count) if 0 <= i + by < count]
    return lax.ppermute(shard, axis, pairs)


def contract_rows(left, right):
    return lax.dot_general(
        left, right, (((0,), (0,)), ((), ())), preferred_element_type=jnp.float32
    )


def contract_cols(left, right):
    return lax.dot_general(
        left, right, (((1,), (1,)), ((), ())), preferred_element_type=jnp.float32
    )


def matmul(left, right):
    return jnp.dot(left, right, preferred_element_type=jnp.float32)


def iota(shape, dim):
    return lax.broadcasted_iota(jnp.int32, shape, dim)


def whole(shape):
    return pl.BlockSpec(shape, lambda *_: (0,) * len(shape))


smem = pl.BlockSpec(memory_space=pltpu.SMEM)


def slot_tables(routes_ref, experts):
    tokens = routes_ref.shape[1]
    row = iota((experts, tokens), 0)
    named = [routes_ref[k : k + 1, :] == row for k in range(2)]
    both = jnp.where(named[0] | named[1], 1.0, 0.0).astype(jnp.bfloat16)
    earlier = jnp.where(iota((tokens, tokens), 0) < iota((tokens, tokens), 1), 1.0, 0.0)
    slot = matmul(both, earlier.astype(jnp.bfloat16))
    return [jnp.where(n, slot, -1.0).astype(jnp.bfloat16) for n in named]


def pick_rows(tables, row_expert, row_slot):
    rows = row_slot.shape[0]
    experts = tables[0].shape[0]
    spread = jnp.where(row_expert == iota((rows, experts), 1), 1.0, 0.0).astype(jnp.bfloat16)
    return [matmul(spread, table) == row_slot.astype(jnp.float32) for table in tables]


def dispatch_body(
    tp_ref, routes_ref, weights_ref, input_ref, grad_ref, out_ref, pick_ref, scale_ref, half
):
    step = pl.program_id(0)
    blocks = pl.num_programs(0) // 2
    rows, tokens = out_ref.shape[0], routes_ref.shape[1]
    experts = rows // 8

    @pl.when(step == 0)
    def _():
        tables = slot_tables(routes_ref, experts)
        place = iota((rows, tokens), 0)
        within = place & 7
        slot = jnp.where(within < half, tp_ref[0] * half + within, -2)
        picks = pick_rows(tables, iota((rows, experts), 0) >> 3, slot)
        pick_ref[...] = jnp.where(picks[0] | picks[1], 1.0, 0.0).astype(jnp.bfloat16)
        chosen = [jnp.where(picks[k], weights_ref[k : k + 1, :], 0.0) for k in range(2)]
        scale_ref[...] = jnp.sum(chosen[0] + chosen[1], axis=1, keepdims=True)

    @pl.when(step < blocks)
    def _():
        out_ref[...] = matmul(pick_ref[...], input_ref[...]).astype(jnp.bfloat16)

    @pl.when(step >= blocks)
    def _():
        out_ref[...] = (matmul(pick_ref[...], grad_ref[...]) * scale_ref[...]).astype(jnp.bfloat16)


def dispatch(tp, routes, weights, moe_input, out_grad, experts, half):
    tokens, width = out_grad.shape
    rows = experts * 8
    blocks = 4
    wide = width // blocks
    return pl.pallas_call(
        functools.partial(dispatch_body, half=half),
        grid=(2 * blocks,),
        in_specs=[
            smem,
            whole(routes.shape),
            whole(weights.shape),
            pl.BlockSpec((tokens, wide), lambda i: (0, jnp.minimum(i, blocks - 1))),
            pl.BlockSpec((tokens, wide), lambda i: (0, jnp.maximum(i - blocks, 0))),
        ],
        out_specs=pl.BlockSpec((rows, wide), lambda i: (0, i)),
        out_shape=jax.ShapeDtypeStruct((rows, 2 * width), jnp.bfloat16),
        scratch_shapes=[
            pltpu.VMEM((rows, tokens), jnp.bfloat16),
            pltpu.VMEM((rows, 1), jnp.float32),
        ],
        compiler_params=pltpu.CompilerParams(vmem_limit_bytes=16 * 2**20),
        name="dispatch",
    )(tp, routes, weights, moe_input, out_grad)


def picks_body(tp_ref, routes_ref, out_ref, half):
    rows, tokens = out_ref.shape
    experts = rows // 16
    tables = slot_tables(routes_ref, experts)
    place = iota((rows, tokens), 0)
    within = place & 7
    side = (tp_ref[0] + ((place >> 3) & 1)) & 1
    slot = jnp.where(within < half, side * half + within, -2)
    picks = pick_rows(tables, iota((rows, experts), 0) >> 4, slot)
    out_ref[...] = jnp.where(picks[0] | picks[1], 1.0, 0.0).astype(jnp.bfloat16)


def return_picks(tp, routes, experts, half):
    shape = (experts * 16, routes.shape[1])
    return pl.pallas_call(
        functools.partial(picks_body, half=half),
        in_specs=[smem, whole(routes.shape)],
        out_specs=whole(shape),
        out_shape=jax.ShapeDtypeStruct(shape, jnp.bfloat16),
        compiler_params=pltpu.CompilerParams(vmem_limit_bytes=8 * 2**20),
        name="picks",
    )(tp, routes)


def proj_body(side_ref, grad_ref, activ_ref, *refs, scale):
    refs[-1][...] = (contract_rows(grad_ref[...], activ_ref[...]) * scale).astype(jnp.bfloat16)


def proj_part(side, grad, activ, scale, base):
    tokens, share = grad.shape
    units = activ.shape[1]
    blocks = 2
    wide = share // blocks
    extra = [] if base is None else [base]
    return pl.pallas_call(
        functools.partial(proj_body, scale=scale),
        grid_spec=pltpu.PrefetchScalarGridSpec(
            num_scalar_prefetch=1,
            grid=(blocks,),
            in_specs=[
                pl.BlockSpec((tokens, wide), lambda i, side: (0, i)),
                pl.BlockSpec((tokens, units), lambda i, side: (0, 0)),
            ]
            + [pl.BlockSpec(memory_space=pl.ANY)] * len(extra),
            out_specs=pl.BlockSpec((wide, units), lambda i, side: (side[0] * blocks + i, 0)),
        ),
        out_shape=pltpu.HBM((2 * share, units), jnp.bfloat16),
        input_output_aliases={} if base is None else {3: 0},
        compiler_params=pltpu.CompilerParams(vmem_limit_bytes=8 * 2**20),
        name="proj_here" if base is None else "proj_there",
    )(side, grad, activ, *extra)


def expert_body(tp_ref, rows_ref, gate_ref, up_ref, down_ref, hid_ref, gb_ref, ub_ref, pv_ref):
    width = gate_ref.shape[0]
    share = width // 2
    inputs = rows_ref[:, :width]
    gate_pre = matmul(inputs, gate_ref[...])
    up_pre = matmul(inputs, up_ref[...])
    sigma = jax.nn.sigmoid(gate_pre)
    silu_gate = gate_pre * sigma
    hid_ref[...] = (silu_gate * up_pre).astype(jnp.bfloat16)
    hidden_grad = contract_cols(rows_ref[:, width:], down_ref[...])
    gb_ref[...] = (hidden_grad * up_pre * sigma * (1.0 + gate_pre * (1.0 - sigma))).astype(
        jnp.bfloat16
    )
    ub_ref[...] = (hidden_grad * silu_gate).astype(jnp.bfloat16)
    away = pl.ds(pl.multiple_of((1 - tp_ref[0]) * share, share), share)
    pv_ref[...] = (
        contract_cols(gb_ref[...], gate_ref[away, :]) + contract_cols(ub_ref[...], up_ref[away, :])
    ).astype(jnp.bfloat16)


def expert(tp, rows, gate, up, down, name):
    count = rows.shape[0]
    width, units = gate.shape
    outs = [(count, units)] * 3 + [(count, width // 2)]
    return pl.pallas_call(
        expert_body,
        in_specs=[smem, whole(rows.shape), whole(gate.shape), whole(up.shape), whole(down.shape)],
        out_specs=[whole(s) for s in outs],
        out_shape=[jax.ShapeDtypeStruct(s, jnp.bfloat16) for s in outs],
        name=name,
        compiler_params=pltpu.CompilerParams(vmem_limit_bytes=26 * 2**20),
    )(tp, rows, gate, up, down)


def kept_body(tp_ref, gb0_ref, ub0_ref, gb1_ref, ub1_ref, gate_ref, up_ref, out0_ref, out1_ref):
    share = gate_ref.shape[0] // 2
    here = pl.ds(pl.multiple_of(tp_ref[0] * share, share), share)
    for gb_ref, ub_ref, out_ref in ((gb0_ref, ub0_ref, out0_ref), (gb1_ref, ub1_ref, out1_ref)):
        out_ref[...] = (
            contract_cols(gb_ref[...], gate_ref[here, :])
            + contract_cols(ub_ref[...], up_ref[here, :])
        ).astype(jnp.bfloat16)


def kept_partials(tp, gb0, ub0, gb1, ub1, gate, up):
    out = (gb0.shape[0], gate.shape[0] // 2)
    arrays = (gb0, ub0, gb1, ub1, gate, up)
    return pl.pallas_call(
        kept_body,
        in_specs=[smem] + [whole(a.shape) for a in arrays],
        out_specs=[whole(out)] * 2,
        out_shape=[jax.ShapeDtypeStruct(out, jnp.bfloat16)] * 2,
        name="kept",
        compiler_params=pltpu.CompilerParams(vmem_limit_bytes=16 * 2**20),
    )(tp, *arrays)


def total_body(kept0_ref, kept1_ref, came0_ref, came1_ref, out_ref):
    groups = out_ref.shape[0]
    for side, (kept_ref, came_ref) in enumerate(((kept0_ref, came0_ref), (kept1_ref, came1_ref))):
        total = kept_ref[...].astype(jnp.float32) + came_ref[...].astype(jnp.float32)
        out_ref[:, 8 * side : 8 * side + 8, :] = total.reshape(groups, 8, -1).astype(jnp.bfloat16)


def total_rows(kept0, kept1, came0, came1):
    rows, share = kept0.shape
    blocks = 4
    wide = share // blocks
    spec = pl.BlockSpec((rows, wide), lambda i: (0, i))
    return pl.pallas_call(
        total_body,
        grid=(blocks,),
        in_specs=[spec] * 4,
        out_specs=pl.BlockSpec((rows // 8, 16, wide), lambda i: (0, 0, i)),
        out_shape=pltpu.HBM((rows // 8, 16, share), jnp.bfloat16),
        name="total",
        compiler_params=pltpu.CompilerParams(vmem_limit_bytes=16 * 2**20),
    )(kept0, kept1, came0, came1)


def weights_body(
    in0_ref, in1_ref, gr0_ref, gr1_ref, hid0_ref, hid1_ref, gb0_ref, gb1_ref, ub0_ref, ub1_ref,
    gate_ref, up_ref, down_ref, scale,
):
    gate_ref[...] = (
        contract_rows(in0_ref[...], gb0_ref[...]) + contract_rows(in1_ref[...], gb1_ref[...])
    ) * scale
    up_ref[...] = (
        contract_rows(in0_ref[...], ub0_ref[...]) + contract_rows(in1_ref[...], ub1_ref[...])
    ) * scale
    down_ref[...] = (
        contract_rows(hid0_ref[...], gr0_ref[...]) + contract_rows(hid1_ref[...], gr1_ref[...])
    ) * scale


def weight_grads(rows0, rows1, own, other, scale):
    count, units = own[0].shape
    width = rows0.shape[1] // 2
    blocks = 8
    wide = width // blocks
    first = pl.BlockSpec((count, wide), lambda i: (0, i))
    second = pl.BlockSpec((count, wide), lambda i: (0, blocks + i))
    flops = 3 * 2 * 2 * count * width * units
    return pl.pallas_call(
        functools.partial(weights_body, scale=scale),
        grid=(blocks,),
        in_specs=[first, first, second, second] + [whole((count, units))] * 6,
        out_specs=[
            pl.BlockSpec((wide, units), lambda i: (i, 0)),
            pl.BlockSpec((wide, units), lambda i: (i, 0)),
            pl.BlockSpec((units, wide), lambda i: (0, i)),
        ],
        out_shape=[
            jax.ShapeDtypeStruct((width, units), jnp.float32),
            jax.ShapeDtypeStruct((width, units), jnp.float32),
            jax.ShapeDtypeStruct((units, width), jnp.float32),
        ],
        cost_estimate=pl.CostEstimate(
            flops=flops, bytes_accessed=12 * width * units, transcendentals=0
        ),
        name="weight_grads",
        compiler_params=pltpu.CompilerParams(vmem_limit_bytes=20 * 2**20),
    )(rows0, rows1, rows0, rows1, own[0], other[0], own[1], other[1], own[2], other[2])


def per_device(
    out_grad,
    moe_input,
    routes,
    route_weights,
    conv_result,
    glu_value,
    glu_gate,
    conv_taps,
    norm_gain,
    proj_weight,
    expert_gate,
    expert_up,
    expert_down,
):
    n_sp = lax.axis_size("sp")
    n_tp = lax.axis_size("tp")
    tok_rows, width = out_grad.shape
    top_count = routes.shape[1]
    capacity = 2 * top_count * tok_rows // n_sp
    half = capacity // n_tp
    slots = n_sp * capacity
    tp = lax.axis_index("tp")
    tp_array = tp.reshape(1).astype(jnp.int32)
    share = width // n_tp
    channels = conv_result.shape[1] * n_tp

    send = dispatch(tp_array, routes.T, route_weights.T, moe_input, out_grad, n_sp, half)
    rows0 = lax.all_to_all(
        send.reshape(n_sp, 8, 2 * width), "sp", split_axis=0, concat_axis=0, tiled=True
    ).reshape(n_sp * 8, 2 * width)
    rows1 = lax.ppermute(rows0, "tp", swap)

    gate, up, down = expert_gate[0], expert_up[0], expert_down[0]
    own = expert(tp_array, rows0, gate, up, down, "expert_own")
    other = expert(tp_array, rows1, gate, up, down, "expert_other")
    came1 = lax.ppermute(own[3], "tp", swap)
    came0 = lax.ppermute(other[3], "tp", swap)
    kept0, kept1 = kept_partials(tp_array, own[1], own[2], other[1], other[2], gate, up)
    summed = total_rows(kept0, kept1, came0, came1)
    returned = lax.all_to_all(summed, "sp", split_axis=0, concat_axis=0, tiled=True).reshape(
        n_sp * 16, share
    )
    gate_g, up_g, down_g = weight_grads(rows0, rows1, own, other, float(slots) ** (-0.5))

    values = conv_result.astype(jnp.float32)
    sums = lax.psum(
        (jnp.sum(values, axis=1), jnp.sum(values * values, axis=1)), "tp"
    )
    center = sums[0] / channels
    spread = sums[1] / channels - center * center
    inv_std = lax.rsqrt(spread + norm_eps)[:, None]
    normed = (values - center[:, None]) * inv_std
    scaled = normed * norm_gain[None, :]
    sig_norm = jax.nn.sigmoid(scaled)
    activ = (scaled * sig_norm).astype(jnp.bfloat16)

    picks = return_picks(tp_array, routes.T, n_sp, half)
    returned, activ, picks = lax.optimization_barrier((returned, activ, picks))
    grad_here = lax.dynamic_slice_in_dim(out_grad, tp * share, share, 1).astype(jnp.float32)
    here = (grad_here + contract_rows(picks, returned)).astype(jnp.bfloat16)
    there = lax.ppermute(here, "tp", swap)
    token_scale = float(tok_rows * n_sp) ** (-0.5)
    proj = proj_part(tp_array, here, activ, token_scale, None)
    proj = proj_part(1 - tp_array, there, activ, token_scale, proj)
    proj_grad = summed_on_arrival(proj, "sp", 0)
    here, there, conv_taps, _ = lax.optimization_barrier((here, there, conv_taps, proj))
    input_grad = jnp.where(
        tp == 0,
        jnp.concatenate([here, there], axis=1),
        jnp.concatenate([there, here], axis=1),
    )
    act_grad = matmul(input_grad, proj_weight)
    norm_grad = act_grad * sig_norm * (1.0 + scaled * (1.0 - sig_norm)) * norm_gain[None, :]
    first, second = lax.psum(
        (jnp.sum(norm_grad, axis=1), jnp.sum(norm_grad * normed, axis=1)), "tp"
    )
    conv_grad = inv_std * (
        norm_grad - first[:, None] / channels - normed * (second[:, None] / channels)
    )
    reach = conv_taps.shape[0]
    rim = from_behind(conv_grad[: reach - 1].astype(jnp.bfloat16), "sp", -1).astype(jnp.float32)
    extended = jnp.concatenate([conv_grad, rim], axis=0)
    taps_float = conv_taps.astype(jnp.float32)
    mixed_grad = jnp.zeros_like(conv_grad)
    for lag in range(reach):
        mixed_grad = (
            mixed_grad + taps_float[reach - 1 - lag][None, :] * extended[lag : lag + tok_rows]
        )
    sig_gate = jax.nn.sigmoid(glu_gate.astype(jnp.float32))
    value_grad = (mixed_grad * sig_gate).astype(jnp.bfloat16)
    gate_side_grad = (
        mixed_grad * glu_value.astype(jnp.float32) * sig_gate * (1.0 - sig_gate)
    ).astype(jnp.bfloat16)
    return (
        input_grad,
        proj_grad,
        gate_g[None],
        up_g[None],
        down_g[None],
        value_grad,
        gate_side_grad,
    )


def solution(mesh):
    in_specs = (
        P("sp", None),
        P("sp", None),
        P("sp", None),
        P("sp", None),
        P("sp", "tp"),
        P("sp", "tp"),
        P("sp", "tp"),
        P(None, "tp"),
        P("tp"),
        P(None, "tp"),
        P("sp", None, "tp"),
        P("sp", None, "tp"),
        P("sp", "tp", None),
    )
    out_specs = (
        P("sp", None),
        P("sp", "tp"),
        P("sp", None, "tp"),
        P("sp", None, "tp"),
        P("sp", "tp", None),
        P("sp", "tp"),
        P("sp", "tp"),
    )
    return jax.shard_map(
        per_device, mesh=mesh, in_specs=in_specs, out_specs=out_specs, check_vma=False
    )
```

```python
import functools

import jax
import jax.numpy as jnp
from jax import lax
from jax.experimental import pallas as pl
from jax.experimental.pallas import tpu as pltpu
from jax.sharding import PartitionSpec as P

norm_eps = 1e-05
swap = [(0, 1), (1, 0)]


def in_blocks(shard, dim, count):
    before, after = (shard.shape[:dim], shard.shape[dim + 1 :])
    return jnp.moveaxis(shard.reshape(*before, count, -1, *after), dim, 0)


def summed_on_arrival(shard, axis, dim):
    parts = in_blocks(shard, dim, lax.axis_size(axis))
    arrived = lax.all_to_all(parts, axis, split_axis=0, concat_axis=0, tiled=True)
    return arrived.astype(jnp.float32).sum(axis=0)


def from_behind(shard, axis, by):
    count = lax.axis_size(axis)
    pairs = [(i, i + by) for i in range(count) if 0 <= i + by < count]
    return lax.ppermute(shard, axis, pairs)


def contract_rows(left, right):
    return lax.dot_general(
        left, right, (((0,), (0,)), ((), ())), preferred_element_type=jnp.float32
    )


def contract_cols(left, right):
    return lax.dot_general(
        left, right, (((1,), (1,)), ((), ())), preferred_element_type=jnp.float32
    )


def matmul(left, right):
    return jnp.dot(left, right, preferred_element_type=jnp.float32)


def iota(shape, dim):
    return lax.broadcasted_iota(jnp.int32, shape, dim)


def whole(shape):
    return pl.BlockSpec(shape, lambda *_: (0,) * len(shape))


smem = pl.BlockSpec(memory_space=pltpu.SMEM)


def slot_tables(routes_ref, experts):
    tokens = routes_ref.shape[1]
    row = iota((experts, tokens), 0)
    named = [routes_ref[k : k + 1, :] == row for k in range(2)]
    both = jnp.where(named[0] | named[1], 1.0, 0.0).astype(jnp.bfloat16)
    earlier = jnp.where(iota((tokens, tokens), 0) < iota((tokens, tokens), 1), 1.0, 0.0)
    slot = matmul(both, earlier.astype(jnp.bfloat16))
    return [jnp.where(n, slot, -1.0).astype(jnp.bfloat16) for n in named]


def pick_rows(tables, row_expert, row_slot):
    rows = row_slot.shape[0]
    experts = tables[0].shape[0]
    spread = jnp.where(row_expert == iota((rows, experts), 1), 1.0, 0.0).astype(jnp.bfloat16)
    return [matmul(spread, table) == row_slot.astype(jnp.float32) for table in tables]


def dispatch_body(
    tp_ref, routes_any, weights_any, input_any, grad_any, out_any,
    routes_ref, weights_ref, input_ref, grad_ref, out_ref, sems, out_sems, half,
):
    pairs = (
        (routes_any, routes_ref),
        (weights_any, weights_ref),
        (input_any, input_ref),
        (grad_any, grad_ref),
    )
    copies = [pltpu.make_async_copy(a, b, sems.at[i]) for i, (a, b) in enumerate(pairs)]
    for copy in copies:
        copy.start()
    rows, tokens = out_ref.shape[0], routes_ref.shape[1]
    experts = rows // 8
    width = input_ref.shape[1]
    copies[0].wait()
    tables = slot_tables(routes_ref, experts)
    place = iota((rows, tokens), 0)
    within = place & 7
    slot = jnp.where(within < half, tp_ref[0] * half + within, -2)
    picks = pick_rows(tables, iota((rows, experts), 0) >> 3, slot)
    pick = jnp.where(picks[0] | picks[1], 1.0, 0.0).astype(jnp.bfloat16)
    copies[1].wait()
    chosen = [jnp.where(picks[k], weights_ref[k : k + 1, :], 0.0) for k in range(2)]
    scale = jnp.sum(chosen[0] + chosen[1], axis=1, keepdims=True)
    wide = width // 4
    leaving = []

    def put(start, block):
        columns = pl.ds(start, wide)
        out_ref[:, columns] = block.astype(jnp.bfloat16)
        copy = pltpu.make_async_copy(
            out_ref.at[:, columns], out_any.at[:, columns], out_sems.at[len(leaving)]
        )
        copy.start()
        leaving.append(copy)

    copies[2].wait()
    for i in range(4):
        put(i * wide, matmul(pick, input_ref[:, i * wide : (i + 1) * wide]))
    copies[3].wait()
    for i in range(4):
        put(width + i * wide, matmul(pick, grad_ref[:, i * wide : (i + 1) * wide]) * scale)
    for copy in leaving:
        copy.wait()


def dispatch(tp, routes, weights, moe_input, out_grad, experts, half):
    rows = experts * 8
    shape = (rows, 2 * out_grad.shape[1])
    arrays = (routes, weights, moe_input, out_grad)
    return pl.pallas_call(
        functools.partial(dispatch_body, half=half),
        in_specs=[smem] + [pl.BlockSpec(memory_space=pltpu.HBM)] * 4,
        out_specs=pl.BlockSpec(memory_space=pltpu.HBM),
        out_shape=pltpu.HBM(shape, jnp.bfloat16),
        scratch_shapes=[pltpu.VMEM(a.shape, a.dtype) for a in arrays]
        + [pltpu.VMEM(shape, jnp.bfloat16)]
        + [pltpu.SemaphoreType.DMA((4,)), pltpu.SemaphoreType.DMA((8,))],
        compiler_params=pltpu.CompilerParams(vmem_limit_bytes=58300000),
        name="dispatch",
    )(tp, *arrays)


def picks_body(tp_ref, routes_ref, out_ref, half):
    rows, tokens = out_ref.shape
    experts = rows // 16
    tables = slot_tables(routes_ref, experts)
    place = iota((rows, tokens), 0)
    within = place & 7
    side = (tp_ref[0] + ((place >> 3) & 1)) & 1
    slot = jnp.where(within < half, side * half + within, -2)
    picks = pick_rows(tables, iota((rows, experts), 0) >> 4, slot)
    out_ref[...] = jnp.where(picks[0] | picks[1], 1.0, 0.0).astype(jnp.bfloat16)


def return_picks(tp, routes, experts, half):
    shape = (experts * 16, routes.shape[1])
    return pl.pallas_call(
        functools.partial(picks_body, half=half),
        in_specs=[smem, whole(routes.shape)],
        out_specs=whole(shape),
        out_shape=jax.ShapeDtypeStruct(shape, jnp.bfloat16),
        compiler_params=pltpu.CompilerParams(vmem_limit_bytes=8 * 2**20),
        name="picks",
    )(tp, routes)


def proj_body(side_ref, grad_ref, activ_ref, *refs, scale):
    refs[-1][...] = (contract_rows(grad_ref[...], activ_ref[...]) * scale).astype(jnp.bfloat16)


def proj_part(side, grad, activ, scale, base):
    tokens, share = grad.shape
    units = activ.shape[1]
    blocks = 2
    wide = share // blocks
    extra = [] if base is None else [base]
    return pl.pallas_call(
        functools.partial(proj_body, scale=scale),
        grid_spec=pltpu.PrefetchScalarGridSpec(
            num_scalar_prefetch=1,
            grid=(blocks,),
            in_specs=[
                pl.BlockSpec((tokens, wide), lambda i, side: (0, i)),
                pl.BlockSpec((tokens, units), lambda i, side: (0, 0)),
            ]
            + [pl.BlockSpec(memory_space=pl.ANY)] * len(extra),
            out_specs=pl.BlockSpec((wide, units), lambda i, side: (side[0] * blocks + i, 0)),
        ),
        out_shape=pltpu.HBM((2 * share, units), jnp.bfloat16),
        input_output_aliases={} if base is None else {3: 0},
        compiler_params=pltpu.CompilerParams(vmem_limit_bytes=8 * 2**20),
        name="proj_here" if base is None else "proj_there",
    )(side, grad, activ, *extra)


def expert_body(tp_ref, rows_ref, gate_ref, up_ref, down_ref, hid_ref, gb_ref, ub_ref, pv_ref):
    width = gate_ref.shape[0]
    share = width // 2
    inputs = rows_ref[:, :width]
    gate_pre = matmul(inputs, gate_ref[...])
    up_pre = matmul(inputs, up_ref[...])
    sigma = jax.nn.sigmoid(gate_pre)
    silu_gate = gate_pre * sigma
    hid_ref[...] = (silu_gate * up_pre).astype(jnp.bfloat16)
    hidden_grad = contract_cols(rows_ref[:, width:], down_ref[...])
    gb_ref[...] = (hidden_grad * up_pre * sigma * (1.0 + gate_pre * (1.0 - sigma))).astype(
        jnp.bfloat16
    )
    ub_ref[...] = (hidden_grad * silu_gate).astype(jnp.bfloat16)
    away = pl.ds(pl.multiple_of((1 - tp_ref[0]) * share, share), share)
    pv_ref[...] = (
        contract_cols(gb_ref[...], gate_ref[away, :]) + contract_cols(ub_ref[...], up_ref[away, :])
    ).astype(jnp.bfloat16)


def expert(tp, rows, gate, up, down, name):
    count = rows.shape[0]
    width, units = gate.shape
    outs = [(count, units)] * 3 + [(count, width // 2)]
    return pl.pallas_call(
        expert_body,
        in_specs=[smem, whole(rows.shape), whole(gate.shape), whole(up.shape), whole(down.shape)],
        out_specs=[whole(s) for s in outs],
        out_shape=[jax.ShapeDtypeStruct(s, jnp.bfloat16) for s in outs],
        name=name,
        compiler_params=pltpu.CompilerParams(vmem_limit_bytes=26 * 2**20),
    )(tp, rows, gate, up, down)


def kept_body(tp_ref, gb0_ref, ub0_ref, gb1_ref, ub1_ref, gate_ref, up_ref, out0_ref, out1_ref):
    share = gate_ref.shape[0] // 2
    here = pl.ds(pl.multiple_of(tp_ref[0] * share, share), share)
    for gb_ref, ub_ref, out_ref in ((gb0_ref, ub0_ref, out0_ref), (gb1_ref, ub1_ref, out1_ref)):
        out_ref[...] = (
            contract_cols(gb_ref[...], gate_ref[here, :])
            + contract_cols(ub_ref[...], up_ref[here, :])
        ).astype(jnp.bfloat16)


def kept_partials(tp, gb0, ub0, gb1, ub1, gate, up):
    out = (gb0.shape[0], gate.shape[0] // 2)
    arrays = (gb0, ub0, gb1, ub1, gate, up)
    return pl.pallas_call(
        kept_body,
        in_specs=[smem] + [whole(a.shape) for a in arrays],
        out_specs=[whole(out)] * 2,
        out_shape=[jax.ShapeDtypeStruct(out, jnp.bfloat16)] * 2,
        name="kept",
        compiler_params=pltpu.CompilerParams(vmem_limit_bytes=16 * 2**20),
    )(tp, *arrays)


def total_body(kept0_ref, kept1_ref, came0_ref, came1_ref, out_ref):
    groups = out_ref.shape[0]
    for side, (kept_ref, came_ref) in enumerate(((kept0_ref, came0_ref), (kept1_ref, came1_ref))):
        total = kept_ref[...].astype(jnp.float32) + came_ref[...].astype(jnp.float32)
        out_ref[:, 8 * side : 8 * side + 8, :] = total.reshape(groups, 8, -1).astype(jnp.bfloat16)


def total_rows(kept0, kept1, came0, came1):
    rows, share = kept0.shape
    blocks = 4
    wide = share // blocks
    spec = pl.BlockSpec((rows, wide), lambda i: (0, i))
    return pl.pallas_call(
        total_body,
        grid=(blocks,),
        in_specs=[spec] * 4,
        out_specs=pl.BlockSpec((rows // 8, 16, wide), lambda i: (0, 0, i)),
        out_shape=pltpu.HBM((rows // 8, 16, share), jnp.bfloat16),
        name="total",
        compiler_params=pltpu.CompilerParams(vmem_limit_bytes=16 * 2**20),
    )(kept0, kept1, came0, came1)


def weights_body(
    in0_ref, in1_ref, gr0_ref, gr1_ref, hid0_ref, hid1_ref, gb0_ref, gb1_ref, ub0_ref, ub1_ref,
    gate_ref, up_ref, down_ref, scale,
):
    gate_ref[...] = (
        contract_rows(in0_ref[...], gb0_ref[...]) + contract_rows(in1_ref[...], gb1_ref[...])
    ) * scale
    up_ref[...] = (
        contract_rows(in0_ref[...], ub0_ref[...]) + contract_rows(in1_ref[...], ub1_ref[...])
    ) * scale
    down_ref[...] = (
        contract_rows(hid0_ref[...], gr0_ref[...]) + contract_rows(hid1_ref[...], gr1_ref[...])
    ) * scale


def weight_grads(rows0, rows1, own, other, scale):
    count, units = own[0].shape
    width = rows0.shape[1] // 2
    blocks = 8
    wide = width // blocks
    first = pl.BlockSpec((count, wide), lambda i: (0, i))
    second = pl.BlockSpec((count, wide), lambda i: (0, blocks + i))
    flops = 3 * 2 * 2 * count * width * units
    return pl.pallas_call(
        functools.partial(weights_body, scale=scale),
        grid=(blocks,),
        in_specs=[first, first, second, second] + [whole((count, units))] * 6,
        out_specs=[
            pl.BlockSpec((wide, units), lambda i: (i, 0)),
            pl.BlockSpec((wide, units), lambda i: (i, 0)),
            pl.BlockSpec((units, wide), lambda i: (0, i)),
        ],
        out_shape=[
            jax.ShapeDtypeStruct((width, units), jnp.float32),
            jax.ShapeDtypeStruct((width, units), jnp.float32),
            jax.ShapeDtypeStruct((units, width), jnp.float32),
        ],
        cost_estimate=pl.CostEstimate(
            flops=flops, bytes_accessed=12 * width * units, transcendentals=0
        ),
        name="weight_grads",
        compiler_params=pltpu.CompilerParams(vmem_limit_bytes=20 * 2**20),
    )(rows0, rows1, rows0, rows1, own[0], other[0], own[1], other[1], own[2], other[2])


def per_device(
    out_grad,
    moe_input,
    routes,
    route_weights,
    conv_result,
    glu_value,
    glu_gate,
    conv_taps,
    norm_gain,
    proj_weight,
    expert_gate,
    expert_up,
    expert_down,
):
    n_sp = lax.axis_size("sp")
    n_tp = lax.axis_size("tp")
    tok_rows, width = out_grad.shape
    top_count = routes.shape[1]
    capacity = 2 * top_count * tok_rows // n_sp
    half = capacity // n_tp
    slots = n_sp * capacity
    tp = lax.axis_index("tp")
    tp_array = tp.reshape(1).astype(jnp.int32)
    share = width // n_tp
    channels = conv_result.shape[1] * n_tp

    send = dispatch(tp_array, routes.T, route_weights.T, moe_input, out_grad, n_sp, half)
    rows0 = lax.all_to_all(
        send.reshape(n_sp, 8, 2 * width), "sp", split_axis=0, concat_axis=0, tiled=True
    ).reshape(n_sp * 8, 2 * width)
    rows1 = lax.ppermute(rows0, "tp", swap)

    gate, up, down = expert_gate[0], expert_up[0], expert_down[0]
    own = expert(tp_array, rows0, gate, up, down, "expert_own")
    other = expert(tp_array, rows1, gate, up, down, "expert_other")
    came1 = lax.ppermute(own[3], "tp", swap)
    came0 = lax.ppermute(other[3], "tp", swap)
    kept0, kept1 = kept_partials(tp_array, own[1], own[2], other[1], other[2], gate, up)
    summed = total_rows(kept0, kept1, came0, came1)
    returned = lax.all_to_all(summed, "sp", split_axis=0, concat_axis=0, tiled=True).reshape(
        n_sp * 16, share
    )
    gate_g, up_g, down_g = weight_grads(rows0, rows1, own, other, float(slots) ** (-0.5))

    values = conv_result.astype(jnp.float32)
    sums = lax.psum(
        (jnp.sum(values, axis=1), jnp.sum(values * values, axis=1)), "tp"
    )
    center = sums[0] / channels
    spread = sums[1] / channels - center * center
    inv_std = lax.rsqrt(spread + norm_eps)[:, None]
    normed = (values - center[:, None]) * inv_std
    scaled = normed * norm_gain[None, :]
    sig_norm = jax.nn.sigmoid(scaled)
    activ = (scaled * sig_norm).astype(jnp.bfloat16)

    picks = return_picks(tp_array, routes.T, n_sp, half)
    returned, activ, picks, gate_g, up_g, down_g = lax.optimization_barrier(
        (returned, activ, picks, gate_g, up_g, down_g)
    )
    grad_here = lax.dynamic_slice_in_dim(out_grad, tp * share, share, 1).astype(jnp.float32)
    here = (grad_here + contract_rows(picks, returned)).astype(jnp.bfloat16)
    there = lax.ppermute(here, "tp", swap)
    token_scale = float(tok_rows * n_sp) ** (-0.5)
    proj = proj_part(tp_array, here, activ, token_scale, None)
    proj = proj_part(1 - tp_array, there, activ, token_scale, proj)
    proj_grad = summed_on_arrival(proj, "sp", 0)
    here, there, conv_taps, _ = lax.optimization_barrier((here, there, conv_taps, proj))
    input_grad = jnp.where(
        tp == 0,
        jnp.concatenate([here, there], axis=1),
        jnp.concatenate([there, here], axis=1),
    )
    act_grad = matmul(input_grad, proj_weight)
    norm_grad = act_grad * sig_norm * (1.0 + scaled * (1.0 - sig_norm)) * norm_gain[None, :]
    first, second = lax.psum(
        (jnp.sum(norm_grad, axis=1), jnp.sum(norm_grad * normed, axis=1)), "tp"
    )
    conv_grad = inv_std * (
        norm_grad - first[:, None] / channels - normed * (second[:, None] / channels)
    )
    reach = conv_taps.shape[0]
    rim = from_behind(conv_grad[: reach - 1].astype(jnp.bfloat16), "sp", -1).astype(jnp.float32)
    extended = jnp.concatenate([conv_grad, rim], axis=0)
    taps_float = conv_taps.astype(jnp.float32)
    mixed_grad = jnp.zeros_like(conv_grad)
    for lag in range(reach):
        mixed_grad = (
            mixed_grad + taps_float[reach - 1 - lag][None, :] * extended[lag : lag + tok_rows]
        )
    sig_gate = jax.nn.sigmoid(glu_gate.astype(jnp.float32))
    value_grad = (mixed_grad * sig_gate).astype(jnp.bfloat16)
    gate_side_grad = (
        mixed_grad * glu_value.astype(jnp.float32) * sig_gate * (1.0 - sig_gate)
    ).astype(jnp.bfloat16)
    return (
        input_grad,
        proj_grad,
        gate_g[None],
        up_g[None],
        down_g[None],
        value_grad,
        gate_side_grad,
    )


def solution(mesh):
    in_specs = (
        P("sp", None),
        P("sp", None),
        P("sp", None),
        P("sp", None),
        P("sp", "tp"),
        P("sp", "tp"),
        P("sp", "tp"),
        P(None, "tp"),
        P("tp"),
        P(None, "tp"),
        P("sp", None, "tp"),
        P("sp", None, "tp"),
        P("sp", "tp", None),
    )
    out_specs = (
        P("sp", None),
        P("sp", "tp"),
        P("sp", None, "tp"),
        P("sp", None, "tp"),
        P("sp", "tp", None),
        P("sp", "tp"),
        P("sp", "tp"),
    )
    return jax.shard_map(
        per_device, mesh=mesh, in_specs=in_specs, out_specs=out_specs, check_vma=False
    )
```

```python
import functools

import jax
import jax.numpy as jnp
from jax import lax
from jax.experimental import pallas as pl
from jax.experimental.pallas import tpu as pltpu
from jax.sharding import PartitionSpec as P

norm_eps = 1e-05
swap = [(0, 1), (1, 0)]


def from_behind(shard, axis, by):
    count = lax.axis_size(axis)
    pairs = [(i, i + by) for i in range(count) if 0 <= i + by < count]
    return lax.ppermute(shard, axis, pairs)


def contract_rows(left, right):
    return lax.dot_general(
        left, right, (((0,), (0,)), ((), ())), preferred_element_type=jnp.float32
    )


def contract_cols(left, right):
    return lax.dot_general(
        left, right, (((1,), (1,)), ((), ())), preferred_element_type=jnp.float32
    )


def matmul(left, right):
    return jnp.dot(left, right, preferred_element_type=jnp.float32)


def iota(shape, dim):
    return lax.broadcasted_iota(jnp.int32, shape, dim)


def whole(shape):
    return pl.BlockSpec(shape, lambda *_: (0,) * len(shape))


smem = pl.BlockSpec(memory_space=pltpu.SMEM)


def slot_tables(routes_ref, experts):
    tokens = routes_ref.shape[1]
    row = iota((experts, tokens), 0)
    named = [routes_ref[k : k + 1, :] == row for k in range(2)]
    both = jnp.where(named[0] | named[1], 1.0, 0.0).astype(jnp.bfloat16)
    earlier = jnp.where(iota((tokens, tokens), 0) < iota((tokens, tokens), 1), 1.0, 0.0)
    slot = matmul(both, earlier.astype(jnp.bfloat16))
    return [jnp.where(n, slot, -1.0).astype(jnp.bfloat16) for n in named]


def pick_rows(tables, row_expert, row_slot):
    rows = row_slot.shape[0]
    experts = tables[0].shape[0]
    spread = jnp.where(row_expert == iota((rows, experts), 1), 1.0, 0.0).astype(jnp.bfloat16)
    return [matmul(spread, table) == row_slot.astype(jnp.float32) for table in tables]


def dispatch_body(
    tp_ref, routes_any, weights_any, input_any, grad_any, out_any,
    routes_ref, weights_ref, input_ref, grad_ref, out_ref, sems, out_sems, half,
):
    pairs = (
        (routes_any, routes_ref),
        (weights_any, weights_ref),
        (input_any, input_ref),
        (grad_any, grad_ref),
    )
    copies = [pltpu.make_async_copy(a, b, sems.at[i]) for i, (a, b) in enumerate(pairs)]
    for copy in copies:
        copy.start()
    rows, tokens = out_ref.shape[0], routes_ref.shape[1]
    experts = rows // 8
    width = input_ref.shape[1]
    copies[0].wait()
    tables = slot_tables(routes_ref, experts)
    place = iota((rows, tokens), 0)
    within = place & 7
    slot = jnp.where(within < half, tp_ref[0] * half + within, -2)
    picks = pick_rows(tables, iota((rows, experts), 0) >> 3, slot)
    pick = jnp.where(picks[0] | picks[1], 1.0, 0.0).astype(jnp.bfloat16)
    copies[1].wait()
    chosen = [jnp.where(picks[k], weights_ref[k : k + 1, :], 0.0) for k in range(2)]
    scale = jnp.sum(chosen[0] + chosen[1], axis=1, keepdims=True)
    wide = width // 4
    leaving = []

    def put(start, block):
        columns = pl.ds(start, wide)
        out_ref[:, columns] = block.astype(jnp.bfloat16)
        copy = pltpu.make_async_copy(
            out_ref.at[:, columns], out_any.at[:, columns], out_sems.at[len(leaving)]
        )
        copy.start()
        leaving.append(copy)

    copies[2].wait()
    for i in range(4):
        put(i * wide, matmul(pick, input_ref[:, i * wide : (i + 1) * wide]))
    copies[3].wait()
    for i in range(4):
        put(width + i * wide, matmul(pick, grad_ref[:, i * wide : (i + 1) * wide]) * scale)
    for copy in leaving:
        copy.wait()


def dispatch(tp, routes, weights, moe_input, out_grad, experts, half):
    rows = experts * 8
    shape = (rows, 2 * out_grad.shape[1])
    arrays = (routes, weights, moe_input, out_grad)
    return pl.pallas_call(
        functools.partial(dispatch_body, half=half),
        in_specs=[smem] + [pl.BlockSpec(memory_space=pltpu.HBM)] * 4,
        out_specs=pl.BlockSpec(memory_space=pltpu.HBM),
        out_shape=pltpu.HBM(shape, jnp.bfloat16),
        scratch_shapes=[pltpu.VMEM(a.shape, a.dtype) for a in arrays]
        + [pltpu.VMEM(shape, jnp.bfloat16)]
        + [pltpu.SemaphoreType.DMA((4,)), pltpu.SemaphoreType.DMA((8,))],
        compiler_params=pltpu.CompilerParams(vmem_limit_bytes=58300000),
        name="dispatch",
    )(tp, *arrays)


parcels = ((4, 0), (4, 1), (5, 1), (5, 2), (6, 2), (6, 3))


def picks_body(tp_ref, routes_ref, out_ref, half):
    tokens, rows = out_ref.shape[1:]
    experts = rows // 8
    tables = slot_tables(routes_ref, experts)
    spread = jnp.where(iota((experts, rows), 1) >> 3 == iota((experts, rows), 0), 1.0, 0.0)
    spread = spread.astype(jnp.bfloat16)
    found = [contract_rows(table, spread).astype(jnp.int32) for table in tables]
    within = iota((tokens, rows), 1) & 7
    near, far = tp_ref[0] * half, (1 - tp_ref[0]) * half
    slots = [jnp.where(within < half, near + within, far + half - 1)]
    for tile, chunk in parcels:
        rest = 8 * (tile - 4) + within - (half - 1) * chunk
        slots.append(jnp.where((rest >= 0) & (rest < half - 1), far + rest, -2))
    for index, slot in enumerate(slots):
        hit = (found[0] == slot) | (found[1] == slot)
        out_ref[index] = jnp.where(hit, 1.0, 0.0).astype(jnp.bfloat16)


def return_picks(tp, routes, experts, half):
    shape = (1 + len(parcels), routes.shape[1], experts * 8)
    return pl.pallas_call(
        functools.partial(picks_body, half=half),
        in_specs=[smem, whole(routes.shape)],
        out_specs=whole(shape),
        out_shape=jax.ShapeDtypeStruct(shape, jnp.bfloat16),
        compiler_params=pltpu.CompilerParams(vmem_limit_bytes=12 * 2**20),
        name="picks",
    )(tp, routes)


def combine_body(tp_ref, picks_ref, returned_any, grad_any, out_ref, tiles_ref, grad_ref, sems):
    groups, tiles, _, wide = returned_any.shape
    share = grad_ref.shape[1]
    columns = pl.ds(pl.multiple_of(tp_ref[0] * share, share), share)
    fetch = pltpu.make_async_copy(grad_any.at[:, columns], grad_ref, sems.at[tiles])
    fetch.start()
    copies = {}
    for tile in (0, 4, 1, 5, 2, 6, 3):
        copies[tile] = pltpu.make_async_copy(
            returned_any.at[:, tile], tiles_ref.at[tile], sems.at[tile]
        )
        copies[tile].start()
    fetch.wait()
    ready = {}

    def rows_of(tile):
        if tile not in ready:
            copies[tile].wait()
            ready[tile] = True
        return tiles_ref[tile].reshape(groups * 8, wide)

    for chunk in range(4):
        part = matmul(picks_ref[0], rows_of(chunk))
        for index, (tile, of) in enumerate(parcels):
            if of == chunk:
                part = part + matmul(picks_ref[1 + index], rows_of(tile))
        here = slice(chunk * wide, (chunk + 1) * wide)
        out_ref[:, here] = (grad_ref[:, here].astype(jnp.float32) + part).astype(jnp.bfloat16)


def combine(tp, picks, returned, out_grad):
    groups, tiles, _, wide = returned.shape
    shape = (out_grad.shape[0], 4 * wide)
    hbm = pl.BlockSpec(memory_space=pltpu.HBM)
    return pl.pallas_call(
        combine_body,
        in_specs=[smem, whole(picks.shape), hbm, hbm],
        out_specs=whole(shape),
        out_shape=jax.ShapeDtypeStruct(shape, jnp.bfloat16),
        scratch_shapes=[
            pltpu.VMEM((tiles, groups, 8, wide), jnp.bfloat16),
            pltpu.VMEM(shape, jnp.bfloat16),
            pltpu.SemaphoreType.DMA((tiles + 1,)),
        ],
        compiler_params=pltpu.CompilerParams(vmem_limit_bytes=12 * 2**20),
        name="combine",
    )(tp, picks, returned, out_grad)


def last_sum_body(parts_any, out_ref, parts_ref, sems):
    count, steps = parts_any.shape[0], sems.shape[0]
    each = count // steps
    spans = [pl.ds(i * each, each) for i in range(steps)]
    copies = [
        pltpu.make_async_copy(parts_any.at[span], parts_ref.at[span], sems.at[i])
        for i, span in enumerate(spans)
    ]
    for copy in copies:
        copy.start()
    total = jnp.zeros(out_ref.shape, jnp.float32)
    for i, copy in enumerate(copies):
        copy.wait()
        total = total + jnp.sum(parts_ref[spans[i]].astype(jnp.float32), axis=0)
    out_ref[...] = total


def last_sum(parts):
    shape = parts.shape[1:]
    return pl.pallas_call(
        last_sum_body,
        in_specs=[pl.BlockSpec(memory_space=pltpu.HBM)],
        out_specs=whole(shape),
        out_shape=jax.ShapeDtypeStruct(shape, jnp.float32),
        scratch_shapes=[pltpu.VMEM(parts.shape, parts.dtype), pltpu.SemaphoreType.DMA((8,))],
        compiler_params=pltpu.CompilerParams(vmem_limit_bytes=8 * 2**20),
        name="last_sum",
    )(parts)


def proj_body(side_ref, grad_ref, activ_ref, *refs, scale):
    refs[-1][...] = (contract_rows(grad_ref[...], activ_ref[...]) * scale).astype(jnp.bfloat16)


def proj_part(side, grad, activ, scale, base):
    tokens, share = grad.shape
    units = activ.shape[1]
    blocks = 2
    wide = share // blocks
    extra = [] if base is None else [base]
    return pl.pallas_call(
        functools.partial(proj_body, scale=scale),
        grid_spec=pltpu.PrefetchScalarGridSpec(
            num_scalar_prefetch=1,
            grid=(blocks,),
            in_specs=[
                pl.BlockSpec((tokens, wide), lambda i, side: (0, i)),
                pl.BlockSpec((tokens, units), lambda i, side: (0, 0)),
            ]
            + [pl.BlockSpec(memory_space=pl.ANY)] * len(extra),
            out_specs=pl.BlockSpec((wide, units), lambda i, side: (side[0] * blocks + i, 0)),
        ),
        out_shape=pltpu.HBM((2 * share, units), jnp.bfloat16),
        input_output_aliases={} if base is None else {3: 0},
        compiler_params=pltpu.CompilerParams(vmem_limit_bytes=8 * 2**20),
        name="proj_here" if base is None else "proj_there",
    )(side, grad, activ, *extra)


def expert_body(tp_ref, rows_ref, gate_ref, up_ref, down_ref, hid_ref, gb_ref, ub_ref, pv_ref):
    width = gate_ref.shape[0]
    share = width // 2
    inputs = rows_ref[:, :width]
    gate_pre = matmul(inputs, gate_ref[...])
    up_pre = matmul(inputs, up_ref[...])
    sigma = jax.nn.sigmoid(gate_pre)
    silu_gate = gate_pre * sigma
    hid_ref[...] = (silu_gate * up_pre).astype(jnp.bfloat16)
    hidden_grad = contract_cols(rows_ref[:, width:], down_ref[...])
    gb_ref[...] = (hidden_grad * up_pre * sigma * (1.0 + gate_pre * (1.0 - sigma))).astype(
        jnp.bfloat16
    )
    ub_ref[...] = (hidden_grad * silu_gate).astype(jnp.bfloat16)
    away = pl.ds(pl.multiple_of((1 - tp_ref[0]) * share, share), share)
    pv_ref[...] = (
        contract_cols(gb_ref[...], gate_ref[away, :]) + contract_cols(ub_ref[...], up_ref[away, :])
    ).astype(jnp.bfloat16)


def expert(tp, rows, gate, up, down, name):
    count = rows.shape[0]
    width, units = gate.shape
    outs = [(count, units)] * 3 + [(count, width // 2)]
    return pl.pallas_call(
        expert_body,
        in_specs=[smem, whole(rows.shape), whole(gate.shape), whole(up.shape), whole(down.shape)],
        out_specs=[whole(s) for s in outs],
        out_shape=[jax.ShapeDtypeStruct(s, jnp.bfloat16) for s in outs],
        name=name,
        compiler_params=pltpu.CompilerParams(vmem_limit_bytes=26 * 2**20),
    )(tp, rows, gate, up, down)


def kept_body(tp_ref, gb0_ref, ub0_ref, gb1_ref, ub1_ref, gate_ref, up_ref, out0_ref, out1_ref):
    share = gate_ref.shape[0] // 2
    here = pl.ds(pl.multiple_of(tp_ref[0] * share, share), share)
    for gb_ref, ub_ref, out_ref in ((gb0_ref, ub0_ref, out0_ref), (gb1_ref, ub1_ref, out1_ref)):
        out_ref[...] = (
            contract_cols(gb_ref[...], gate_ref[here, :])
            + contract_cols(ub_ref[...], up_ref[here, :])
        ).astype(jnp.bfloat16)


def kept_partials(tp, gb0, ub0, gb1, ub1, gate, up):
    out = (gb0.shape[0], gate.shape[0] // 2)
    arrays = (gb0, ub0, gb1, ub1, gate, up)
    return pl.pallas_call(
        kept_body,
        in_specs=[smem] + [whole(a.shape) for a in arrays],
        out_specs=[whole(out)] * 2,
        out_shape=[jax.ShapeDtypeStruct(out, jnp.bfloat16)] * 2,
        name="kept",
        compiler_params=pltpu.CompilerParams(vmem_limit_bytes=16 * 2**20),
    )(tp, *arrays)


def total_body(kept0_ref, kept1_ref, came0_ref, came1_ref, out_any, out_ref, sems, half):
    groups, tiles, _, wide = out_ref.shape
    within = iota((groups, 8, wide), 1)
    leaving = []

    def put(tile, value):
        out_ref[:, tile] = value.astype(jnp.bfloat16)
        copy = pltpu.make_async_copy(out_ref.at[:, tile], out_any.at[:, tile], sems.at[tile])
        copy.start()
        leaving.append(copy)

    def total(kept_ref, came_ref, chunk):
        here = slice(chunk * wide, (chunk + 1) * wide)
        value = kept_ref[:, here].astype(jnp.float32) + came_ref[:, here].astype(jnp.float32)
        return value.reshape(groups, 8, wide)

    before = None
    for chunk in range(4):
        far = total(kept1_ref, came1_ref, chunk)
        near = total(kept0_ref, came0_ref, chunk)
        put(chunk, jnp.where(within < half, near, pltpu.roll(far, 1, 1)))
        start = (half - 1) * chunk % 8
        moved = pltpu.roll(far, start, 1) if start else far
        if chunk:
            put(3 + chunk, jnp.where(within < start, before, moved))
        before = moved
    for copy in leaving:
        copy.wait()


def total_rows(kept0, kept1, came0, came1, half):
    rows, share = kept0.shape
    shape = (rows // 8, 7, 8, share // 4)
    return pl.pallas_call(
        functools.partial(total_body, half=half),
        in_specs=[whole((rows, share))] * 4,
        out_specs=pl.BlockSpec(memory_space=pltpu.HBM),
        out_shape=pltpu.HBM(shape, jnp.bfloat16),
        scratch_shapes=[pltpu.VMEM(shape, jnp.bfloat16), pltpu.SemaphoreType.DMA((7,))],
        compiler_params=pltpu.CompilerParams(vmem_limit_bytes=16 * 2**20),
        name="total",
    )(kept0, kept1, came0, came1)


def weights_body(
    in0_ref, in1_ref, gr0_ref, gr1_ref, hid0_ref, hid1_ref, gb0_ref, gb1_ref, ub0_ref, ub1_ref,
    gate_ref, up_ref, down_ref, scale,
):
    gate_ref[...] = (
        contract_rows(in0_ref[...], gb0_ref[...]) + contract_rows(in1_ref[...], gb1_ref[...])
    ) * scale
    up_ref[...] = (
        contract_rows(in0_ref[...], ub0_ref[...]) + contract_rows(in1_ref[...], ub1_ref[...])
    ) * scale
    down_ref[...] = (
        contract_rows(hid0_ref[...], gr0_ref[...]) + contract_rows(hid1_ref[...], gr1_ref[...])
    ) * scale


def weight_grads(rows0, rows1, own, other, scale):
    count, units = own[0].shape
    width = rows0.shape[1] // 2
    blocks = 8
    wide = width // blocks
    first = pl.BlockSpec((count, wide), lambda i: (0, i))
    second = pl.BlockSpec((count, wide), lambda i: (0, blocks + i))
    flops = 3 * 2 * 2 * count * width * units
    return pl.pallas_call(
        functools.partial(weights_body, scale=scale),
        grid=(blocks,),
        in_specs=[first, first, second, second] + [whole((count, units))] * 6,
        out_specs=[
            pl.BlockSpec((wide, units), lambda i: (i, 0)),
            pl.BlockSpec((wide, units), lambda i: (i, 0)),
            pl.BlockSpec((units, wide), lambda i: (0, i)),
        ],
        out_shape=[
            jax.ShapeDtypeStruct((width, units), jnp.float32),
            jax.ShapeDtypeStruct((width, units), jnp.float32),
            jax.ShapeDtypeStruct((units, width), jnp.float32),
        ],
        cost_estimate=pl.CostEstimate(
            flops=flops, bytes_accessed=12 * width * units, transcendentals=0
        ),
        name="weight_grads",
        compiler_params=pltpu.CompilerParams(vmem_limit_bytes=20 * 2**20),
    )(rows0, rows1, rows0, rows1, own[0], other[0], own[1], other[1], own[2], other[2])


def per_device(
    out_grad,
    moe_input,
    routes,
    route_weights,
    conv_result,
    glu_value,
    glu_gate,
    conv_taps,
    norm_gain,
    proj_weight,
    expert_gate,
    expert_up,
    expert_down,
):
    n_sp = lax.axis_size("sp")
    n_tp = lax.axis_size("tp")
    tok_rows, width = out_grad.shape
    top_count = routes.shape[1]
    capacity = 2 * top_count * tok_rows // n_sp
    half = capacity // n_tp
    slots = n_sp * capacity
    tp = lax.axis_index("tp")
    tp_array = tp.reshape(1).astype(jnp.int32)
    share = width // n_tp
    channels = conv_result.shape[1] * n_tp

    send = dispatch(tp_array, routes.T, route_weights.T, moe_input, out_grad, n_sp, half)
    rows0 = lax.all_to_all(
        send.reshape(n_sp, 8, 2 * width), "sp", split_axis=0, concat_axis=0, tiled=True
    ).reshape(n_sp * 8, 2 * width)
    rows1 = lax.ppermute(rows0, "tp", swap)

    gate, up, down = expert_gate[0], expert_up[0], expert_down[0]
    own = expert(tp_array, rows0, gate, up, down, "expert_own")
    other = expert(tp_array, rows1, gate, up, down, "expert_other")
    came1 = lax.ppermute(own[3], "tp", swap)
    came0 = lax.ppermute(other[3], "tp", swap)
    kept0, kept1 = kept_partials(tp_array, own[1], own[2], other[1], other[2], gate, up)
    summed = total_rows(kept0, kept1, came0, came1, half)
    returned = lax.all_to_all(
        summed.reshape(n_sp, 56, share // 4), "sp", split_axis=0, concat_axis=0, tiled=True
    ).reshape(summed.shape)
    gate_g, up_g, down_g = weight_grads(rows0, rows1, own, other, float(slots) ** (-0.5))

    values = conv_result.astype(jnp.float32)
    sums = lax.psum(
        (jnp.sum(values, axis=1), jnp.sum(values * values, axis=1)), "tp"
    )
    center = sums[0] / channels
    spread = sums[1] / channels - center * center
    inv_std = lax.rsqrt(spread + norm_eps)[:, None]
    normed = (values - center[:, None]) * inv_std
    scaled = normed * norm_gain[None, :]
    sig_norm = jax.nn.sigmoid(scaled)
    activ = (scaled * sig_norm).astype(jnp.bfloat16)

    picks = return_picks(tp_array, routes.T, n_sp, half)
    returned, activ, picks, gate_g, up_g, down_g = lax.optimization_barrier(
        (returned, activ, picks, gate_g, up_g, down_g)
    )
    here = combine(tp_array, picks, returned, out_grad)
    there = lax.ppermute(here, "tp", swap)
    token_scale = float(tok_rows * n_sp) ** (-0.5)
    proj = proj_part(tp_array, here, activ, token_scale, None)
    proj = proj_part(1 - tp_array, there, activ, token_scale, proj)
    proj_parts = proj.reshape(n_sp, width // n_sp, -1)
    proj_grad = last_sum(
        lax.all_to_all(proj_parts, "sp", split_axis=0, concat_axis=0, tiled=True)
    )
    here, there, conv_taps, _ = lax.optimization_barrier((here, there, conv_taps, proj))
    input_grad = jnp.where(
        tp == 0,
        jnp.concatenate([here, there], axis=1),
        jnp.concatenate([there, here], axis=1),
    )
    act_grad = matmul(input_grad, proj_weight)
    norm_grad = act_grad * sig_norm * (1.0 + scaled * (1.0 - sig_norm)) * norm_gain[None, :]
    first, second = lax.psum(
        (jnp.sum(norm_grad, axis=1), jnp.sum(norm_grad * normed, axis=1)), "tp"
    )
    conv_grad = inv_std * (
        norm_grad - first[:, None] / channels - normed * (second[:, None] / channels)
    )
    reach = conv_taps.shape[0]
    rim = from_behind(conv_grad[: reach - 1].astype(jnp.bfloat16), "sp", -1).astype(jnp.float32)
    extended = jnp.concatenate([conv_grad, rim], axis=0)
    taps_float = conv_taps.astype(jnp.float32)
    mixed_grad = jnp.zeros_like(conv_grad)
    for lag in range(reach):
        mixed_grad = (
            mixed_grad + taps_float[reach - 1 - lag][None, :] * extended[lag : lag + tok_rows]
        )
    sig_gate = jax.nn.sigmoid(glu_gate.astype(jnp.float32))
    value_grad = (mixed_grad * sig_gate).astype(jnp.bfloat16)
    gate_side_grad = (
        mixed_grad * glu_value.astype(jnp.float32) * sig_gate * (1.0 - sig_gate)
    ).astype(jnp.bfloat16)
    return (
        input_grad,
        proj_grad,
        gate_g[None],
        up_g[None],
        down_g[None],
        value_grad,
        gate_side_grad,
    )


def solution(mesh):
    in_specs = (
        P("sp", None),
        P("sp", None),
        P("sp", None),
        P("sp", None),
        P("sp", "tp"),
        P("sp", "tp"),
        P("sp", "tp"),
        P(None, "tp"),
        P("tp"),
        P(None, "tp"),
        P("sp", None, "tp"),
        P("sp", None, "tp"),
        P("sp", "tp", None),
    )
    out_specs = (
        P("sp", None),
        P("sp", "tp"),
        P("sp", None, "tp"),
        P("sp", None, "tp"),
        P("sp", "tp", None),
        P("sp", "tp"),
        P("sp", "tp"),
    )
    return jax.shard_map(
        per_device, mesh=mesh, in_specs=in_specs, out_specs=out_specs, check_vma=False
    )
```

```python
import functools

import jax
import jax.numpy as jnp
from jax import lax
from jax.experimental import pallas as pl
from jax.experimental.pallas import tpu as pltpu
from jax.sharding import PartitionSpec as P

norm_eps = 1e-05
swap = [(0, 1), (1, 0)]


def from_behind(shard, axis, by):
    count = lax.axis_size(axis)
    pairs = [(i, i + by) for i in range(count) if 0 <= i + by < count]
    return lax.ppermute(shard, axis, pairs)


def contract_rows(left, right):
    return lax.dot_general(
        left, right, (((0,), (0,)), ((), ())), preferred_element_type=jnp.float32
    )


def contract_cols(left, right):
    return lax.dot_general(
        left, right, (((1,), (1,)), ((), ())), preferred_element_type=jnp.float32
    )


def matmul(left, right):
    return jnp.dot(left, right, preferred_element_type=jnp.float32)


def iota(shape, dim):
    return lax.broadcasted_iota(jnp.int32, shape, dim)


def whole(shape):
    return pl.BlockSpec(shape, lambda *_: (0,) * len(shape))


smem = pl.BlockSpec(memory_space=pltpu.SMEM)


def slot_tables(routes_ref, experts):
    tokens = routes_ref.shape[1]
    row = iota((experts, tokens), 0)
    named = [routes_ref[k : k + 1, :] == row for k in range(2)]
    both = jnp.where(named[0] | named[1], 1.0, 0.0).astype(jnp.bfloat16)
    earlier = jnp.where(iota((tokens, tokens), 0) < iota((tokens, tokens), 1), 1.0, 0.0)
    slot = matmul(both, earlier.astype(jnp.bfloat16))
    return [jnp.where(n, slot, -1.0).astype(jnp.bfloat16) for n in named]


def pick_rows(tables, row_expert, row_slot):
    rows = row_slot.shape[0]
    experts = tables[0].shape[0]
    spread = jnp.where(row_expert == iota((rows, experts), 1), 1.0, 0.0).astype(jnp.bfloat16)
    return [matmul(spread, table) == row_slot.astype(jnp.float32) for table in tables]


def dispatch_body(
    tp_ref, routes_any, weights_any, input_any, grad_any, out_any,
    routes_ref, weights_ref, input_ref, grad_ref, out_ref, sems, out_sems, half,
):
    pairs = (
        (routes_any, routes_ref),
        (weights_any, weights_ref),
        (input_any, input_ref),
        (grad_any, grad_ref),
    )
    copies = [pltpu.make_async_copy(a, b, sems.at[i]) for i, (a, b) in enumerate(pairs)]
    for copy in copies:
        copy.start()
    rows, tokens = out_ref.shape[0], routes_ref.shape[1]
    experts = rows // 8
    width = input_ref.shape[1]
    copies[0].wait()
    tables = slot_tables(routes_ref, experts)
    place = iota((rows, tokens), 0)
    within = place & 7
    slot = jnp.where(within < half, tp_ref[0] * half + within, -2)
    picks = pick_rows(tables, iota((rows, experts), 0) >> 3, slot)
    pick = jnp.where(picks[0] | picks[1], 1.0, 0.0).astype(jnp.bfloat16)
    copies[1].wait()
    chosen = [jnp.where(picks[k], weights_ref[k : k + 1, :], 0.0) for k in range(2)]
    scale = jnp.sum(chosen[0] + chosen[1], axis=1, keepdims=True)
    wide = width // 4
    leaving = []

    def put(start, block):
        columns = pl.ds(start, wide)
        out_ref[:, columns] = block.astype(jnp.bfloat16)
        copy = pltpu.make_async_copy(
            out_ref.at[:, columns], out_any.at[:, columns], out_sems.at[len(leaving)]
        )
        copy.start()
        leaving.append(copy)

    copies[2].wait()
    for i in range(4):
        put(i * wide, matmul(pick, input_ref[:, i * wide : (i + 1) * wide]))
    copies[3].wait()
    for i in range(4):
        put(width + i * wide, matmul(pick, grad_ref[:, i * wide : (i + 1) * wide]) * scale)
    for copy in leaving:
        copy.wait()


def dispatch(tp, routes, weights, moe_input, out_grad, experts, half):
    rows = experts * 8
    shape = (rows, 2 * out_grad.shape[1])
    arrays = (routes, weights, moe_input, out_grad)
    return pl.pallas_call(
        functools.partial(dispatch_body, half=half),
        in_specs=[smem] + [pl.BlockSpec(memory_space=pltpu.HBM)] * 4,
        out_specs=pl.BlockSpec(memory_space=pltpu.HBM),
        out_shape=pltpu.HBM(shape, jnp.bfloat16),
        scratch_shapes=[pltpu.VMEM(a.shape, a.dtype) for a in arrays]
        + [pltpu.VMEM(shape, jnp.bfloat16)]
        + [pltpu.SemaphoreType.DMA((4,)), pltpu.SemaphoreType.DMA((8,))],
        compiler_params=pltpu.CompilerParams(vmem_limit_bytes=58300000),
        name="dispatch",
    )(tp, *arrays)


parcels = ((4, 0), (4, 1), (5, 1), (5, 2), (6, 2), (6, 3))


def return_picks(tp_ref, routes_ref, picks_ref, half):
    tokens, rows = picks_ref.shape[1:]
    experts = rows // 8
    tables = slot_tables(routes_ref, experts)
    spread = jnp.where(iota((experts, rows), 1) >> 3 == iota((experts, rows), 0), 1.0, 0.0)
    spread = spread.astype(jnp.bfloat16)
    found = [contract_rows(table, spread).astype(jnp.int32) for table in tables]
    within = iota((tokens, rows), 1) & 7
    near, far = tp_ref[0] * half, (1 - tp_ref[0]) * half
    slots = [jnp.where(within < half, near + within, far + half - 1)]
    for tile, chunk in parcels:
        rest = 8 * (tile - 4) + within - (half - 1) * chunk
        slots.append(jnp.where((rest >= 0) & (rest < half - 1), far + rest, -2))
    for index, slot in enumerate(slots):
        hit = (found[0] == slot) | (found[1] == slot)
        picks_ref[index] = jnp.where(hit, 1.0, 0.0).astype(jnp.bfloat16)


def combine_body(
    tp_ref, routes_any, returned_any, grad_any, out_ref,
    routes_ref, picks_ref, tiles_ref, grad_ref, sems, half,
):
    groups, tiles, _, wide = returned_any.shape
    share = grad_ref.shape[1]
    columns = pl.ds(pl.multiple_of(tp_ref[0] * share, share), share)
    pairs = ((routes_any, routes_ref), (grad_any.at[:, columns], grad_ref))
    copies = {}
    for index, (source, target) in enumerate(pairs):
        copies[tiles + index] = pltpu.make_async_copy(source, target, sems.at[tiles + index])
    for tile in (0, 4, 1, 5, 2, 6, 3):
        copies[tile] = pltpu.make_async_copy(
            returned_any.at[:, tile], tiles_ref.at[tile], sems.at[tile]
        )
    for copy in copies.values():
        copy.start()
    copies[tiles].wait()
    return_picks(tp_ref, routes_ref, picks_ref, half)
    copies[tiles + 1].wait()
    ready = {}

    def rows_of(tile):
        if tile not in ready:
            copies[tile].wait()
            ready[tile] = True
        return tiles_ref[tile].reshape(groups * 8, wide)

    for chunk in range(4):
        part = matmul(picks_ref[0], rows_of(chunk))
        for index, (tile, of) in enumerate(parcels):
            if of == chunk:
                part = part + matmul(picks_ref[1 + index], rows_of(tile))
        here = slice(chunk * wide, (chunk + 1) * wide)
        out_ref[:, here] = (grad_ref[:, here].astype(jnp.float32) + part).astype(jnp.bfloat16)


def combine(tp, routes, returned, out_grad, half):
    groups, tiles, _, wide = returned.shape
    tokens = out_grad.shape[0]
    shape = (tokens, 4 * wide)
    return pl.pallas_call(
        functools.partial(combine_body, half=half),
        in_specs=[smem] + [pl.BlockSpec(memory_space=pltpu.HBM)] * 3,
        out_specs=whole(shape),
        out_shape=jax.ShapeDtypeStruct(shape, jnp.bfloat16),
        scratch_shapes=[
            pltpu.VMEM(routes.shape, routes.dtype),
            pltpu.VMEM((1 + len(parcels), tokens, groups * 8), jnp.bfloat16),
            pltpu.VMEM((tiles, groups, 8, wide), jnp.bfloat16),
            pltpu.VMEM(shape, jnp.bfloat16),
            pltpu.SemaphoreType.DMA((tiles + 2,)),
        ],
        compiler_params=pltpu.CompilerParams(vmem_limit_bytes=16 * 2**20),
        name="combine",
    )(tp, routes, returned, out_grad)


def last_sum_body(parts_any, out_ref, parts_ref, sems):
    count, steps = parts_any.shape[0], sems.shape[0]
    each = count // steps
    spans = [pl.ds(i * each, each) for i in range(steps)]
    copies = [
        pltpu.make_async_copy(parts_any.at[span], parts_ref.at[span], sems.at[i])
        for i, span in enumerate(spans)
    ]
    for copy in copies:
        copy.start()
    total = jnp.zeros(out_ref.shape, jnp.float32)
    for i, copy in enumerate(copies):
        copy.wait()
        total = total + jnp.sum(parts_ref[spans[i]].astype(jnp.float32), axis=0)
    out_ref[...] = total


def last_sum(parts):
    shape = parts.shape[1:]
    return pl.pallas_call(
        last_sum_body,
        in_specs=[pl.BlockSpec(memory_space=pltpu.HBM)],
        out_specs=whole(shape),
        out_shape=jax.ShapeDtypeStruct(shape, jnp.float32),
        scratch_shapes=[pltpu.VMEM(parts.shape, parts.dtype), pltpu.SemaphoreType.DMA((8,))],
        compiler_params=pltpu.CompilerParams(vmem_limit_bytes=8 * 2**20),
        name="last_sum",
    )(parts)


def proj_body(side_ref, grad_ref, activ_ref, *refs, scale):
    refs[-1][...] = (contract_rows(grad_ref[...], activ_ref[...]) * scale).astype(jnp.bfloat16)


def proj_part(side, grad, activ, scale, base):
    tokens, share = grad.shape
    units = activ.shape[1]
    blocks = 2
    wide = share // blocks
    extra = [] if base is None else [base]

    def place(i, side):
        return ((side[0] if base is None else 1 - side[0]) * blocks + i, 0)

    return pl.pallas_call(
        functools.partial(proj_body, scale=scale),
        grid_spec=pltpu.PrefetchScalarGridSpec(
            num_scalar_prefetch=1,
            grid=(blocks,),
            in_specs=[
                pl.BlockSpec((tokens, wide), lambda i, side: (0, i)),
                pl.BlockSpec((tokens, units), lambda i, side: (0, 0)),
            ]
            + [pl.BlockSpec(memory_space=pl.ANY)] * len(extra),
            out_specs=pl.BlockSpec((wide, units), place),
        ),
        out_shape=pltpu.HBM((2 * share, units), jnp.bfloat16),
        input_output_aliases={} if base is None else {3: 0},
        compiler_params=pltpu.CompilerParams(vmem_limit_bytes=8 * 2**20),
        name="proj_here" if base is None else "proj_there",
    )(side, grad, activ, *extra)


def expert_body(
    tp_ref, rows_ref, gate_ref, up_ref, down_ref, hid_any, gb_ref, ub_ref, pv_ref, hid_ref, sem
):
    width = gate_ref.shape[0]
    share = width // 2
    inputs = rows_ref[:, :width]
    gate_pre = matmul(inputs, gate_ref[...])
    up_pre = matmul(inputs, up_ref[...])
    sigma = jax.nn.sigmoid(gate_pre)
    silu_gate = gate_pre * sigma
    hid_ref[...] = (silu_gate * up_pre).astype(jnp.bfloat16)
    leaving = pltpu.make_async_copy(hid_ref, hid_any, sem)
    leaving.start()
    hidden_grad = contract_cols(rows_ref[:, width:], down_ref[...])
    gb_ref[...] = (hidden_grad * up_pre * sigma * (1.0 + gate_pre * (1.0 - sigma))).astype(
        jnp.bfloat16
    )
    ub_ref[...] = (hidden_grad * silu_gate).astype(jnp.bfloat16)
    away = pl.ds(pl.multiple_of((1 - tp_ref[0]) * share, share), share)
    pv_ref[...] = (
        contract_cols(gb_ref[...], gate_ref[away, :]) + contract_cols(ub_ref[...], up_ref[away, :])
    ).astype(jnp.bfloat16)
    leaving.wait()


def expert(tp, rows, gate, up, down, name):
    count = rows.shape[0]
    width, units = gate.shape
    outs = [(count, units)] * 3 + [(count, width // 2)]
    return pl.pallas_call(
        expert_body,
        in_specs=[smem, whole(rows.shape), whole(gate.shape), whole(up.shape), whole(down.shape)],
        out_specs=[pl.BlockSpec(memory_space=pltpu.HBM)] + [whole(s) for s in outs[1:]],
        out_shape=[pltpu.HBM(outs[0], jnp.bfloat16)]
        + [jax.ShapeDtypeStruct(s, jnp.bfloat16) for s in outs[1:]],
        scratch_shapes=[pltpu.VMEM(outs[0], jnp.bfloat16), pltpu.SemaphoreType.DMA],
        name=name,
        compiler_params=pltpu.CompilerParams(vmem_limit_bytes=17 * 2**20),
    )(tp, rows, gate, up, down)


def kept_body(tp_ref, gb0_ref, ub0_ref, gb1_ref, ub1_ref, gate_ref, up_ref, out0_ref, out1_ref):
    share = gate_ref.shape[0] // 2
    here = pl.ds(pl.multiple_of(tp_ref[0] * share, share), share)
    for gb_ref, ub_ref, out_ref in ((gb0_ref, ub0_ref, out0_ref), (gb1_ref, ub1_ref, out1_ref)):
        out_ref[...] = (
            contract_cols(gb_ref[...], gate_ref[here, :])
            + contract_cols(ub_ref[...], up_ref[here, :])
        ).astype(jnp.bfloat16)


def kept_partials(tp, gb0, ub0, gb1, ub1, gate, up):
    out = (gb0.shape[0], gate.shape[0] // 2)
    arrays = (gb0, ub0, gb1, ub1, gate, up)
    return pl.pallas_call(
        kept_body,
        in_specs=[smem] + [whole(a.shape) for a in arrays],
        out_specs=[whole(out)] * 2,
        out_shape=[jax.ShapeDtypeStruct(out, jnp.bfloat16)] * 2,
        name="kept",
        compiler_params=pltpu.CompilerParams(vmem_limit_bytes=16 * 2**20),
    )(tp, *arrays)


def total_body(kept0_ref, kept1_ref, came0_ref, came1_ref, out_any, out_ref, sems, half):
    groups, tiles, _, wide = out_ref.shape
    within = iota((groups, 8, wide), 1)
    leaving = []

    def put(tile, value):
        out_ref[:, tile] = value.astype(jnp.bfloat16)
        copy = pltpu.make_async_copy(out_ref.at[:, tile], out_any.at[:, tile], sems.at[tile])
        copy.start()
        leaving.append(copy)

    def total(kept_ref, came_ref, chunk):
        here = slice(chunk * wide, (chunk + 1) * wide)
        value = kept_ref[:, here].astype(jnp.float32) + came_ref[:, here].astype(jnp.float32)
        return value.reshape(groups, 8, wide)

    before = None
    for chunk in range(4):
        far = total(kept1_ref, came1_ref, chunk)
        near = total(kept0_ref, came0_ref, chunk)
        put(chunk, jnp.where(within < half, near, pltpu.roll(far, 1, 1)))
        start = (half - 1) * chunk % 8
        moved = pltpu.roll(far, start, 1) if start else far
        if chunk:
            put(3 + chunk, jnp.where(within < start, before, moved))
        before = moved
    for copy in leaving:
        copy.wait()


def total_rows(kept0, kept1, came0, came1, half):
    rows, share = kept0.shape
    shape = (rows // 8, 7, 8, share // 4)
    return pl.pallas_call(
        functools.partial(total_body, half=half),
        in_specs=[whole((rows, share))] * 4,
        out_specs=pl.BlockSpec(memory_space=pltpu.HBM),
        out_shape=pltpu.HBM(shape, jnp.bfloat16),
        scratch_shapes=[pltpu.VMEM(shape, jnp.bfloat16), pltpu.SemaphoreType.DMA((7,))],
        compiler_params=pltpu.CompilerParams(vmem_limit_bytes=16 * 2**20),
        name="total",
    )(kept0, kept1, came0, came1)


def weights_body(
    in0_ref, in1_ref, gr0_ref, gr1_ref, hid0_ref, hid1_ref, gb0_ref, gb1_ref, ub0_ref, ub1_ref,
    gate_ref, up_ref, down_ref, scale,
):
    gate_ref[...] = (
        contract_rows(in0_ref[...], gb0_ref[...]) + contract_rows(in1_ref[...], gb1_ref[...])
    ) * scale
    up_ref[...] = (
        contract_rows(in0_ref[...], ub0_ref[...]) + contract_rows(in1_ref[...], ub1_ref[...])
    ) * scale
    down_ref[...] = (
        contract_rows(hid0_ref[...], gr0_ref[...]) + contract_rows(hid1_ref[...], gr1_ref[...])
    ) * scale


def weight_grads(rows0, rows1, own, other, scale):
    count, units = own[0].shape
    width = rows0.shape[1] // 2
    blocks = 8
    wide = width // blocks
    first = pl.BlockSpec((count, wide), lambda i: (0, i))
    second = pl.BlockSpec((count, wide), lambda i: (0, blocks + i))
    flops = 3 * 2 * 2 * count * width * units
    return pl.pallas_call(
        functools.partial(weights_body, scale=scale),
        grid=(blocks,),
        in_specs=[first, first, second, second] + [whole((count, units))] * 6,
        out_specs=[
            pl.BlockSpec((wide, units), lambda i: (i, 0)),
            pl.BlockSpec((wide, units), lambda i: (i, 0)),
            pl.BlockSpec((units, wide), lambda i: (0, i)),
        ],
        out_shape=[
            jax.ShapeDtypeStruct((width, units), jnp.float32),
            jax.ShapeDtypeStruct((width, units), jnp.float32),
            jax.ShapeDtypeStruct((units, width), jnp.float32),
        ],
        cost_estimate=pl.CostEstimate(
            flops=flops, bytes_accessed=12 * width * units, transcendentals=0
        ),
        name="weight_grads",
        compiler_params=pltpu.CompilerParams(vmem_limit_bytes=58300000),
    )(rows0, rows1, rows0, rows1, own[0], other[0], own[1], other[1], own[2], other[2])


def per_device(
    out_grad,
    moe_input,
    routes,
    route_weights,
    conv_result,
    glu_value,
    glu_gate,
    conv_taps,
    norm_gain,
    proj_weight,
    expert_gate,
    expert_up,
    expert_down,
):
    n_sp = lax.axis_size("sp")
    n_tp = lax.axis_size("tp")
    tok_rows, width = out_grad.shape
    top_count = routes.shape[1]
    capacity = 2 * top_count * tok_rows // n_sp
    half = capacity // n_tp
    slots = n_sp * capacity
    tp = lax.axis_index("tp")
    tp_array = tp.reshape(1).astype(jnp.int32)
    share = width // n_tp
    channels = conv_result.shape[1] * n_tp

    send = dispatch(tp_array, routes.T, route_weights.T, moe_input, out_grad, n_sp, half)
    rows0 = lax.all_to_all(
        send.reshape(n_sp, 8, 2 * width), "sp", split_axis=0, concat_axis=0, tiled=True
    ).reshape(n_sp * 8, 2 * width)
    rows1 = lax.ppermute(rows0, "tp", swap)

    gate, up, down = expert_gate[0], expert_up[0], expert_down[0]
    own = expert(tp_array, rows0, gate, up, down, "expert_own")
    other = expert(tp_array, rows1, gate, up, down, "expert_other")
    came1 = lax.ppermute(own[3], "tp", swap)
    came0 = lax.ppermute(other[3], "tp", swap)
    kept0, kept1 = kept_partials(tp_array, own[1], own[2], other[1], other[2], gate, up)
    summed = total_rows(kept0, kept1, came0, came1, half)
    returned = lax.all_to_all(
        summed.reshape(n_sp, 56, share // 4), "sp", split_axis=0, concat_axis=0, tiled=True
    ).reshape(summed.shape)
    gate_g, up_g, down_g = weight_grads(rows0, rows1, own, other, float(slots) ** (-0.5))

    conv_result, gate_g = lax.optimization_barrier((conv_result, gate_g))
    values = conv_result.astype(jnp.float32)
    sums = lax.psum(
        (jnp.sum(values, axis=1), jnp.sum(values * values, axis=1)), "tp"
    )
    center = sums[0] / channels
    spread = sums[1] / channels - center * center
    inv_std = lax.rsqrt(spread + norm_eps)[:, None]
    normed = (values - center[:, None]) * inv_std
    scaled = normed * norm_gain[None, :]
    sig_norm = jax.nn.sigmoid(scaled)
    activ = (scaled * sig_norm).astype(jnp.bfloat16)

    returned, activ, gate_g, up_g, down_g = lax.optimization_barrier(
        (returned, activ, gate_g, up_g, down_g)
    )
    here = combine(tp_array, routes.T, returned, out_grad, half)
    there = lax.ppermute(here, "tp", swap)
    token_scale = float(tok_rows * n_sp) ** (-0.5)
    proj = proj_part(tp_array, here, activ, token_scale, None)
    proj = proj_part(tp_array, there, activ, token_scale, proj)
    proj_parts = proj.reshape(n_sp, width // n_sp, -1)
    proj_grad = last_sum(
        lax.all_to_all(proj_parts, "sp", split_axis=0, concat_axis=0, tiled=True)
    )
    here, there, conv_taps, side, _ = lax.optimization_barrier(
        (here, there, conv_taps, tp_array, proj)
    )
    input_grad = jnp.where(
        side[0] == 0,
        jnp.concatenate([here, there], axis=1),
        jnp.concatenate([there, here], axis=1),
    )
    act_grad = matmul(input_grad, proj_weight)
    norm_grad = act_grad * sig_norm * (1.0 + scaled * (1.0 - sig_norm)) * norm_gain[None, :]
    first, second = lax.psum(
        (jnp.sum(norm_grad, axis=1), jnp.sum(norm_grad * normed, axis=1)), "tp"
    )
    conv_grad = inv_std * (
        norm_grad - first[:, None] / channels - normed * (second[:, None] / channels)
    )
    reach = conv_taps.shape[0]
    rim = from_behind(conv_grad[: reach - 1].astype(jnp.bfloat16), "sp", -1).astype(jnp.float32)
    extended = jnp.concatenate([conv_grad, rim], axis=0)
    taps_float = conv_taps.astype(jnp.float32)
    mixed_grad = jnp.zeros_like(conv_grad)
    for lag in range(reach):
        mixed_grad = (
            mixed_grad + taps_float[reach - 1 - lag][None, :] * extended[lag : lag + tok_rows]
        )
    sig_gate = jax.nn.sigmoid(glu_gate.astype(jnp.float32))
    value_grad = (mixed_grad * sig_gate).astype(jnp.bfloat16)
    gate_side_grad = (
        mixed_grad * glu_value.astype(jnp.float32) * sig_gate * (1.0 - sig_gate)
    ).astype(jnp.bfloat16)
    return (
        input_grad,
        proj_grad,
        gate_g[None],
        up_g[None],
        down_g[None],
        value_grad,
        gate_side_grad,
    )


def solution(mesh):
    in_specs = (
        P("sp", None),
        P("sp", None),
        P("sp", None),
        P("sp", None),
        P("sp", "tp"),
        P("sp", "tp"),
        P("sp", "tp"),
        P(None, "tp"),
        P("tp"),
        P(None, "tp"),
        P("sp", None, "tp"),
        P("sp", None, "tp"),
        P("sp", "tp", None),
    )
    out_specs = (
        P("sp", None),
        P("sp", "tp"),
        P("sp", None, "tp"),
        P("sp", None, "tp"),
        P("sp", "tp", None),
        P("sp", "tp"),
        P("sp", "tp"),
    )
    return jax.shard_map(
        per_device, mesh=mesh, in_specs=in_specs, out_specs=out_specs, check_vma=False
    )
```

```python
import functools

import jax
import jax.numpy as jnp
from jax import lax
from jax.experimental import pallas as pl
from jax.experimental.pallas import tpu as pltpu
from jax.sharding import PartitionSpec as P


norm_eps = 1e-05
swap = [(0, 1), (1, 0)]


def from_behind(shard, axis, by):
    count = lax.axis_size(axis)
    pairs = [(i, i + by) for i in range(count) if 0 <= i + by < count]
    return lax.ppermute(shard, axis, pairs)


def contract_rows(left, right):
    return lax.dot_general(
        left, right, (((0,), (0,)), ((), ())), preferred_element_type=jnp.float32
    )


def contract_cols(left, right):
    return lax.dot_general(
        left, right, (((1,), (1,)), ((), ())), preferred_element_type=jnp.float32
    )


def matmul(left, right):
    return jnp.dot(left, right, preferred_element_type=jnp.float32)


def iota(shape, dim):
    return lax.broadcasted_iota(jnp.int32, shape, dim)


def whole(shape):
    return pl.BlockSpec(shape, lambda *_: (0,) * len(shape))


smem = pl.BlockSpec(memory_space=pltpu.SMEM)


def slot_tables(routes_ref, experts):
    tokens = routes_ref.shape[1]
    row = iota((experts, tokens), 0)
    named = [routes_ref[k : k + 1, :] == row for k in range(2)]
    both = jnp.where(named[0] | named[1], 1.0, 0.0).astype(jnp.bfloat16)
    earlier = jnp.where(iota((tokens, tokens), 0) < iota((tokens, tokens), 1), 1.0, 0.0)
    slot = matmul(both, earlier.astype(jnp.bfloat16))
    return [jnp.where(n, slot, -1.0).astype(jnp.bfloat16) for n in named]


def pick_rows(tables, row_expert, row_slot):
    rows = row_slot.shape[0]
    experts = tables[0].shape[0]
    spread = jnp.where(row_expert == iota((rows, experts), 1), 1.0, 0.0).astype(jnp.bfloat16)
    return [matmul(spread, table) == row_slot.astype(jnp.float32) for table in tables]


def dispatch_body(
    tp_ref, routes_any, weights_any, input_any, grad_any, out_any,
    routes_ref, weights_ref, input_ref, grad_ref, out_ref, sems, out_sems, half,
):
    pairs = (
        (routes_any, routes_ref),
        (weights_any, weights_ref),
        (input_any, input_ref),
        (grad_any, grad_ref),
    )
    copies = [pltpu.make_async_copy(a, b, sems.at[i]) for i, (a, b) in enumerate(pairs)]
    for copy in copies:
        copy.start()
    rows, tokens = out_ref.shape[0], routes_ref.shape[1]
    experts = rows // 8
    width = input_ref.shape[1]
    copies[0].wait()
    tables = slot_tables(routes_ref, experts)
    place = iota((rows, tokens), 0)
    within = place & 7
    slot = jnp.where(within < half, tp_ref[0] * half + within, -2)
    picks = pick_rows(tables, iota((rows, experts), 0) >> 3, slot)
    pick = jnp.where(picks[0] | picks[1], 1.0, 0.0).astype(jnp.bfloat16)
    copies[1].wait()
    chosen = [jnp.where(picks[k], weights_ref[k : k + 1, :], 0.0) for k in range(2)]
    scale = jnp.sum(chosen[0] + chosen[1], axis=1, keepdims=True)
    wide = width // 4
    leaving = []

    def put(start, block):
        columns = pl.ds(start, wide)
        out_ref[:, columns] = block.astype(jnp.bfloat16)
        copy = pltpu.make_async_copy(
            out_ref.at[:, columns], out_any.at[:, columns], out_sems.at[len(leaving)]
        )
        copy.start()
        leaving.append(copy)

    copies[2].wait()
    for i in range(4):
        put(i * wide, matmul(pick, input_ref[:, i * wide : (i + 1) * wide]))
    copies[3].wait()
    for i in range(4):
        put(width + i * wide, matmul(pick, grad_ref[:, i * wide : (i + 1) * wide]) * scale)
    for copy in leaving:
        copy.wait()


def dispatch(tp, routes, weights, moe_input, out_grad, experts, half):
    rows = experts * 8
    shape = (rows, 2 * out_grad.shape[1])
    arrays = (routes, weights, moe_input, out_grad)
    return pl.pallas_call(
        functools.partial(dispatch_body, half=half),
        in_specs=[smem] + [pl.BlockSpec(memory_space=pltpu.HBM)] * 4,
        out_specs=pl.BlockSpec(memory_space=pltpu.HBM),
        out_shape=pltpu.HBM(shape, jnp.bfloat16),
        scratch_shapes=[pltpu.VMEM(a.shape, a.dtype) for a in arrays]
        + [pltpu.VMEM(shape, jnp.bfloat16)]
        + [pltpu.SemaphoreType.DMA((4,)), pltpu.SemaphoreType.DMA((8,))],
        compiler_params=pltpu.CompilerParams(vmem_limit_bytes=58300000),
        name="dispatch",
    )(tp, *arrays)


parcels = ((4, 0), (4, 1), (5, 1), (5, 2), (6, 2), (6, 3))


def return_picks(tp_ref, routes_ref, picks_ref, half):
    tokens, rows = picks_ref.shape[1:]
    experts = rows // 8
    tables = slot_tables(routes_ref, experts)
    spread = jnp.where(iota((experts, rows), 1) >> 3 == iota((experts, rows), 0), 1.0, 0.0)
    spread = spread.astype(jnp.bfloat16)
    found = [contract_rows(table, spread).astype(jnp.int32) for table in tables]
    within = iota((tokens, rows), 1) & 7
    near, far = tp_ref[0] * half, (1 - tp_ref[0]) * half
    slots = [jnp.where(within < half, near + within, far + half - 1)]
    for tile, chunk in parcels:
        rest = 8 * (tile - 4) + within - (half - 1) * chunk
        slots.append(jnp.where((rest >= 0) & (rest < half - 1), far + rest, -2))
    for index, slot in enumerate(slots):
        hit = (found[0] == slot) | (found[1] == slot)
        picks_ref[index] = jnp.where(hit, 1.0, 0.0).astype(jnp.bfloat16)


def combine_body(
    tp_ref, routes_any, returned_any, grad_any, out_ref,
    routes_ref, picks_ref, tiles_ref, grad_ref, sems, half,
):
    groups, tiles, _, wide = returned_any.shape
    share = grad_ref.shape[1]
    columns = pl.ds(pl.multiple_of(tp_ref[0] * share, share), share)
    pairs = ((routes_any, routes_ref), (grad_any.at[:, columns], grad_ref))
    copies = {}
    for index, (source, target) in enumerate(pairs):
        copies[tiles + index] = pltpu.make_async_copy(source, target, sems.at[tiles + index])
    for tile in (0, 4, 1, 5, 2, 6, 3):
        copies[tile] = pltpu.make_async_copy(
            returned_any.at[:, tile], tiles_ref.at[tile], sems.at[tile]
        )
    for copy in copies.values():
        copy.start()
    copies[tiles].wait()
    return_picks(tp_ref, routes_ref, picks_ref, half)
    copies[tiles + 1].wait()
    ready = {}

    def rows_of(tile):
        if tile not in ready:
            copies[tile].wait()
            ready[tile] = True
        return tiles_ref[tile].reshape(groups * 8, wide)

    for chunk in range(4):
        part = matmul(picks_ref[0], rows_of(chunk))
        for index, (tile, of) in enumerate(parcels):
            if of == chunk:
                part = part + matmul(picks_ref[1 + index], rows_of(tile))
        here = slice(chunk * wide, (chunk + 1) * wide)
        out_ref[:, here] = (grad_ref[:, here].astype(jnp.float32) + part).astype(jnp.bfloat16)


def combine(tp, routes, returned, out_grad, half):
    groups, tiles, _, wide = returned.shape
    tokens = out_grad.shape[0]
    shape = (tokens, 4 * wide)
    return pl.pallas_call(
        functools.partial(combine_body, half=half),
        in_specs=[smem] + [pl.BlockSpec(memory_space=pltpu.HBM)] * 3,
        out_specs=whole(shape),
        out_shape=jax.ShapeDtypeStruct(shape, jnp.bfloat16),
        scratch_shapes=[
            pltpu.VMEM(routes.shape, routes.dtype),
            pltpu.VMEM((1 + len(parcels), tokens, groups * 8), jnp.bfloat16),
            pltpu.VMEM((tiles, groups, 8, wide), jnp.bfloat16),
            pltpu.VMEM(shape, jnp.bfloat16),
            pltpu.SemaphoreType.DMA((tiles + 2,)),
        ],
        compiler_params=pltpu.CompilerParams(vmem_limit_bytes=16 * 2**20),
        name="combine",
    )(tp, routes, returned, out_grad)


def last_sum_body(parts_any, out_ref, parts_ref, sems):
    count, steps = parts_any.shape[0], sems.shape[0]
    each = count // steps
    spans = [pl.ds(i * each, each) for i in range(steps)]
    copies = [
        pltpu.make_async_copy(parts_any.at[span], parts_ref.at[span], sems.at[i])
        for i, span in enumerate(spans)
    ]
    for copy in copies:
        copy.start()
    total = jnp.zeros(out_ref.shape, jnp.float32)
    for i, copy in enumerate(copies):
        copy.wait()
        total = total + jnp.sum(parts_ref[spans[i]].astype(jnp.float32), axis=0)
    out_ref[...] = total


def last_sum(parts):
    shape = parts.shape[1:]
    return pl.pallas_call(
        last_sum_body,
        in_specs=[pl.BlockSpec(memory_space=pltpu.HBM)],
        out_specs=whole(shape),
        out_shape=jax.ShapeDtypeStruct(shape, jnp.float32),
        scratch_shapes=[pltpu.VMEM(parts.shape, parts.dtype), pltpu.SemaphoreType.DMA((8,))],
        compiler_params=pltpu.CompilerParams(vmem_limit_bytes=8 * 2**20),
        name="last_sum",
    )(parts)


def proj_body(side_ref, grad_ref, activ_ref, *refs, scale):
    refs[-1][...] = (contract_rows(grad_ref[...], activ_ref[...]) * scale).astype(jnp.bfloat16)


def proj_part(side, grad, activ, scale, base):
    tokens, share = grad.shape
    units = activ.shape[1]
    blocks = 2
    wide = share // blocks
    extra = [] if base is None else [base]

    def place(i, side):
        return ((side[0] if base is None else 1 - side[0]) * blocks + i, 0)

    return pl.pallas_call(
        functools.partial(proj_body, scale=scale),
        grid_spec=pltpu.PrefetchScalarGridSpec(
            num_scalar_prefetch=1,
            grid=(blocks,),
            in_specs=[
                pl.BlockSpec((tokens, wide), lambda i, side: (0, i)),
                pl.BlockSpec((tokens, units), lambda i, side: (0, 0)),
            ]
            + [pl.BlockSpec(memory_space=pl.ANY)] * len(extra),
            out_specs=pl.BlockSpec((wide, units), place),
        ),
        out_shape=pltpu.HBM((2 * share, units), jnp.bfloat16),
        input_output_aliases={} if base is None else {3: 0},
        compiler_params=pltpu.CompilerParams(vmem_limit_bytes=8 * 2**20),
        name="proj_here" if base is None else "proj_there",
    )(side, grad, activ, *extra)


def partial_rows(near, far, gate_near, up_near, gate_far, up_far):
    first = contract_cols(near[0], gate_near) + contract_cols(near[1], up_near)
    second = contract_cols(far[0], gate_far) + contract_cols(far[1], up_far)
    first = first.astype(jnp.bfloat16).astype(jnp.float32)
    second = second.astype(jnp.bfloat16).astype(jnp.float32)
    return (first + second).astype(jnp.bfloat16)


def expert_body(
    tp_ref, rows_any, gate0_ref, up0_ref, down0_ref, gate1_ref, up1_ref, down1_ref,
    hid_any, gb_ref, ub_ref, far_ref, pv_ref, rows_ref, hid_ref, sem, sems,
):
    width, units = gate0_ref.shape
    share = width // 2
    coming = []
    for index in range(4):
        columns = pl.ds(index * share, share)
        coming.append(
            pltpu.make_async_copy(rows_any.at[:, columns], rows_ref.at[:, columns], sems.at[index])
        )
    for copy in coming:
        copy.start()

    def rows_times(weight_ref, first):
        if first:
            coming[0].wait()
        part = matmul(rows_ref[:, :share], weight_ref[:share, :])
        if first:
            coming[1].wait()
        return part + matmul(rows_ref[:, share:width], weight_ref[share:, :])

    def side(gate_ref, up_ref, down_ref, first):
        gate_pre = rows_times(gate_ref, first)
        up_pre = rows_times(up_ref, False)
        sigma = jax.nn.sigmoid(gate_pre)
        silu_gate = gate_pre * sigma
        hidden = (silu_gate * up_pre).astype(jnp.bfloat16)
        if first:
            coming[2].wait()
            coming[3].wait()
        hidden_grad = contract_cols(rows_ref[:, width:], down_ref[...])
        gate_back = hidden_grad * up_pre * sigma * (1.0 + gate_pre * (1.0 - sigma))
        return hidden, gate_back.astype(jnp.bfloat16), (hidden_grad * silu_gate).astype(jnp.bfloat16)

    hid_ref[...], gb_ref[...], ub_ref[...] = side(gate0_ref, up0_ref, down0_ref, True)
    leaving = pltpu.make_async_copy(hid_ref, hid_any, sem)
    leaving.start()
    far = side(gate1_ref, up1_ref, down1_ref, False)
    for index in range(3):
        far_ref[:, index * units : (index + 1) * units] = far[index]
    away = pl.ds(pl.multiple_of((1 - tp_ref[0]) * share, share), share)
    pv_ref[...] = partial_rows(
        (gb_ref[...], ub_ref[...]),
        (far_ref[:, units : 2 * units], far_ref[:, 2 * units :]),
        gate0_ref[away, :],
        up0_ref[away, :],
        gate1_ref[away, :],
        up1_ref[away, :],
    )
    leaving.wait()


def expert(tp, rows, near, far):
    count = rows.shape[0]
    width, units = near[0].shape
    outs = [(count, units)] * 3 + [(count, 3 * units), (count, width // 2)]
    arrays = (rows, *near, *far)
    return pl.pallas_call(
        expert_body,
        in_specs=[smem, pl.BlockSpec(memory_space=pltpu.HBM)]
        + [whole(a.shape) for a in arrays[1:]],
        out_specs=[pl.BlockSpec(memory_space=pltpu.HBM)] + [whole(s) for s in outs[1:]],
        out_shape=[pltpu.HBM(outs[0], jnp.bfloat16)]
        + [jax.ShapeDtypeStruct(s, jnp.bfloat16) for s in outs[1:]],
        scratch_shapes=[
            pltpu.VMEM(rows.shape, rows.dtype),
            pltpu.VMEM(outs[0], jnp.bfloat16),
            pltpu.SemaphoreType.DMA,
            pltpu.SemaphoreType.DMA((4,)),
        ],
        compiler_params=pltpu.CompilerParams(vmem_limit_bytes=24 * 2**20),
        name="expert",
    )(tp, *arrays)


def kept_body(tp_ref, gb_ref, ub_ref, far_ref, gate0_ref, up0_ref, gate1_ref, up1_ref, out_ref):
    width, units = gate0_ref.shape
    share = width // 2
    here = pl.ds(pl.multiple_of(tp_ref[0] * share, share), share)
    out_ref[...] = partial_rows(
        (gb_ref[...], ub_ref[...]),
        (far_ref[:, units : 2 * units], far_ref[:, 2 * units :]),
        gate0_ref[here, :],
        up0_ref[here, :],
        gate1_ref[here, :],
        up1_ref[here, :],
    )


def kept_rows(tp, gb, ub, far, near_weights, far_weights):
    out = (gb.shape[0], near_weights[0].shape[0] // 2)
    arrays = (gb, ub, far, near_weights[0], near_weights[1], far_weights[0], far_weights[1])
    return pl.pallas_call(
        kept_body,
        in_specs=[smem] + [whole(a.shape) for a in arrays],
        out_specs=whole(out),
        out_shape=jax.ShapeDtypeStruct(out, jnp.bfloat16),
        compiler_params=pltpu.CompilerParams(vmem_limit_bytes=16 * 2**20),
        name="kept",
    )(tp, *arrays)


def total_body(near_ref, far_ref, out_any, out_ref, sems, half):
    groups, _, _, wide = out_ref.shape
    within = iota((groups, 8, wide), 1)
    leaving = []

    def put(tile, value):
        out_ref[:, tile] = value.astype(jnp.bfloat16)
        copy = pltpu.make_async_copy(out_ref.at[:, tile], out_any.at[:, tile], sems.at[tile])
        copy.start()
        leaving.append(copy)

    def rows_of(ref, chunk):
        value = ref[:, chunk * wide : (chunk + 1) * wide].astype(jnp.float32)
        return value.reshape(groups, 8, wide)

    before = None
    for chunk in range(4):
        far = rows_of(far_ref, chunk)
        near = rows_of(near_ref, chunk)
        put(chunk, jnp.where(within < half, near, pltpu.roll(far, 1, 1)))
        start = (half - 1) * chunk % 8
        moved = pltpu.roll(far, start, 1) if start else far
        if chunk:
            put(3 + chunk, jnp.where(within < start, before, moved))
        before = moved
    for copy in leaving:
        copy.wait()


def total_rows(near, far, half):
    rows, share = near.shape
    shape = (rows // 8, 7, 8, share // 4)
    return pl.pallas_call(
        functools.partial(total_body, half=half),
        in_specs=[whole((rows, share))] * 2,
        out_specs=pl.BlockSpec(memory_space=pltpu.HBM),
        out_shape=pltpu.HBM(shape, jnp.bfloat16),
        scratch_shapes=[pltpu.VMEM(shape, jnp.bfloat16), pltpu.SemaphoreType.DMA((7,))],
        compiler_params=pltpu.CompilerParams(vmem_limit_bytes=16 * 2**20),
        name="total",
    )(near, far)


def weights_body(
    in0_ref, in1_ref, gr0_ref, gr1_ref, hid0_ref, gb0_ref, ub0_ref, hid1_ref, gb1_ref, ub1_ref,
    gate_ref, up_ref, down_ref, scale,
):
    gate_ref[...] = (
        contract_rows(in0_ref[...], gb0_ref[...]) + contract_rows(in1_ref[...], gb1_ref[...])
    ) * scale
    up_ref[...] = (
        contract_rows(in0_ref[...], ub0_ref[...]) + contract_rows(in1_ref[...], ub1_ref[...])
    ) * scale
    down_ref[...] = (
        contract_rows(hid0_ref[...], gr0_ref[...]) + contract_rows(hid1_ref[...], gr1_ref[...])
    ) * scale


def weight_grads(rows0, rows1, own, other, scale):
    count, units = own[0].shape
    width = rows0.shape[1] // 2
    blocks = 8
    wide = width // blocks
    first = pl.BlockSpec((count, wide), lambda i: (0, i))
    second = pl.BlockSpec((count, wide), lambda i: (0, blocks + i))
    flops = 3 * 2 * 2 * count * width * units
    return pl.pallas_call(
        functools.partial(weights_body, scale=scale),
        grid=(blocks,),
        in_specs=[first, first, second, second]
        + [whole((count, units))] * 3
        + [pl.BlockSpec((count, units), lambda i, index=index: (0, index)) for index in range(3)],
        out_specs=[
            pl.BlockSpec((wide, units), lambda i: (i, 0)),
            pl.BlockSpec((wide, units), lambda i: (i, 0)),
            pl.BlockSpec((units, wide), lambda i: (0, i)),
        ],
        out_shape=[
            jax.ShapeDtypeStruct((width, units), jnp.float32),
            jax.ShapeDtypeStruct((width, units), jnp.float32),
            jax.ShapeDtypeStruct((units, width), jnp.float32),
        ],
        cost_estimate=pl.CostEstimate(
            flops=flops, bytes_accessed=12 * width * units, transcendentals=0
        ),
        name="weight_grads",
        compiler_params=pltpu.CompilerParams(vmem_limit_bytes=58300000),
    )(rows0, rows1, rows0, rows1, *own, other, other, other)


def per_device(
    out_grad,
    moe_input,
    routes,
    route_weights,
    conv_result,
    glu_value,
    glu_gate,
    conv_taps,
    norm_gain,
    proj_weight,
    expert_gate,
    expert_up,
    expert_down,
):
    n_sp = lax.axis_size("sp")
    n_tp = lax.axis_size("tp")
    tok_rows, width = out_grad.shape
    top_count = routes.shape[1]
    capacity = 2 * top_count * tok_rows // n_sp
    half = capacity // n_tp
    slots = n_sp * capacity
    tp = lax.axis_index("tp")
    tp_array = tp.reshape(1).astype(jnp.int32)
    share = width // n_tp
    channels = conv_result.shape[1] * n_tp

    send = dispatch(tp_array, routes.T, route_weights.T, moe_input, out_grad, n_sp, half)
    near_weights = (expert_gate[0], expert_up[0], expert_down[0])
    send, *sources = lax.optimization_barrier((send, *near_weights))
    far_weights = []
    for weight in sources:
        far_weights.append(lax.ppermute(weight, "tp", swap))
    rows0 = lax.all_to_all(
        send.reshape(n_sp, 8, 2 * width), "sp", split_axis=0, concat_axis=0, tiled=True
    )
    rows0 = rows0.reshape(n_sp * 8, 2 * width)
    rows1 = lax.ppermute(rows0, "tp", swap)

    *own, far, away = expert(tp_array, rows0, near_weights, far_weights)
    came = lax.ppermute(away, "tp", swap)
    other = lax.ppermute(far, "tp", swap)
    kept = kept_rows(tp_array, own[1], own[2], far, near_weights, far_weights)
    summed = total_rows(kept, came, half)
    returned = lax.all_to_all(
        summed.reshape(n_sp, 56, share // 4), "sp", split_axis=0, concat_axis=0, tiled=True
    ).reshape(summed.shape)
    gate_g, up_g, down_g = weight_grads(rows0, rows1, own, other, float(slots) ** (-0.5))

    conv_result, gate_g = lax.optimization_barrier((conv_result, gate_g))
    values = conv_result.astype(jnp.float32)
    sums = lax.psum(
        (jnp.sum(values, axis=1), jnp.sum(values * values, axis=1)), "tp"
    )
    center = sums[0] / channels
    spread = sums[1] / channels - center * center
    inv_std = lax.rsqrt(spread + norm_eps)[:, None]
    normed = (values - center[:, None]) * inv_std
    scaled = normed * norm_gain[None, :]
    sig_norm = jax.nn.sigmoid(scaled)
    activ = (scaled * sig_norm).astype(jnp.bfloat16)

    returned, activ, gate_g, up_g, down_g = lax.optimization_barrier(
        (returned, activ, gate_g, up_g, down_g)
    )
    here = combine(tp_array, routes.T, returned, out_grad, half)
    there = lax.ppermute(here, "tp", swap)
    token_scale = float(tok_rows * n_sp) ** (-0.5)
    proj = proj_part(tp_array, here, activ, token_scale, None)
    proj = proj_part(tp_array, there, activ, token_scale, proj)
    proj_parts = proj.reshape(n_sp, width // n_sp, -1)
    proj_grad = last_sum(
        lax.all_to_all(proj_parts, "sp", split_axis=0, concat_axis=0, tiled=True)
    )
    here, there, conv_taps, side, _ = lax.optimization_barrier(
        (here, there, conv_taps, tp_array, proj)
    )
    input_grad = jnp.where(
        side[0] == 0,
        jnp.concatenate([here, there], axis=1),
        jnp.concatenate([there, here], axis=1),
    )
    act_grad = matmul(input_grad, proj_weight)
    norm_grad = act_grad * sig_norm * (1.0 + scaled * (1.0 - sig_norm)) * norm_gain[None, :]
    first, second = lax.psum(
        (jnp.sum(norm_grad, axis=1), jnp.sum(norm_grad * normed, axis=1)), "tp"
    )
    conv_grad = inv_std * (
        norm_grad - first[:, None] / channels - normed * (second[:, None] / channels)
    )
    reach = conv_taps.shape[0]
    rim = from_behind(conv_grad[: reach - 1].astype(jnp.bfloat16), "sp", -1).astype(jnp.float32)
    extended = jnp.concatenate([conv_grad, rim], axis=0)
    taps_float = conv_taps.astype(jnp.float32)
    mixed_grad = jnp.zeros_like(conv_grad)
    for lag in range(reach):
        mixed_grad = (
            mixed_grad + taps_float[reach - 1 - lag][None, :] * extended[lag : lag + tok_rows]
        )
    sig_gate = jax.nn.sigmoid(glu_gate.astype(jnp.float32))
    value_grad = (mixed_grad * sig_gate).astype(jnp.bfloat16)
    gate_side_grad = (
        mixed_grad * glu_value.astype(jnp.float32) * sig_gate * (1.0 - sig_gate)
    ).astype(jnp.bfloat16)
    return (
        input_grad,
        proj_grad,
        gate_g[None],
        up_g[None],
        down_g[None],
        value_grad,
        gate_side_grad,
    )


def solution(mesh):
    in_specs = (
        P("sp", None),
        P("sp", None),
        P("sp", None),
        P("sp", None),
        P("sp", "tp"),
        P("sp", "tp"),
        P("sp", "tp"),
        P(None, "tp"),
        P("tp"),
        P(None, "tp"),
        P("sp", None, "tp"),
        P("sp", None, "tp"),
        P("sp", "tp", None),
    )
    out_specs = (
        P("sp", None),
        P("sp", "tp"),
        P("sp", None, "tp"),
        P("sp", None, "tp"),
        P("sp", "tp", None),
        P("sp", "tp"),
        P("sp", "tp"),
    )
    return jax.shard_map(
        per_device, mesh=mesh, in_specs=in_specs, out_specs=out_specs, check_vma=False
    )
```

```python
import functools

import jax
import jax.numpy as jnp
from jax import lax
from jax.experimental import pallas as pl
from jax.experimental.pallas import tpu as pltpu
from jax.sharding import PartitionSpec as P

norm_eps = 1e-05
swap = [(0, 1), (1, 0)]


def from_behind(shard, axis, by):
    count = lax.axis_size(axis)
    pairs = [(i, i + by) for i in range(count) if 0 <= i + by < count]
    return lax.ppermute(shard, axis, pairs)


def contract_rows(left, right):
    return lax.dot_general(
        left, right, (((0,), (0,)), ((), ())), preferred_element_type=jnp.float32
    )


def contract_cols(left, right):
    return lax.dot_general(
        left, right, (((1,), (1,)), ((), ())), preferred_element_type=jnp.float32
    )


def matmul(left, right):
    return jnp.dot(left, right, preferred_element_type=jnp.float32)


def iota(shape, dim):
    return lax.broadcasted_iota(jnp.int32, shape, dim)


def whole(shape):
    return pl.BlockSpec(shape, lambda *_: (0,) * len(shape))


smem = pl.BlockSpec(memory_space=pltpu.SMEM)


def slot_tables(routes_ref, experts):
    tokens = routes_ref.shape[1]
    row = iota((experts, tokens), 0)
    named = [routes_ref[k : k + 1, :] == row for k in range(2)]
    both = jnp.where(named[0] | named[1], 1.0, 0.0).astype(jnp.bfloat16)
    earlier = jnp.where(iota((tokens, tokens), 0) < iota((tokens, tokens), 1), 1.0, 0.0)
    slot = matmul(both, earlier.astype(jnp.bfloat16))
    return [jnp.where(n, slot, -1.0).astype(jnp.bfloat16) for n in named]


def pick_rows(tables, row_expert, row_slot):
    rows = row_slot.shape[0]
    experts = tables[0].shape[0]
    spread = jnp.where(row_expert == iota((rows, experts), 1), 1.0, 0.0).astype(jnp.bfloat16)
    return [matmul(spread, table) == row_slot.astype(jnp.float32) for table in tables]


def dispatch_body(
    tp_ref, routes_any, weights_any, grad_any, input_any, out_any,
    routes_ref, weights_ref, grad_ref, input_ref, out_ref, sems, out_sems, half,
):
    pairs = (
        (routes_any, routes_ref),
        (weights_any, weights_ref),
        (grad_any, grad_ref),
        (input_any, input_ref),
    )
    copies = [pltpu.make_async_copy(a, b, sems.at[i]) for i, (a, b) in enumerate(pairs)]
    for copy in copies:
        copy.start()
    experts, tokens = out_ref.shape[0], routes_ref.shape[1]
    rows = experts * 8
    width = input_ref.shape[1]
    copies[0].wait()
    tables = slot_tables(routes_ref, experts)
    place = iota((rows, tokens), 0)
    within = place & 7
    slot = jnp.where(within < half, tp_ref[0] * half + within, -2)
    picks = pick_rows(tables, iota((rows, experts), 0) >> 3, slot)
    pick = jnp.where(picks[0] | picks[1], 1.0, 0.0).astype(jnp.bfloat16)
    copies[1].wait()
    chosen = [jnp.where(picks[k], weights_ref[k : k + 1, :], 0.0) for k in range(2)]
    scale = jnp.sum(chosen[0] + chosen[1], axis=1, keepdims=True)
    tiles, wide = out_ref.shape[1], out_ref.shape[3]
    last = width // wide - 1
    within = iota((experts, 8, wide), 1)
    leaving = []

    def chunk_of(ref, index):
        return matmul(pick, ref[:, index * wide : (index + 1) * wide])

    copies[2].wait()
    extra = (chunk_of(grad_ref, last) * scale).reshape(experts, 8, wide)

    def put(tile, value):
        value = value.reshape(experts, 8, wide)
        value = jnp.where(within < half, value, pltpu.roll(extra, half - tile, 1))
        out_ref[:, tile] = value.astype(jnp.bfloat16)
        copy = pltpu.make_async_copy(
            out_ref.at[:, tile], out_any.at[:, tile], out_sems.at[tile]
        )
        copy.start()
        leaving.append(copy)

    for index in range(last):
        put(last + 1 + index, chunk_of(grad_ref, index) * scale)
    copies[3].wait()
    for index in range(last + 1):
        put(index, chunk_of(input_ref, index))
    for copy in leaving:
        copy.wait()


def dispatch(tp, routes, weights, moe_input, out_grad, experts, half):
    shape = (experts, half, 8, 2 * out_grad.shape[1] // 8)
    arrays = (routes, weights, out_grad, moe_input)
    return pl.pallas_call(
        functools.partial(dispatch_body, half=half),
        in_specs=[smem] + [pl.BlockSpec(memory_space=pltpu.HBM)] * 4,
        out_specs=pl.BlockSpec(memory_space=pltpu.HBM),
        out_shape=pltpu.HBM(shape, jnp.bfloat16),
        scratch_shapes=[pltpu.VMEM(a.shape, a.dtype) for a in arrays]
        + [pltpu.VMEM(shape, jnp.bfloat16)]
        + [pltpu.SemaphoreType.DMA((4,)), pltpu.SemaphoreType.DMA((half,))],
        compiler_params=pltpu.CompilerParams(vmem_limit_bytes=58300000),
        name="dispatch",
    )(tp, *arrays)


parcels = ((4, 0), (4, 1), (5, 1), (5, 2), (6, 2), (6, 3))


def return_picks(tp_ref, routes_ref, picks_ref, half):
    tokens, rows = picks_ref.shape[1:]
    experts = rows // 8
    tables = slot_tables(routes_ref, experts)
    spread = jnp.where(iota((experts, rows), 1) >> 3 == iota((experts, rows), 0), 1.0, 0.0)
    spread = spread.astype(jnp.bfloat16)
    found = [contract_rows(table, spread).astype(jnp.int32) for table in tables]
    within = iota((tokens, rows), 1) & 7
    near, far = tp_ref[0] * half, (1 - tp_ref[0]) * half
    slots = [jnp.where(within < half, near + within, far + half - 1)]
    for tile, chunk in parcels:
        rest = 8 * (tile - 4) + within - (half - 1) * chunk
        slots.append(jnp.where((rest >= 0) & (rest < half - 1), far + rest, -2))
    for index, slot in enumerate(slots):
        hit = (found[0] == slot) | (found[1] == slot)
        picks_ref[index] = jnp.where(hit, 1.0, 0.0).astype(jnp.bfloat16)


def combine_body(
    tp_ref, routes_any, returned_any, grad_any, out_ref,
    routes_ref, picks_ref, tiles_ref, grad_ref, sems, half,
):
    groups, tiles, _, wide = returned_any.shape
    share = grad_ref.shape[1]
    columns = pl.ds(pl.multiple_of(tp_ref[0] * share, share), share)
    pairs = ((routes_any, routes_ref), (grad_any.at[:, columns], grad_ref))
    copies = {}
    for index, (source, target) in enumerate(pairs):
        copies[tiles + index] = pltpu.make_async_copy(source, target, sems.at[tiles + index])
    for tile in (0, 4, 1, 5, 2, 6, 3):
        copies[tile] = pltpu.make_async_copy(
            returned_any.at[:, tile], tiles_ref.at[tile], sems.at[tile]
        )
    for copy in copies.values():
        copy.start()
    copies[tiles].wait()
    return_picks(tp_ref, routes_ref, picks_ref, half)
    copies[tiles + 1].wait()
    ready = {}

    def rows_of(tile):
        if tile not in ready:
            copies[tile].wait()
            ready[tile] = True
        return tiles_ref[tile].reshape(groups * 8, wide)

    for chunk in range(4):
        part = matmul(picks_ref[0], rows_of(chunk))
        for index, (tile, of) in enumerate(parcels):
            if of == chunk:
                part = part + matmul(picks_ref[1 + index], rows_of(tile))
        here = slice(chunk * wide, (chunk + 1) * wide)
        out_ref[:, here] = (grad_ref[:, here].astype(jnp.float32) + part).astype(jnp.bfloat16)


def combine(tp, routes, returned, out_grad, half):
    groups, tiles, _, wide = returned.shape
    tokens = out_grad.shape[0]
    shape = (tokens, 4 * wide)
    return pl.pallas_call(
        functools.partial(combine_body, half=half),
        in_specs=[smem] + [pl.BlockSpec(memory_space=pltpu.HBM)] * 3,
        out_specs=whole(shape),
        out_shape=jax.ShapeDtypeStruct(shape, jnp.bfloat16),
        scratch_shapes=[
            pltpu.VMEM(routes.shape, routes.dtype),
            pltpu.VMEM((1 + len(parcels), tokens, groups * 8), jnp.bfloat16),
            pltpu.VMEM((tiles, groups, 8, wide), jnp.bfloat16),
            pltpu.VMEM(shape, jnp.bfloat16),
            pltpu.SemaphoreType.DMA((tiles + 2,)),
        ],
        compiler_params=pltpu.CompilerParams(vmem_limit_bytes=16 * 2**20),
        name="combine",
    )(tp, routes, returned, out_grad)


def last_sum_body(parts_any, out_ref, parts_ref, sems):
    count, steps = parts_any.shape[0], sems.shape[0]
    each = count // steps
    spans = [pl.ds(i * each, each) for i in range(steps)]
    copies = [
        pltpu.make_async_copy(parts_any.at[span], parts_ref.at[span], sems.at[i])
        for i, span in enumerate(spans)
    ]
    for copy in copies:
        copy.start()
    total = jnp.zeros(out_ref.shape, jnp.float32)
    for i, copy in enumerate(copies):
        copy.wait()
        total = total + jnp.sum(parts_ref[spans[i]].astype(jnp.float32), axis=0)
    out_ref[...] = total


def last_sum(parts):
    shape = parts.shape[1:]
    return pl.pallas_call(
        last_sum_body,
        in_specs=[pl.BlockSpec(memory_space=pltpu.HBM)],
        out_specs=whole(shape),
        out_shape=jax.ShapeDtypeStruct(shape, jnp.float32),
        scratch_shapes=[pltpu.VMEM(parts.shape, parts.dtype), pltpu.SemaphoreType.DMA((8,))],
        compiler_params=pltpu.CompilerParams(vmem_limit_bytes=8 * 2**20),
        name="last_sum",
    )(parts)


def proj_body(side_ref, grad_ref, activ_ref, *refs, scale):
    refs[-1][...] = (contract_rows(grad_ref[...], activ_ref[...]) * scale).astype(jnp.bfloat16)


def proj_part(side, grad, activ, scale, base):
    tokens, share = grad.shape
    units = activ.shape[1]
    blocks = 2
    wide = share // blocks
    extra = [] if base is None else [base]

    def place(i, side):
        return ((side[0] if base is None else 1 - side[0]) * blocks + i, 0)

    return pl.pallas_call(
        functools.partial(proj_body, scale=scale),
        grid_spec=pltpu.PrefetchScalarGridSpec(
            num_scalar_prefetch=1,
            grid=(blocks,),
            in_specs=[
                pl.BlockSpec((tokens, wide), lambda i, side: (0, i)),
                pl.BlockSpec((tokens, units), lambda i, side: (0, 0)),
            ]
            + [pl.BlockSpec(memory_space=pl.ANY)] * len(extra),
            out_specs=pl.BlockSpec((wide, units), place),
        ),
        out_shape=pltpu.HBM((2 * share, units), jnp.bfloat16),
        input_output_aliases={} if base is None else {3: 0},
        compiler_params=pltpu.CompilerParams(vmem_limit_bytes=8 * 2**20),
        name="proj_here" if base is None else "proj_there",
    )(side, grad, activ, *extra)


def expert_body(
    tp_ref, rows_ref, gate_ref, up_ref, down_ref,
    hid_any, last_any, gb_ref, ub_ref, pv_ref, hid_ref, last_ref, sems,
):
    groups, tiles, _, wide = rows_ref.shape
    width, units = gate_ref.shape
    count = width // wide
    share = width // 2

    def chunk_of(tile):
        return rows_ref[:, tile].reshape(groups * 8, wide)

    def spans(index):
        return slice(index * wide, (index + 1) * wide)

    gate_pre = sum(matmul(chunk_of(i), gate_ref[spans(i), :]) for i in range(count))
    up_pre = sum(matmul(chunk_of(i), up_ref[spans(i), :]) for i in range(count))
    within = iota((groups, 8, wide), 1)
    last = jnp.zeros((groups, 8, wide), jnp.float32)
    for tile in range(tiles):
        moved = pltpu.roll(rows_ref[:, tile].astype(jnp.float32), tile + 1, 1)
        last = jnp.where(within == tile, moved, last)
    last_ref[...] = last.reshape(groups * 8, wide).astype(jnp.bfloat16)
    leaving = [pltpu.make_async_copy(last_ref, last_any, sems.at[0])]
    leaving[0].start()
    hidden_grad = contract_cols(last_ref[...], down_ref[:, spans(count - 1)])
    for index in range(count - 1):
        hidden_grad = hidden_grad + contract_cols(chunk_of(count + index), down_ref[:, spans(index)])
    real = iota((groups * 8, units), 0) & 7 < tiles
    sigma = jax.nn.sigmoid(gate_pre)
    silu_gate = gate_pre * sigma
    hid_ref[...] = jnp.where(real, silu_gate * up_pre, 0.0).astype(jnp.bfloat16)
    leaving.append(pltpu.make_async_copy(hid_ref, hid_any, sems.at[1]))
    leaving[1].start()
    gate_back = hidden_grad * up_pre * sigma * (1.0 + gate_pre * (1.0 - sigma))
    gb_ref[...] = jnp.where(real, gate_back, 0.0).astype(jnp.bfloat16)
    ub_ref[...] = jnp.where(real, hidden_grad * silu_gate, 0.0).astype(jnp.bfloat16)
    away = pl.ds(pl.multiple_of((1 - tp_ref[0]) * share, share), share)
    pv_ref[...] = (
        contract_cols(gb_ref[...], gate_ref[away, :]) + contract_cols(ub_ref[...], up_ref[away, :])
    ).astype(jnp.bfloat16)
    for copy in leaving:
        copy.wait()


def expert(tp, rows, gate, up, down, name):
    count, wide = rows.shape[0] * 8, rows.shape[3]
    width, units = gate.shape
    outs = [(count, units), (count, wide), (count, units), (count, units), (count, width // 2)]
    return pl.pallas_call(
        expert_body,
        in_specs=[smem, whole(rows.shape), whole(gate.shape), whole(up.shape), whole(down.shape)],
        out_specs=[pl.BlockSpec(memory_space=pltpu.HBM)] * 2 + [whole(s) for s in outs[2:]],
        out_shape=[pltpu.HBM(s, jnp.bfloat16) for s in outs[:2]]
        + [jax.ShapeDtypeStruct(s, jnp.bfloat16) for s in outs[2:]],
        scratch_shapes=[pltpu.VMEM(s, jnp.bfloat16) for s in outs[:2]]
        + [pltpu.SemaphoreType.DMA((2,))],
        name=name,
        compiler_params=pltpu.CompilerParams(vmem_limit_bytes=24 * 2**20),
    )(tp, rows, gate, up, down)


def kept_body(tp_ref, gb0_ref, ub0_ref, gb1_ref, ub1_ref, gate_ref, up_ref, out0_ref, out1_ref):
    share = gate_ref.shape[0] // 2
    here = pl.ds(pl.multiple_of(tp_ref[0] * share, share), share)
    for gb_ref, ub_ref, out_ref in ((gb0_ref, ub0_ref, out0_ref), (gb1_ref, ub1_ref, out1_ref)):
        out_ref[...] = (
            contract_cols(gb_ref[...], gate_ref[here, :])
            + contract_cols(ub_ref[...], up_ref[here, :])
        ).astype(jnp.bfloat16)


def kept_partials(tp, gb0, ub0, gb1, ub1, gate, up):
    out = (gb0.shape[0], gate.shape[0] // 2)
    arrays = (gb0, ub0, gb1, ub1, gate, up)
    return pl.pallas_call(
        kept_body,
        in_specs=[smem] + [whole(a.shape) for a in arrays],
        out_specs=[whole(out)] * 2,
        out_shape=[jax.ShapeDtypeStruct(out, jnp.bfloat16)] * 2,
        name="kept",
        compiler_params=pltpu.CompilerParams(vmem_limit_bytes=16 * 2**20),
    )(tp, *arrays)


def total_body(kept0_ref, kept1_ref, came0_ref, came1_ref, out_any, out_ref, sems, half):
    groups, tiles, _, wide = out_ref.shape
    within = iota((groups, 8, wide), 1)
    leaving = []

    def put(tile, value):
        out_ref[:, tile] = value.astype(jnp.bfloat16)
        copy = pltpu.make_async_copy(out_ref.at[:, tile], out_any.at[:, tile], sems.at[tile])
        copy.start()
        leaving.append(copy)

    def total(kept_ref, came_ref, chunk):
        here = slice(chunk * wide, (chunk + 1) * wide)
        value = kept_ref[:, here].astype(jnp.float32) + came_ref[:, here].astype(jnp.float32)
        return value.reshape(groups, 8, wide)

    before = None
    for chunk in range(4):
        far = total(kept1_ref, came1_ref, chunk)
        near = total(kept0_ref, came0_ref, chunk)
        put(chunk, jnp.where(within < half, near, pltpu.roll(far, 1, 1)))
        start = (half - 1) * chunk % 8
        moved = pltpu.roll(far, start, 1) if start else far
        if chunk:
            put(3 + chunk, jnp.where(within < start, before, moved))
        before = moved
    for copy in leaving:
        copy.wait()


def total_rows(kept0, kept1, came0, came1, half):
    rows, share = kept0.shape
    shape = (rows // 8, 7, 8, share // 4)
    return pl.pallas_call(
        functools.partial(total_body, half=half),
        in_specs=[whole((rows, share))] * 4,
        out_specs=pl.BlockSpec(memory_space=pltpu.HBM),
        out_shape=pltpu.HBM(shape, jnp.bfloat16),
        scratch_shapes=[pltpu.VMEM(shape, jnp.bfloat16), pltpu.SemaphoreType.DMA((7,))],
        compiler_params=pltpu.CompilerParams(vmem_limit_bytes=16 * 2**20),
        name="total",
    )(kept0, kept1, came0, came1)


def weights_body(
    in0_ref, in1_ref, gr0_ref, gr1_ref, last0_ref, last1_ref,
    hid0_ref, hid1_ref, gb0_ref, gb1_ref, ub0_ref, ub1_ref,
    gate_ref, up_ref, down_ref, scale, early,
):
    count, wide = last0_ref.shape

    def flat(ref):
        return ref[:, 0].reshape(count, wide)

    gate_ref[...] = (
        contract_rows(flat(in0_ref), gb0_ref[...]) + contract_rows(flat(in1_ref), gb1_ref[...])
    ) * scale
    up_ref[...] = (
        contract_rows(flat(in0_ref), ub0_ref[...]) + contract_rows(flat(in1_ref), ub1_ref[...])
    ) * scale

    def put_down(grads0, grads1):
        down_ref[...] = (
            contract_rows(hid0_ref[...], grads0) + contract_rows(hid1_ref[...], grads1)
        ) * scale

    @pl.when(pl.program_id(0) < early)
    def _():
        put_down(flat(gr0_ref), flat(gr1_ref))

    @pl.when(pl.program_id(0) >= early)
    def _():
        put_down(last0_ref[...], last1_ref[...])


def weight_grads(rows0, rows1, own, other, scale):
    count, units = own[0].shape
    groups, tiles, _, chunk = rows0.shape
    width = chunk * (tiles + 1) // 2
    blocks = 8
    wide = width // blocks
    per = chunk // wide
    early = (width // chunk - 1) * per
    first = pl.BlockSpec((groups, 1, 8, wide), lambda i: (0, i // per, 0, i % per))

    def later(i):
        j = jnp.minimum(i, early - 1)
        return (0, width // chunk + j // per, 0, j % per)

    second = pl.BlockSpec((groups, 1, 8, wide), later)
    third = pl.BlockSpec((count, wide), lambda i: (0, jnp.maximum(i - early, 0)))
    flops = 3 * 2 * 2 * count * width * units
    return pl.pallas_call(
        functools.partial(weights_body, scale=scale, early=early),
        grid=(blocks,),
        in_specs=[first, first, second, second, third, third] + [whole((count, units))] * 6,
        out_specs=[
            pl.BlockSpec((wide, units), lambda i: (i, 0)),
            pl.BlockSpec((wide, units), lambda i: (i, 0)),
            pl.BlockSpec((units, wide), lambda i: (0, i)),
        ],
        out_shape=[
            jax.ShapeDtypeStruct((width, units), jnp.float32),
            jax.ShapeDtypeStruct((width, units), jnp.float32),
            jax.ShapeDtypeStruct((units, width), jnp.float32),
        ],
        cost_estimate=pl.CostEstimate(
            flops=flops, bytes_accessed=12 * width * units, transcendentals=0
        ),
        name="weight_grads",
        compiler_params=pltpu.CompilerParams(vmem_limit_bytes=58300000),
    )(
        rows0, rows1, rows0, rows1, own[1], other[1],
        own[0], other[0], own[2], other[2], own[3], other[3],
    )


def per_device(
    out_grad,
    moe_input,
    routes,
    route_weights,
    conv_result,
    glu_value,
    glu_gate,
    conv_taps,
    norm_gain,
    proj_weight,
    expert_gate,
    expert_up,
    expert_down,
):
    n_sp = lax.axis_size("sp")
    n_tp = lax.axis_size("tp")
    tok_rows, width = out_grad.shape
    top_count = routes.shape[1]
    capacity = 2 * top_count * tok_rows // n_sp
    half = capacity // n_tp
    slots = n_sp * capacity
    tp = lax.axis_index("tp")
    tp_array = tp.reshape(1).astype(jnp.int32)
    share = width // n_tp
    channels = conv_result.shape[1] * n_tp

    send = dispatch(tp_array, routes.T, route_weights.T, moe_input, out_grad, n_sp, half)
    rows0 = lax.all_to_all(
        send.reshape(n_sp, half * 8, -1), "sp", split_axis=0, concat_axis=0, tiled=True
    ).reshape(send.shape)
    rows1 = lax.ppermute(rows0, "tp", swap)

    gate, up, down = expert_gate[0], expert_up[0], expert_down[0]
    own = expert(tp_array, rows0, gate, up, down, "expert_own")
    other = expert(tp_array, rows1, gate, up, down, "expert_other")
    came1 = lax.ppermute(own[4], "tp", swap)
    came0 = lax.ppermute(other[4], "tp", swap)
    kept0, kept1 = kept_partials(tp_array, own[2], own[3], other[2], other[3], gate, up)
    summed = total_rows(kept0, kept1, came0, came1, half)
    returned = lax.all_to_all(
        summed.reshape(n_sp, 56, share // 4), "sp", split_axis=0, concat_axis=0, tiled=True
    ).reshape(summed.shape)
    gate_g, up_g, down_g = weight_grads(rows0, rows1, own, other, float(slots) ** (-0.5))

    conv_result, gate_g = lax.optimization_barrier((conv_result, gate_g))
    values = conv_result.astype(jnp.float32)
    sums = lax.psum(
        (jnp.sum(values, axis=1), jnp.sum(values * values, axis=1)), "tp"
    )
    center = sums[0] / channels
    spread = sums[1] / channels - center * center
    inv_std = lax.rsqrt(spread + norm_eps)[:, None]
    normed = (values - center[:, None]) * inv_std
    scaled = normed * norm_gain[None, :]
    sig_norm = jax.nn.sigmoid(scaled)
    activ = (scaled * sig_norm).astype(jnp.bfloat16)

    returned, activ, gate_g, up_g, down_g = lax.optimization_barrier(
        (returned, activ, gate_g, up_g, down_g)
    )
    here = combine(tp_array, routes.T, returned, out_grad, half)
    there = lax.ppermute(here, "tp", swap)
    token_scale = float(tok_rows * n_sp) ** (-0.5)
    proj = proj_part(tp_array, here, activ, token_scale, None)
    proj = proj_part(tp_array, there, activ, token_scale, proj)
    proj_parts = proj.reshape(n_sp, width // n_sp, -1)
    proj_grad = last_sum(
        lax.all_to_all(proj_parts, "sp", split_axis=0, concat_axis=0, tiled=True)
    )
    here, there, conv_taps, side, _ = lax.optimization_barrier(
        (here, there, conv_taps, tp_array, proj)
    )
    input_grad = jnp.where(
        side[0] == 0,
        jnp.concatenate([here, there], axis=1),
        jnp.concatenate([there, here], axis=1),
    )
    act_grad = matmul(input_grad, proj_weight)
    norm_grad = act_grad * sig_norm * (1.0 + scaled * (1.0 - sig_norm)) * norm_gain[None, :]
    first, second = lax.psum(
        (jnp.sum(norm_grad, axis=1), jnp.sum(norm_grad * normed, axis=1)), "tp"
    )
    conv_grad = inv_std * (
        norm_grad - first[:, None] / channels - normed * (second[:, None] / channels)
    )
    reach = conv_taps.shape[0]
    rim = from_behind(conv_grad[: reach - 1].astype(jnp.bfloat16), "sp", -1).astype(jnp.float32)
    extended = jnp.concatenate([conv_grad, rim], axis=0)
    taps_float = conv_taps.astype(jnp.float32)
    mixed_grad = jnp.zeros_like(conv_grad)
    for lag in range(reach):
        mixed_grad = (
            mixed_grad + taps_float[reach - 1 - lag][None, :] * extended[lag : lag + tok_rows]
        )
    sig_gate = jax.nn.sigmoid(glu_gate.astype(jnp.float32))
    value_grad = (mixed_grad * sig_gate).astype(jnp.bfloat16)
    gate_side_grad = (
        mixed_grad * glu_value.astype(jnp.float32) * sig_gate * (1.0 - sig_gate)
    ).astype(jnp.bfloat16)
    return (
        input_grad,
        proj_grad,
        gate_g[None],
        up_g[None],
        down_g[None],
        value_grad,
        gate_side_grad,
    )


def solution(mesh):
    in_specs = (
        P("sp", None),
        P("sp", None),
        P("sp", None),
        P("sp", None),
        P("sp", "tp"),
        P("sp", "tp"),
        P("sp", "tp"),
        P(None, "tp"),
        P("tp"),
        P(None, "tp"),
        P("sp", None, "tp"),
        P("sp", None, "tp"),
        P("sp", "tp", None),
    )
    out_specs = (
        P("sp", None),
        P("sp", "tp"),
        P("sp", None, "tp"),
        P("sp", None, "tp"),
        P("sp", "tp", None),
        P("sp", "tp"),
        P("sp", "tp"),
    )
    return jax.shard_map(
        per_device, mesh=mesh, in_specs=in_specs, out_specs=out_specs, check_vma=False
    )
```

```python
import functools

import jax
import jax.numpy as jnp
from jax import lax
from jax.experimental import pallas as pl
from jax.experimental.pallas import tpu as pltpu
from jax.sharding import PartitionSpec as P

norm_eps = 1e-05
swap = [(0, 1), (1, 0)]


def from_behind(shard, axis, by):
    count = lax.axis_size(axis)
    pairs = [(i, i + by) for i in range(count) if 0 <= i + by < count]
    return lax.ppermute(shard, axis, pairs)


def contract_rows(left, right):
    return lax.dot_general(
        left, right, (((0,), (0,)), ((), ())), preferred_element_type=jnp.float32
    )


def contract_cols(left, right):
    return lax.dot_general(
        left, right, (((1,), (1,)), ((), ())), preferred_element_type=jnp.float32
    )


def matmul(left, right):
    return jnp.dot(left, right, preferred_element_type=jnp.float32)


def iota(shape, dim):
    return lax.broadcasted_iota(jnp.int32, shape, dim)


def whole(shape):
    return pl.BlockSpec(shape, lambda *_: (0,) * len(shape))


smem = pl.BlockSpec(memory_space=pltpu.SMEM)


def slot_tables(routes_ref, experts):
    tokens = routes_ref.shape[1]
    row = iota((experts, tokens), 0)
    named = [routes_ref[k : k + 1, :] == row for k in range(2)]
    both = jnp.where(named[0] | named[1], 1.0, 0.0).astype(jnp.bfloat16)
    earlier = jnp.where(iota((tokens, tokens), 0) < iota((tokens, tokens), 1), 1.0, 0.0)
    slot = matmul(both, earlier.astype(jnp.bfloat16))
    return [jnp.where(n, slot, -1.0).astype(jnp.bfloat16) for n in named]


def pick_rows(tables, row_expert, row_slot):
    rows = row_slot.shape[0]
    experts = tables[0].shape[0]
    spread = jnp.where(row_expert == iota((rows, experts), 1), 1.0, 0.0).astype(jnp.bfloat16)
    return [matmul(spread, table) == row_slot.astype(jnp.float32) for table in tables]


def dispatch_body(
    tp_ref, routes_any, weights_any, grad_any, input_any, out_any,
    routes_ref, weights_ref, grad_ref, input_ref, out_ref, sems, out_sems, half,
):
    pairs = (
        (routes_any, routes_ref),
        (weights_any, weights_ref),
        (grad_any, grad_ref),
        (input_any, input_ref),
    )
    copies = [pltpu.make_async_copy(a, b, sems.at[i]) for i, (a, b) in enumerate(pairs)]
    for copy in copies:
        copy.start()
    experts, tokens = out_ref.shape[0], routes_ref.shape[1]
    rows = experts * 8
    width = input_ref.shape[1]
    copies[0].wait()
    tables = slot_tables(routes_ref, experts)
    place = iota((rows, tokens), 0)
    within = place & 7
    slot = jnp.where(within < half, tp_ref[0] * half + within, -2)
    picks = pick_rows(tables, iota((rows, experts), 0) >> 3, slot)
    pick = jnp.where(picks[0] | picks[1], 1.0, 0.0).astype(jnp.bfloat16)
    copies[1].wait()
    chosen = [jnp.where(picks[k], weights_ref[k : k + 1, :], 0.0) for k in range(2)]
    scale = jnp.sum(chosen[0] + chosen[1], axis=1, keepdims=True)
    tiles, wide = out_ref.shape[1], out_ref.shape[3]
    last = width // wide - 1
    within = iota((experts, 8, wide), 1)
    leaving = []

    def chunk_of(ref, index):
        return matmul(pick, ref[:, index * wide : (index + 1) * wide])

    copies[2].wait()
    extra = (chunk_of(grad_ref, last) * scale).reshape(experts, 8, wide)

    def put(tile, value):
        value = value.reshape(experts, 8, wide)
        value = jnp.where(within < half, value, pltpu.roll(extra, half - tile, 1))
        out_ref[:, tile] = value.astype(jnp.bfloat16)
        copy = pltpu.make_async_copy(
            out_ref.at[:, tile], out_any.at[:, tile], out_sems.at[tile]
        )
        copy.start()
        leaving.append(copy)

    for index in range(last):
        put(last + 1 + index, chunk_of(grad_ref, index) * scale)
    copies[3].wait()
    for index in range(last + 1):
        put(index, chunk_of(input_ref, index))
    for copy in leaving:
        copy.wait()


def dispatch(tp, routes, weights, moe_input, out_grad, experts, half):
    shape = (experts, half, 8, 2 * out_grad.shape[1] // 8)
    arrays = (routes, weights, out_grad, moe_input)
    return pl.pallas_call(
        functools.partial(dispatch_body, half=half),
        in_specs=[smem] + [pl.BlockSpec(memory_space=pltpu.HBM)] * 4,
        out_specs=pl.BlockSpec(memory_space=pltpu.HBM),
        out_shape=pltpu.HBM(shape, jnp.bfloat16),
        scratch_shapes=[pltpu.VMEM(a.shape, a.dtype) for a in arrays]
        + [pltpu.VMEM(shape, jnp.bfloat16)]
        + [pltpu.SemaphoreType.DMA((4,)), pltpu.SemaphoreType.DMA((half,))],
        compiler_params=pltpu.CompilerParams(vmem_limit_bytes=58300000),
        name="dispatch",
    )(tp, *arrays)


parcels = ((4, 0), (4, 1), (5, 1), (5, 2), (6, 2), (6, 3))


def return_picks(tp_ref, routes_ref, picks_ref, half):
    tokens, rows = picks_ref.shape[1:]
    experts = rows // 8
    tables = slot_tables(routes_ref, experts)
    spread = jnp.where(iota((experts, rows), 1) >> 3 == iota((experts, rows), 0), 1.0, 0.0)
    spread = spread.astype(jnp.bfloat16)
    found = [contract_rows(table, spread).astype(jnp.int32) for table in tables]
    within = iota((tokens, rows), 1) & 7
    near, far = tp_ref[0] * half, (1 - tp_ref[0]) * half
    slots = [jnp.where(within < half, near + within, far + half - 1)]
    for tile, chunk in parcels:
        rest = 8 * (tile - 4) + within - (half - 1) * chunk
        slots.append(jnp.where((rest >= 0) & (rest < half - 1), far + rest, -2))
    for index, slot in enumerate(slots):
        hit = (found[0] == slot) | (found[1] == slot)
        picks_ref[index] = jnp.where(hit, 1.0, 0.0).astype(jnp.bfloat16)


def combine_body(
    tp_ref, routes_ref, returned_any, grad_any, out_ref,
    picks_ref, tiles_ref, grad_ref, sems, half,
):
    groups, tiles, _, wide = returned_any.shape
    share = grad_ref.shape[1]
    columns = pl.ds(pl.multiple_of(tp_ref[0] * share, share), share)
    copies = {}
    for tile in (0, 4, 1, 5, 2, 6, 3):
        copies[tile] = pltpu.make_async_copy(
            returned_any.at[:, tile], tiles_ref.at[tile], sems.at[tile]
        )
    copies[tiles] = pltpu.make_async_copy(grad_any.at[:, columns], grad_ref, sems.at[tiles])
    for copy in copies.values():
        copy.start()
    return_picks(tp_ref, routes_ref, picks_ref, half)
    ready = {}

    def rows_of(tile):
        if tile not in ready:
            copies[tile].wait()
            ready[tile] = True
        return tiles_ref[tile].reshape(groups * 8, wide)

    for chunk in range(4):
        part = matmul(picks_ref[0], rows_of(chunk))
        for index, (tile, of) in enumerate(parcels):
            if of == chunk:
                part = part + matmul(picks_ref[1 + index], rows_of(tile))
        if chunk == 0:
            copies[tiles].wait()
        here = slice(chunk * wide, (chunk + 1) * wide)
        out_ref[:, here] = (grad_ref[:, here].astype(jnp.float32) + part).astype(jnp.bfloat16)


def combine(tp, routes, returned, out_grad, half):
    groups, tiles, _, wide = returned.shape
    tokens = out_grad.shape[0]
    shape = (tokens, 4 * wide)
    return pl.pallas_call(
        functools.partial(combine_body, half=half),
        in_specs=[smem, whole(routes.shape)] + [pl.BlockSpec(memory_space=pltpu.HBM)] * 2,
        out_specs=whole(shape),
        out_shape=jax.ShapeDtypeStruct(shape, jnp.bfloat16),
        scratch_shapes=[
            pltpu.VMEM((1 + len(parcels), tokens, groups * 8), jnp.bfloat16),
            pltpu.VMEM((tiles, groups, 8, wide), jnp.bfloat16),
            pltpu.VMEM(shape, jnp.bfloat16),
            pltpu.SemaphoreType.DMA((tiles + 1,)),
        ],
        compiler_params=pltpu.CompilerParams(vmem_limit_bytes=16 * 2**20),
        name="combine",
    )(tp, routes, returned, out_grad)


def last_sum_body(parts_any, out_ref, parts_ref, sems):
    count, steps = parts_any.shape[0], sems.shape[0]
    each = count // steps
    spans = [pl.ds(i * each, each) for i in range(steps)]
    copies = [
        pltpu.make_async_copy(parts_any.at[span], parts_ref.at[span], sems.at[i])
        for i, span in enumerate(spans)
    ]
    for copy in copies:
        copy.start()
    total = jnp.zeros(out_ref.shape, jnp.float32)
    for i, copy in enumerate(copies):
        copy.wait()
        total = total + jnp.sum(parts_ref[spans[i]].astype(jnp.float32), axis=0)
    out_ref[...] = total


def last_sum(parts):
    shape = parts.shape[1:]
    return pl.pallas_call(
        last_sum_body,
        in_specs=[pl.BlockSpec(memory_space=pltpu.HBM)],
        out_specs=whole(shape),
        out_shape=jax.ShapeDtypeStruct(shape, jnp.float32),
        scratch_shapes=[pltpu.VMEM(parts.shape, parts.dtype), pltpu.SemaphoreType.DMA((8,))],
        compiler_params=pltpu.CompilerParams(vmem_limit_bytes=8 * 2**20),
        name="last_sum",
    )(parts)


def proj_body(side_ref, grad_ref, activ_ref, *refs, scale):
    refs[-1][...] = (contract_rows(grad_ref[...], activ_ref[...]) * scale).astype(jnp.bfloat16)


def proj_part(side, grad, activ, scale, base):
    tokens, share = grad.shape
    units = activ.shape[1]
    blocks = 4
    wide = share // blocks
    extra = [] if base is None else [base]

    def place(i, side):
        return ((side[0] if base is None else 1 - side[0]) * blocks + i, 0)

    return pl.pallas_call(
        functools.partial(proj_body, scale=scale),
        grid_spec=pltpu.PrefetchScalarGridSpec(
            num_scalar_prefetch=1,
            grid=(blocks,),
            in_specs=[
                pl.BlockSpec((tokens, wide), lambda i, side: (0, i)),
                pl.BlockSpec((tokens, units), lambda i, side: (0, 0)),
            ]
            + [pl.BlockSpec(memory_space=pl.ANY)] * len(extra),
            out_specs=pl.BlockSpec((wide, units), place),
        ),
        out_shape=pltpu.HBM((2 * share, units), jnp.bfloat16),
        input_output_aliases={} if base is None else {3: 0},
        compiler_params=pltpu.CompilerParams(vmem_limit_bytes=8 * 2**20),
        name="proj_here" if base is None else "proj_there",
    )(side, grad, activ, *extra)


def expert_body(
    tp_ref, rows_ref, gate_ref, up_ref, down_ref,
    hid_any, last_any, gb_ref, ub_ref, pv_ref, hid_ref, last_ref, sems,
):
    groups, tiles, _, wide = rows_ref.shape
    width, units = gate_ref.shape
    count = width // wide
    share = width // 2

    def chunk_of(tile):
        return rows_ref[:, tile].reshape(groups * 8, wide)

    def spans(index):
        return slice(index * wide, (index + 1) * wide)

    within = iota((groups, 8, wide), 1)
    last = jnp.zeros((groups, 8, wide), jnp.float32)
    sums = []
    tile = 0
    for weight_ref in (gate_ref, up_ref):
        total = None
        for index in range(count):
            part = matmul(chunk_of(index), weight_ref[spans(index), :])
            total = part if total is None else total + part
            if tile < tiles:
                moved = pltpu.roll(rows_ref[:, tile].astype(jnp.float32), tile + 1, 1)
                last = jnp.where(within == tile, moved, last)
                tile += 1
        sums.append(total)
    gate_pre, up_pre = sums
    last_ref[...] = last.reshape(groups * 8, wide).astype(jnp.bfloat16)
    leaving = [pltpu.make_async_copy(last_ref, last_any, sems.at[0])]
    leaving[0].start()
    hidden_grad = contract_cols(last_ref[...], down_ref[:, spans(count - 1)])
    for index in range(count - 1):
        hidden_grad = hidden_grad + contract_cols(chunk_of(count + index), down_ref[:, spans(index)])
    real = iota((groups * 8, units), 0) & 7 < tiles
    sigma = jax.nn.sigmoid(gate_pre)
    silu_gate = gate_pre * sigma
    hid_ref[...] = jnp.where(real, silu_gate * up_pre, 0.0).astype(jnp.bfloat16)
    leaving.append(pltpu.make_async_copy(hid_ref, hid_any, sems.at[1]))
    leaving[1].start()
    gate_back = hidden_grad * up_pre * sigma * (1.0 + gate_pre * (1.0 - sigma))
    gb_ref[...] = jnp.where(real, gate_back, 0.0).astype(jnp.bfloat16)
    ub_ref[...] = jnp.where(real, hidden_grad * silu_gate, 0.0).astype(jnp.bfloat16)
    away = pl.ds(pl.multiple_of((1 - tp_ref[0]) * share, share), share)
    pv_ref[...] = (
        contract_cols(gb_ref[...], gate_ref[away, :]) + contract_cols(ub_ref[...], up_ref[away, :])
    ).astype(jnp.bfloat16)
    for copy in leaving:
        copy.wait()


def expert(tp, rows, gate, up, down, name):
    count, wide = rows.shape[0] * 8, rows.shape[3]
    width, units = gate.shape
    outs = [(count, units), (count, wide), (count, units), (count, units), (count, width // 2)]
    return pl.pallas_call(
        expert_body,
        in_specs=[smem, whole(rows.shape), whole(gate.shape), whole(up.shape), whole(down.shape)],
        out_specs=[pl.BlockSpec(memory_space=pltpu.HBM)] * 2 + [whole(s) for s in outs[2:]],
        out_shape=[pltpu.HBM(s, jnp.bfloat16) for s in outs[:2]]
        + [jax.ShapeDtypeStruct(s, jnp.bfloat16) for s in outs[2:]],
        scratch_shapes=[pltpu.VMEM(s, jnp.bfloat16) for s in outs[:2]]
        + [pltpu.SemaphoreType.DMA((2,))],
        name=name,
        compiler_params=pltpu.CompilerParams(vmem_limit_bytes=24 * 2**20),
    )(tp, rows, gate, up, down)


def kept_body(tp_ref, gb0_ref, ub0_ref, gb1_ref, ub1_ref, gate_ref, up_ref, out0_ref, out1_ref):
    share = gate_ref.shape[0] // 2
    here = pl.ds(pl.multiple_of(tp_ref[0] * share, share), share)
    for gb_ref, ub_ref, out_ref in ((gb0_ref, ub0_ref, out0_ref), (gb1_ref, ub1_ref, out1_ref)):
        out_ref[...] = (
            contract_cols(gb_ref[...], gate_ref[here, :])
            + contract_cols(ub_ref[...], up_ref[here, :])
        ).astype(jnp.bfloat16)


def kept_partials(tp, gb0, ub0, gb1, ub1, gate, up):
    out = (gb0.shape[0], gate.shape[0] // 2)
    arrays = (gb0, ub0, gb1, ub1, gate, up)
    return pl.pallas_call(
        kept_body,
        in_specs=[smem] + [whole(a.shape) for a in arrays],
        out_specs=[whole(out)] * 2,
        out_shape=[jax.ShapeDtypeStruct(out, jnp.bfloat16)] * 2,
        name="kept",
        compiler_params=pltpu.CompilerParams(vmem_limit_bytes=16 * 2**20),
    )(tp, *arrays)


def total_body(kept0_ref, kept1_ref, came0_ref, came1_ref, out_any, out_ref, sems, half):
    groups, tiles, _, wide = out_ref.shape
    within = iota((groups, 8, wide), 1)
    leaving = []

    def put(tile, value):
        out_ref[:, tile] = value.astype(jnp.bfloat16)
        copy = pltpu.make_async_copy(out_ref.at[:, tile], out_any.at[:, tile], sems.at[tile])
        copy.start()
        leaving.append(copy)

    def total(kept_ref, came_ref, chunk):
        here = slice(chunk * wide, (chunk + 1) * wide)
        value = kept_ref[:, here].astype(jnp.float32) + came_ref[:, here].astype(jnp.float32)
        return value.reshape(groups, 8, wide)

    before = None
    for chunk in range(4):
        far = total(kept1_ref, came1_ref, chunk)
        near = total(kept0_ref, came0_ref, chunk)
        put(chunk, jnp.where(within < half, near, pltpu.roll(far, 1, 1)))
        start = (half - 1) * chunk % 8
        moved = pltpu.roll(far, start, 1) if start else far
        if chunk:
            put(3 + chunk, jnp.where(within < start, before, moved))
        before = moved
    for copy in leaving:
        copy.wait()


def total_rows(kept0, kept1, came0, came1, half):
    rows, share = kept0.shape
    shape = (rows // 8, 7, 8, share // 4)
    return pl.pallas_call(
        functools.partial(total_body, half=half),
        in_specs=[whole((rows, share))] * 4,
        out_specs=pl.BlockSpec(memory_space=pltpu.HBM),
        out_shape=pltpu.HBM(shape, jnp.bfloat16),
        scratch_shapes=[pltpu.VMEM(shape, jnp.bfloat16), pltpu.SemaphoreType.DMA((7,))],
        compiler_params=pltpu.CompilerParams(vmem_limit_bytes=16 * 2**20),
        name="total",
    )(kept0, kept1, came0, came1)


def weights_body(
    in0_ref, in1_ref, gr0_ref, gr1_ref, last0_ref, last1_ref,
    hid0_ref, hid1_ref, gb0_ref, gb1_ref, ub0_ref, ub1_ref,
    gate_ref, up_ref, down_ref, scale, early,
):
    count, wide = last0_ref.shape

    def flat(ref):
        return ref[:, 0].reshape(count, wide)

    gate_ref[...] = (
        contract_rows(flat(in0_ref), gb0_ref[...]) + contract_rows(flat(in1_ref), gb1_ref[...])
    ) * scale
    up_ref[...] = (
        contract_rows(flat(in0_ref), ub0_ref[...]) + contract_rows(flat(in1_ref), ub1_ref[...])
    ) * scale

    def put_down(grads0, grads1):
        down_ref[...] = (
            contract_rows(hid0_ref[...], grads0) + contract_rows(hid1_ref[...], grads1)
        ) * scale

    @pl.when(pl.program_id(0) < early)
    def _():
        put_down(flat(gr0_ref), flat(gr1_ref))

    @pl.when(pl.program_id(0) >= early)
    def _():
        put_down(last0_ref[...], last1_ref[...])


def weight_grads(rows0, rows1, own, other, scale):
    count, units = own[0].shape
    groups, tiles, _, chunk = rows0.shape
    width = chunk * (tiles + 1) // 2
    blocks = 8
    wide = width // blocks
    per = chunk // wide
    early = (width // chunk - 1) * per
    first = pl.BlockSpec((groups, 1, 8, wide), lambda i: (0, i // per, 0, i % per))

    def later(i):
        j = jnp.minimum(i, early - 1)
        return (0, width // chunk + j // per, 0, j % per)

    second = pl.BlockSpec((groups, 1, 8, wide), later)
    third = pl.BlockSpec((count, wide), lambda i: (0, jnp.maximum(i - early, 0)))
    flops = 3 * 2 * 2 * count * width * units
    return pl.pallas_call(
        functools.partial(weights_body, scale=scale, early=early),
        grid=(blocks,),
        in_specs=[first, first, second, second, third, third] + [whole((count, units))] * 6,
        out_specs=[
            pl.BlockSpec((wide, units), lambda i: (i, 0)),
            pl.BlockSpec((wide, units), lambda i: (i, 0)),
            pl.BlockSpec((units, wide), lambda i: (0, i)),
        ],
        out_shape=[
            jax.ShapeDtypeStruct((width, units), jnp.float32),
            jax.ShapeDtypeStruct((width, units), jnp.float32),
            jax.ShapeDtypeStruct((units, width), jnp.float32),
        ],
        cost_estimate=pl.CostEstimate(
            flops=flops, bytes_accessed=12 * width * units, transcendentals=0
        ),
        name="weight_grads",
        compiler_params=pltpu.CompilerParams(vmem_limit_bytes=58300000),
    )(
        rows0, rows1, rows0, rows1, own[1], other[1],
        own[0], other[0], own[2], other[2], own[3], other[3],
    )


def per_device(
    out_grad,
    moe_input,
    routes,
    route_weights,
    conv_result,
    glu_value,
    glu_gate,
    conv_taps,
    norm_gain,
    proj_weight,
    expert_gate,
    expert_up,
    expert_down,
):
    n_sp = lax.axis_size("sp")
    n_tp = lax.axis_size("tp")
    tok_rows, width = out_grad.shape
    top_count = routes.shape[1]
    capacity = 2 * top_count * tok_rows // n_sp
    half = capacity // n_tp
    slots = n_sp * capacity
    tp = lax.axis_index("tp")
    tp_array = tp.reshape(1).astype(jnp.int32)
    share = width // n_tp
    channels = conv_result.shape[1] * n_tp

    send = dispatch(tp_array, routes.T, route_weights.T, moe_input, out_grad, n_sp, half)
    rows0 = lax.all_to_all(
        send.reshape(n_sp, half * 8, -1), "sp", split_axis=0, concat_axis=0, tiled=True
    ).reshape(send.shape)
    rows1 = lax.ppermute(rows0, "tp", swap)

    gate, up, down = expert_gate[0], expert_up[0], expert_down[0]
    own = expert(tp_array, rows0, gate, up, down, "expert_own")
    other = expert(tp_array, rows1, gate, up, down, "expert_other")
    came1 = lax.ppermute(own[4], "tp", swap)
    came0 = lax.ppermute(other[4], "tp", swap)
    kept0, kept1 = kept_partials(tp_array, own[2], own[3], other[2], other[3], gate, up)
    summed = total_rows(kept0, kept1, came0, came1, half)
    returned = lax.all_to_all(
        summed.reshape(n_sp, 56, share // 4), "sp", split_axis=0, concat_axis=0, tiled=True
    ).reshape(summed.shape)
    gate_g, up_g, down_g = weight_grads(rows0, rows1, own, other, float(slots) ** (-0.5))

    conv_result, gate_g = lax.optimization_barrier((conv_result, gate_g))
    values = conv_result.astype(jnp.float32)
    sums = lax.psum(
        (jnp.sum(values, axis=1), jnp.sum(values * values, axis=1)), "tp"
    )
    center = sums[0] / channels
    spread = sums[1] / channels - center * center
    inv_std = lax.rsqrt(spread + norm_eps)[:, None]
    normed = (values - center[:, None]) * inv_std
    scaled = normed * norm_gain[None, :]
    sig_norm = jax.nn.sigmoid(scaled)
    activ = (scaled * sig_norm).astype(jnp.bfloat16)

    returned, activ, gate_g, up_g, down_g = lax.optimization_barrier(
        (returned, activ, gate_g, up_g, down_g)
    )
    here = combine(tp_array, routes.T, returned, out_grad, half)
    there = lax.ppermute(here, "tp", swap)
    token_scale = float(tok_rows * n_sp) ** (-0.5)
    proj = proj_part(tp_array, here, activ, token_scale, None)
    proj = proj_part(tp_array, there, activ, token_scale, proj)
    proj_parts = proj.reshape(n_sp, width // n_sp, -1)
    proj_grad = last_sum(
        lax.all_to_all(proj_parts, "sp", split_axis=0, concat_axis=0, tiled=True)
    )
    here, there, conv_taps, side, _ = lax.optimization_barrier(
        (here, there, conv_taps, tp_array, proj)
    )
    input_grad = jnp.where(
        side[0] == 0,
        jnp.concatenate([here, there], axis=1),
        jnp.concatenate([there, here], axis=1),
    )
    act_grad = matmul(input_grad, proj_weight)
    norm_grad = act_grad * sig_norm * (1.0 + scaled * (1.0 - sig_norm)) * norm_gain[None, :]
    first, second = lax.psum(
        (jnp.sum(norm_grad, axis=1), jnp.sum(norm_grad * normed, axis=1)), "tp"
    )
    conv_grad = inv_std * (
        norm_grad - first[:, None] / channels - normed * (second[:, None] / channels)
    )
    reach = conv_taps.shape[0]
    rim = from_behind(conv_grad[: reach - 1].astype(jnp.bfloat16), "sp", -1).astype(jnp.float32)
    extended = jnp.concatenate([conv_grad, rim], axis=0)
    taps_float = conv_taps.astype(jnp.float32)
    mixed_grad = jnp.zeros_like(conv_grad)
    for lag in range(reach):
        mixed_grad = (
            mixed_grad + taps_float[reach - 1 - lag][None, :] * extended[lag : lag + tok_rows]
        )
    sig_gate = jax.nn.sigmoid(glu_gate.astype(jnp.float32))
    value_grad = (mixed_grad * sig_gate).astype(jnp.bfloat16)
    gate_side_grad = (
        mixed_grad * glu_value.astype(jnp.float32) * sig_gate * (1.0 - sig_gate)
    ).astype(jnp.bfloat16)
    return (
        input_grad,
        proj_grad,
        gate_g[None],
        up_g[None],
        down_g[None],
        value_grad,
        gate_side_grad,
    )


def solution(mesh):
    in_specs = (
        P("sp", None),
        P("sp", None),
        P("sp", None),
        P("sp", None),
        P("sp", "tp"),
        P("sp", "tp"),
        P("sp", "tp"),
        P(None, "tp"),
        P("tp"),
        P(None, "tp"),
        P("sp", None, "tp"),
        P("sp", None, "tp"),
        P("sp", "tp", None),
    )
    out_specs = (
        P("sp", None),
        P("sp", "tp"),
        P("sp", None, "tp"),
        P("sp", None, "tp"),
        P("sp", "tp", None),
        P("sp", "tp"),
        P("sp", "tp"),
    )
    return jax.shard_map(
        per_device, mesh=mesh, in_specs=in_specs, out_specs=out_specs, check_vma=False
    )
```

```python
import functools

import jax
import jax.numpy as jnp
from jax import lax
from jax.experimental import pallas as pl
from jax.experimental.pallas import tpu as pltpu
from jax.sharding import PartitionSpec as P

norm_eps = 1e-05
swap = [(0, 1), (1, 0)]


def from_behind(shard, axis, by):
    count = lax.axis_size(axis)
    pairs = [(i, i + by) for i in range(count) if 0 <= i + by < count]
    return lax.ppermute(shard, axis, pairs)


def contract_rows(left, right):
    return lax.dot_general(
        left, right, (((0,), (0,)), ((), ())), preferred_element_type=jnp.float32
    )


def contract_cols(left, right):
    return lax.dot_general(
        left, right, (((1,), (1,)), ((), ())), preferred_element_type=jnp.float32
    )


def matmul(left, right):
    return jnp.dot(left, right, preferred_element_type=jnp.float32)


def iota(shape, dim):
    return lax.broadcasted_iota(jnp.int32, shape, dim)


def whole(shape):
    return pl.BlockSpec(shape, lambda *_: (0,) * len(shape))


smem = pl.BlockSpec(memory_space=pltpu.SMEM)


def slot_tables(routes_ref, experts):
    tokens = routes_ref.shape[1]
    row = iota((experts, tokens), 0)
    named = [routes_ref[k : k + 1, :] == row for k in range(2)]
    both = jnp.where(named[0] | named[1], 1.0, 0.0).astype(jnp.bfloat16)
    earlier = jnp.where(iota((tokens, tokens), 0) < iota((tokens, tokens), 1), 1.0, 0.0)
    slot = matmul(both, earlier.astype(jnp.bfloat16))
    return [jnp.where(n, slot, -1.0).astype(jnp.bfloat16) for n in named]


def pick_rows(tables, row_expert, row_slot):
    rows = row_slot.shape[0]
    experts = tables[0].shape[0]
    spread = jnp.where(row_expert == iota((rows, experts), 1), 1.0, 0.0).astype(jnp.bfloat16)
    return [matmul(spread, table) == row_slot.astype(jnp.float32) for table in tables]


def dispatch_body(
    tp_ref, routes_any, weights_any, grad_any, input_any, out_any,
    routes_ref, weights_ref, grad_ref, input_ref, out_ref, sems, out_sems, half,
):
    pairs = (
        (routes_any, routes_ref),
        (weights_any, weights_ref),
        (grad_any, grad_ref),
        (input_any, input_ref),
    )
    copies = [pltpu.make_async_copy(a, b, sems.at[i]) for i, (a, b) in enumerate(pairs)]
    for copy in copies:
        copy.start()
    experts, tokens = out_ref.shape[0], routes_ref.shape[1]
    rows = experts * 8
    width = input_ref.shape[1]
    copies[0].wait()
    tables = slot_tables(routes_ref, experts)
    place = iota((rows, tokens), 0)
    within = place & 7
    slot = jnp.where(within < half, tp_ref[0] * half + within, -2)
    picks = pick_rows(tables, iota((rows, experts), 0) >> 3, slot)
    pick = jnp.where(picks[0] | picks[1], 1.0, 0.0).astype(jnp.bfloat16)
    copies[1].wait()
    chosen = [jnp.where(picks[k], weights_ref[k : k + 1, :], 0.0) for k in range(2)]
    scale = jnp.sum(chosen[0] + chosen[1], axis=1, keepdims=True)
    tiles, wide = out_ref.shape[1], out_ref.shape[3]
    last = width // wide - 1
    within = iota((experts, 8, wide), 1)
    leaving = []

    def chunk_of(ref, index):
        return matmul(pick, ref[:, index * wide : (index + 1) * wide])

    copies[2].wait()
    extra = (chunk_of(grad_ref, last) * scale).reshape(experts, 8, wide)

    def put(tile, value):
        value = value.reshape(experts, 8, wide)
        value = jnp.where(within < half, value, pltpu.roll(extra, half - tile, 1))
        out_ref[:, tile] = value.astype(jnp.bfloat16)
        copy = pltpu.make_async_copy(
            out_ref.at[:, tile], out_any.at[:, tile], out_sems.at[tile]
        )
        copy.start()
        leaving.append(copy)

    for index in range(last):
        put(last + 1 + index, chunk_of(grad_ref, index) * scale)
    copies[3].wait()
    for index in range(last + 1):
        put(index, chunk_of(input_ref, index))
    for copy in leaving:
        copy.wait()


def dispatch(tp, routes, weights, moe_input, out_grad, experts, half):
    shape = (experts, half, 8, 2 * out_grad.shape[1] // 8)
    arrays = (routes, weights, out_grad, moe_input)
    return pl.pallas_call(
        functools.partial(dispatch_body, half=half),
        in_specs=[smem] + [pl.BlockSpec(memory_space=pltpu.HBM)] * 4,
        out_specs=pl.BlockSpec(memory_space=pltpu.HBM),
        out_shape=pltpu.HBM(shape, jnp.bfloat16),
        scratch_shapes=[pltpu.VMEM(a.shape, a.dtype) for a in arrays]
        + [pltpu.VMEM(shape, jnp.bfloat16)]
        + [pltpu.SemaphoreType.DMA((4,)), pltpu.SemaphoreType.DMA((half,))],
        compiler_params=pltpu.CompilerParams(vmem_limit_bytes=58300000),
        name="dispatch",
    )(tp, *arrays)


parcels = ((4, 0), (4, 1), (5, 1), (5, 2), (6, 2), (6, 3))


def return_picks(tp_ref, routes_ref, picks_ref, half):
    tokens, rows = picks_ref.shape[1:]
    experts = rows // 8
    tables = slot_tables(routes_ref, experts)
    spread = jnp.where(iota((experts, rows), 1) >> 3 == iota((experts, rows), 0), 1.0, 0.0)
    spread = spread.astype(jnp.bfloat16)
    found = [contract_rows(table, spread).astype(jnp.int32) for table in tables]
    within = iota((tokens, rows), 1) & 7
    near, far = tp_ref[0] * half, (1 - tp_ref[0]) * half
    slots = [jnp.where(within < half, near + within, far + half - 1)]
    for tile, chunk in parcels:
        rest = 8 * (tile - 4) + within - (half - 1) * chunk
        slots.append(jnp.where((rest >= 0) & (rest < half - 1), far + rest, -2))
    for index, slot in enumerate(slots):
        hit = (found[0] == slot) | (found[1] == slot)
        picks_ref[index] = jnp.where(hit, 1.0, 0.0).astype(jnp.bfloat16)


def combine_body(
    tp_ref, routes_ref, returned_any, grad_any, out_ref,
    picks_ref, tiles_ref, grad_ref, sems, half,
):
    groups, tiles, _, wide = returned_any.shape
    share = grad_ref.shape[1]
    columns = pl.ds(pl.multiple_of(tp_ref[0] * share, share), share)
    copies = {}
    for tile in (0, 4, 1, 5, 2, 6, 3):
        copies[tile] = pltpu.make_async_copy(
            returned_any.at[:, tile], tiles_ref.at[tile], sems.at[tile]
        )
    copies[tiles] = pltpu.make_async_copy(grad_any.at[:, columns], grad_ref, sems.at[tiles])
    for copy in copies.values():
        copy.start()
    return_picks(tp_ref, routes_ref, picks_ref, half)
    ready = {}

    def rows_of(tile):
        if tile not in ready:
            copies[tile].wait()
            ready[tile] = True
        return tiles_ref[tile].reshape(groups * 8, wide)

    for chunk in range(4):
        part = matmul(picks_ref[0], rows_of(chunk))
        for index, (tile, of) in enumerate(parcels):
            if of == chunk:
                part = part + matmul(picks_ref[1 + index], rows_of(tile))
        if chunk == 0:
            copies[tiles].wait()
        here = slice(chunk * wide, (chunk + 1) * wide)
        out_ref[:, here] = (grad_ref[:, here].astype(jnp.float32) + part).astype(jnp.bfloat16)


def combine(tp, routes, returned, out_grad, half):
    groups, tiles, _, wide = returned.shape
    tokens = out_grad.shape[0]
    shape = (tokens, 4 * wide)
    return pl.pallas_call(
        functools.partial(combine_body, half=half),
        in_specs=[smem, whole(routes.shape)] + [pl.BlockSpec(memory_space=pltpu.HBM)] * 2,
        out_specs=whole(shape),
        out_shape=jax.ShapeDtypeStruct(shape, jnp.bfloat16),
        scratch_shapes=[
            pltpu.VMEM((1 + len(parcels), tokens, groups * 8), jnp.bfloat16),
            pltpu.VMEM((tiles, groups, 8, wide), jnp.bfloat16),
            pltpu.VMEM(shape, jnp.bfloat16),
            pltpu.SemaphoreType.DMA((tiles + 1,)),
        ],
        compiler_params=pltpu.CompilerParams(vmem_limit_bytes=16 * 2**20),
        name="combine",
    )(tp, routes, returned, out_grad)


def last_sum_body(parts_any, out_ref, parts_ref, sems):
    count, steps = parts_any.shape[0], sems.shape[0]
    each = count // steps
    spans = [pl.ds(i * each, each) for i in range(steps)]
    copies = [
        pltpu.make_async_copy(parts_any.at[span], parts_ref.at[span], sems.at[i])
        for i, span in enumerate(spans)
    ]
    for copy in copies:
        copy.start()
    total = jnp.zeros(out_ref.shape, jnp.float32)
    for i, copy in enumerate(copies):
        copy.wait()
        total = total + jnp.sum(parts_ref[spans[i]].astype(jnp.float32), axis=0)
    out_ref[...] = total


def last_sum(parts):
    shape = parts.shape[1:]
    return pl.pallas_call(
        last_sum_body,
        in_specs=[pl.BlockSpec(memory_space=pltpu.HBM)],
        out_specs=whole(shape),
        out_shape=jax.ShapeDtypeStruct(shape, jnp.float32),
        scratch_shapes=[pltpu.VMEM(parts.shape, parts.dtype), pltpu.SemaphoreType.DMA((8,))],
        compiler_params=pltpu.CompilerParams(vmem_limit_bytes=8 * 2**20),
        name="last_sum",
    )(parts)


def proj_body(side_ref, grad_ref, activ_ref, *refs, scale):
    refs[-1][...] = (contract_rows(grad_ref[...], activ_ref[...]) * scale).astype(jnp.bfloat16)


def proj_part(side, grad, activ, scale, base):
    tokens, share = grad.shape
    units = activ.shape[1]
    blocks = 1
    wide = share // blocks
    extra = [] if base is None else [base]

    def place(i, side):
        return ((side[0] if base is None else 1 - side[0]) * blocks + i, 0)

    return pl.pallas_call(
        functools.partial(proj_body, scale=scale),
        grid_spec=pltpu.PrefetchScalarGridSpec(
            num_scalar_prefetch=1,
            grid=(blocks,),
            in_specs=[
                pl.BlockSpec((tokens, wide), lambda i, side: (0, i)),
                pl.BlockSpec((tokens, units), lambda i, side: (0, 0)),
            ]
            + [pl.BlockSpec(memory_space=pl.ANY)] * len(extra),
            out_specs=pl.BlockSpec((wide, units), place),
        ),
        out_shape=pltpu.HBM((2 * share, units), jnp.bfloat16),
        input_output_aliases={} if base is None else {3: 0},
        compiler_params=pltpu.CompilerParams(vmem_limit_bytes=8 * 2**20),
        name="proj_here" if base is None else "proj_there",
    )(side, grad, activ, *extra)


def expert_body(
    tp_ref, rows_ref, gate_ref, up_ref, down_ref,
    hid_any, last_any, gb_ref, ub_ref, pv_ref, hid_ref, last_ref, sems,
):
    groups, tiles, _, wide = rows_ref.shape
    width, units = gate_ref.shape
    count = width // wide
    share = width // 2

    def chunk_of(tile):
        return rows_ref[:, tile].reshape(groups * 8, wide)

    def spans(index):
        return slice(index * wide, (index + 1) * wide)

    within = iota((groups, 8, wide), 1)
    last = jnp.zeros((groups, 8, wide), jnp.float32)
    sums = []
    tile = 0
    for weight_ref in (gate_ref, up_ref):
        total = None
        for index in range(count):
            part = matmul(chunk_of(index), weight_ref[spans(index), :])
            total = part if total is None else total + part
            if tile < tiles:
                moved = pltpu.roll(rows_ref[:, tile].astype(jnp.float32), tile + 1, 1)
                last = jnp.where(within == tile, moved, last)
                tile += 1
        sums.append(total)
    gate_pre, up_pre = sums
    last_ref[...] = last.reshape(groups * 8, wide).astype(jnp.bfloat16)
    leaving = [pltpu.make_async_copy(last_ref, last_any, sems.at[0])]
    leaving[0].start()
    hidden_grad = contract_cols(last_ref[...], down_ref[:, spans(count - 1)])
    for index in range(count - 1):
        hidden_grad = hidden_grad + contract_cols(chunk_of(count + index), down_ref[:, spans(index)])
    real = iota((groups * 8, units), 0) & 7 < tiles
    sigma = jax.nn.sigmoid(gate_pre)
    silu_gate = gate_pre * sigma
    hid_ref[...] = jnp.where(real, silu_gate * up_pre, 0.0).astype(jnp.bfloat16)
    leaving.append(pltpu.make_async_copy(hid_ref, hid_any, sems.at[1]))
    leaving[1].start()
    gate_back = hidden_grad * up_pre * sigma * (1.0 + gate_pre * (1.0 - sigma))
    gb_ref[...] = jnp.where(real, gate_back, 0.0).astype(jnp.bfloat16)
    ub_ref[...] = jnp.where(real, hidden_grad * silu_gate, 0.0).astype(jnp.bfloat16)
    away = pl.ds(pl.multiple_of((1 - tp_ref[0]) * share, share), share)
    pv_ref[...] = (
        contract_cols(gb_ref[...], gate_ref[away, :]) + contract_cols(ub_ref[...], up_ref[away, :])
    ).astype(jnp.bfloat16)
    for copy in leaving:
        copy.wait()


def expert(tp, rows, gate, up, down, name):
    count, wide = rows.shape[0] * 8, rows.shape[3]
    width, units = gate.shape
    outs = [(count, units), (count, wide), (count, units), (count, units), (count, width // 2)]
    return pl.pallas_call(
        expert_body,
        in_specs=[smem, whole(rows.shape), whole(gate.shape), whole(up.shape), whole(down.shape)],
        out_specs=[pl.BlockSpec(memory_space=pltpu.HBM)] * 2 + [whole(s) for s in outs[2:]],
        out_shape=[pltpu.HBM(s, jnp.bfloat16) for s in outs[:2]]
        + [jax.ShapeDtypeStruct(s, jnp.bfloat16) for s in outs[2:]],
        scratch_shapes=[pltpu.VMEM(s, jnp.bfloat16) for s in outs[:2]]
        + [pltpu.SemaphoreType.DMA((2,))],
        name=name,
        compiler_params=pltpu.CompilerParams(vmem_limit_bytes=24 * 2**20),
    )(tp, rows, gate, up, down)


def kept_body(tp_ref, gb0_ref, ub0_ref, gb1_ref, ub1_ref, gate_ref, up_ref, out0_ref, out1_ref):
    share = gate_ref.shape[0] // 2
    here = pl.ds(pl.multiple_of(tp_ref[0] * share, share), share)
    for gb_ref, ub_ref, out_ref in ((gb0_ref, ub0_ref, out0_ref), (gb1_ref, ub1_ref, out1_ref)):
        out_ref[...] = (
            contract_cols(gb_ref[...], gate_ref[here, :])
            + contract_cols(ub_ref[...], up_ref[here, :])
        ).astype(jnp.bfloat16)


def kept_partials(tp, gb0, ub0, gb1, ub1, gate, up):
    out = (gb0.shape[0], gate.shape[0] // 2)
    arrays = (gb0, ub0, gb1, ub1, gate, up)
    return pl.pallas_call(
        kept_body,
        in_specs=[smem] + [whole(a.shape) for a in arrays],
        out_specs=[whole(out)] * 2,
        out_shape=[jax.ShapeDtypeStruct(out, jnp.bfloat16)] * 2,
        name="kept",
        compiler_params=pltpu.CompilerParams(vmem_limit_bytes=16 * 2**20),
    )(tp, *arrays)


def total_body(kept0_ref, kept1_ref, came0_ref, came1_ref, out_any, out_ref, sems, half):
    groups, tiles, _, wide = out_ref.shape
    within = iota((groups, 8, wide), 1)
    leaving = []

    def put(tile, value):
        out_ref[:, tile] = value.astype(jnp.bfloat16)
        copy = pltpu.make_async_copy(out_ref.at[:, tile], out_any.at[:, tile], sems.at[tile])
        copy.start()
        leaving.append(copy)

    def total(kept_ref, came_ref, chunk):
        here = slice(chunk * wide, (chunk + 1) * wide)
        value = kept_ref[:, here].astype(jnp.float32) + came_ref[:, here].astype(jnp.float32)
        return value.reshape(groups, 8, wide)

    before = None
    for chunk in range(4):
        far = total(kept1_ref, came1_ref, chunk)
        near = total(kept0_ref, came0_ref, chunk)
        put(chunk, jnp.where(within < half, near, pltpu.roll(far, 1, 1)))
        start = (half - 1) * chunk % 8
        moved = pltpu.roll(far, start, 1) if start else far
        if chunk:
            put(3 + chunk, jnp.where(within < start, before, moved))
        before = moved
    for copy in leaving:
        copy.wait()


def total_rows(kept0, kept1, came0, came1, half):
    rows, share = kept0.shape
    shape = (rows // 8, 7, 8, share // 4)
    return pl.pallas_call(
        functools.partial(total_body, half=half),
        in_specs=[whole((rows, share))] * 4,
        out_specs=pl.BlockSpec(memory_space=pltpu.HBM),
        out_shape=pltpu.HBM(shape, jnp.bfloat16),
        scratch_shapes=[pltpu.VMEM(shape, jnp.bfloat16), pltpu.SemaphoreType.DMA((7,))],
        compiler_params=pltpu.CompilerParams(vmem_limit_bytes=16 * 2**20),
        name="total",
    )(kept0, kept1, came0, came1)


def weights_body(
    in0_ref, in1_ref, gr0_ref, gr1_ref, last0_ref, last1_ref,
    hid0_ref, hid1_ref, gb0_ref, gb1_ref, ub0_ref, ub1_ref,
    gate_ref, up_ref, down_ref, scale, early,
):
    count, wide = last0_ref.shape

    def flat(ref):
        return ref[:, 0].reshape(count, wide)

    gate_ref[...] = (
        contract_rows(flat(in0_ref), gb0_ref[...]) + contract_rows(flat(in1_ref), gb1_ref[...])
    ) * scale
    up_ref[...] = (
        contract_rows(flat(in0_ref), ub0_ref[...]) + contract_rows(flat(in1_ref), ub1_ref[...])
    ) * scale

    def put_down(grads0, grads1):
        down_ref[...] = (
            contract_rows(hid0_ref[...], grads0) + contract_rows(hid1_ref[...], grads1)
        ) * scale

    @pl.when(pl.program_id(0) < early)
    def _():
        put_down(flat(gr0_ref), flat(gr1_ref))

    @pl.when(pl.program_id(0) >= early)
    def _():
        put_down(last0_ref[...], last1_ref[...])


def weight_grads(rows0, rows1, own, other, scale):
    count, units = own[0].shape
    groups, tiles, _, chunk = rows0.shape
    width = chunk * (tiles + 1) // 2
    blocks = 8
    wide = width // blocks
    per = chunk // wide
    early = (width // chunk - 1) * per
    first = pl.BlockSpec((groups, 1, 8, wide), lambda i: (0, i // per, 0, i % per))

    def later(i):
        j = jnp.minimum(i, early - 1)
        return (0, width // chunk + j // per, 0, j % per)

    second = pl.BlockSpec((groups, 1, 8, wide), later)
    third = pl.BlockSpec((count, wide), lambda i: (0, jnp.maximum(i - early, 0)))
    flops = 3 * 2 * 2 * count * width * units
    return pl.pallas_call(
        functools.partial(weights_body, scale=scale, early=early),
        grid=(blocks,),
        in_specs=[first, first, second, second, third, third] + [whole((count, units))] * 6,
        out_specs=[
            pl.BlockSpec((wide, units), lambda i: (i, 0)),
            pl.BlockSpec((wide, units), lambda i: (i, 0)),
            pl.BlockSpec((units, wide), lambda i: (0, i)),
        ],
        out_shape=[
            jax.ShapeDtypeStruct((width, units), jnp.float32),
            jax.ShapeDtypeStruct((width, units), jnp.float32),
            jax.ShapeDtypeStruct((units, width), jnp.float32),
        ],
        cost_estimate=pl.CostEstimate(
            flops=flops, bytes_accessed=12 * width * units, transcendentals=0
        ),
        name="weight_grads",
        compiler_params=pltpu.CompilerParams(vmem_limit_bytes=58300000),
    )(
        rows0, rows1, rows0, rows1, own[1], other[1],
        own[0], other[0], own[2], other[2], own[3], other[3],
    )


def per_device(
    out_grad,
    moe_input,
    routes,
    route_weights,
    conv_result,
    glu_value,
    glu_gate,
    conv_taps,
    norm_gain,
    proj_weight,
    expert_gate,
    expert_up,
    expert_down,
):
    n_sp = lax.axis_size("sp")
    n_tp = lax.axis_size("tp")
    tok_rows, width = out_grad.shape
    top_count = routes.shape[1]
    capacity = 2 * top_count * tok_rows // n_sp
    half = capacity // n_tp
    slots = n_sp * capacity
    tp = lax.axis_index("tp")
    tp_array = tp.reshape(1).astype(jnp.int32)
    share = width // n_tp
    channels = conv_result.shape[1] * n_tp

    send = dispatch(tp_array, routes.T, route_weights.T, moe_input, out_grad, n_sp, half)
    rows0 = lax.all_to_all(
        send.reshape(n_sp, half * 8, -1), "sp", split_axis=0, concat_axis=0, tiled=True
    ).reshape(send.shape)
    rows1 = lax.ppermute(rows0, "tp", swap)

    gate, up, down = expert_gate[0], expert_up[0], expert_down[0]
    own = expert(tp_array, rows0, gate, up, down, "expert_own")
    other = expert(tp_array, rows1, gate, up, down, "expert_other")
    came1 = lax.ppermute(own[4], "tp", swap)
    came0 = lax.ppermute(other[4], "tp", swap)
    kept0, kept1 = kept_partials(tp_array, own[2], own[3], other[2], other[3], gate, up)
    summed = total_rows(kept0, kept1, came0, came1, half)
    returned = lax.all_to_all(
        summed.reshape(n_sp, 56, share // 4), "sp", split_axis=0, concat_axis=0, tiled=True
    ).reshape(summed.shape)
    gate_g, up_g, down_g = weight_grads(rows0, rows1, own, other, float(slots) ** (-0.5))

    conv_result, gate_g = lax.optimization_barrier((conv_result, gate_g))
    values = conv_result.astype(jnp.float32)
    sums = lax.psum(
        (jnp.sum(values, axis=1), jnp.sum(values * values, axis=1)), "tp"
    )
    center = sums[0] / channels
    spread = sums[1] / channels - center * center
    inv_std = lax.rsqrt(spread + norm_eps)[:, None]
    normed = (values - center[:, None]) * inv_std
    scaled = normed * norm_gain[None, :]
    sig_norm = jax.nn.sigmoid(scaled)
    activ = (scaled * sig_norm).astype(jnp.bfloat16)

    returned, activ, gate_g, up_g, down_g = lax.optimization_barrier(
        (returned, activ, gate_g, up_g, down_g)
    )
    here = combine(tp_array, routes.T, returned, out_grad, half)
    there = lax.ppermute(here, "tp", swap)
    token_scale = float(tok_rows * n_sp) ** (-0.5)
    proj = proj_part(tp_array, here, activ, token_scale, None)
    proj = proj_part(tp_array, there, activ, token_scale, proj)
    proj_parts = proj.reshape(n_sp, width // n_sp, -1)
    proj_grad = last_sum(
        lax.all_to_all(proj_parts, "sp", split_axis=0, concat_axis=0, tiled=True)
    )
    here, there, conv_taps, side, _ = lax.optimization_barrier(
        (here, there, conv_taps, tp_array, proj)
    )
    input_grad = jnp.where(
        side[0] == 0,
        jnp.concatenate([here, there], axis=1),
        jnp.concatenate([there, here], axis=1),
    )
    act_grad = matmul(input_grad, proj_weight)
    norm_grad = act_grad * sig_norm * (1.0 + scaled * (1.0 - sig_norm)) * norm_gain[None, :]
    first, second = lax.psum(
        (jnp.sum(norm_grad, axis=1), jnp.sum(norm_grad * normed, axis=1)), "tp"
    )
    conv_grad = inv_std * (
        norm_grad - first[:, None] / channels - normed * (second[:, None] / channels)
    )
    reach = conv_taps.shape[0]
    rim = from_behind(conv_grad[: reach - 1].astype(jnp.bfloat16), "sp", -1).astype(jnp.float32)
    extended = jnp.concatenate([conv_grad, rim], axis=0)
    taps_float = conv_taps.astype(jnp.float32)
    mixed_grad = jnp.zeros_like(conv_grad)
    for lag in range(reach):
        mixed_grad = (
            mixed_grad + taps_float[reach - 1 - lag][None, :] * extended[lag : lag + tok_rows]
        )
    sig_gate = jax.nn.sigmoid(glu_gate.astype(jnp.float32))
    value_grad = (mixed_grad * sig_gate).astype(jnp.bfloat16)
    gate_side_grad = (
        mixed_grad * glu_value.astype(jnp.float32) * sig_gate * (1.0 - sig_gate)
    ).astype(jnp.bfloat16)
    return (
        input_grad,
        proj_grad,
        gate_g[None],
        up_g[None],
        down_g[None],
        value_grad,
        gate_side_grad,
    )


def solution(mesh):
    in_specs = (
        P("sp", None),
        P("sp", None),
        P("sp", None),
        P("sp", None),
        P("sp", "tp"),
        P("sp", "tp"),
        P("sp", "tp"),
        P(None, "tp"),
        P("tp"),
        P(None, "tp"),
        P("sp", None, "tp"),
        P("sp", None, "tp"),
        P("sp", "tp", None),
    )
    out_specs = (
        P("sp", None),
        P("sp", "tp"),
        P("sp", None, "tp"),
        P("sp", None, "tp"),
        P("sp", "tp", None),
        P("sp", "tp"),
        P("sp", "tp"),
    )
    return jax.shard_map(
        per_device, mesh=mesh, in_specs=in_specs, out_specs=out_specs, check_vma=False
    )
```
